32 devices in a mesh: sp: 4 (over z), fs: 4 (over y, x), tp: 2 (over core).
Axes of the slice: x: 2, y: 2, z: 4, core: 2. Of those that a mesh axis runs over, the one named last changes fastest.
Arguments:
- statespace_input: bfloat16 [4, 1536, 2048], P('fs', 'sp', 'tp'), may hold values from -6 to 6
- output_gate_input: bfloat16 [4, 1536, 2048], P('fs', 'sp', 'tp'), may hold values from -6 to 6
- state_input_projection: bfloat16 [4, 1536, 512], P('fs', 'sp', 'tp'), may hold values from -6 to 6
- state_output_projection: bfloat16 [4, 1536, 512], P('fs', 'sp', 'tp'), may hold values from -6 to 6
- step_size_input: bfloat16 [4, 1536, 32], P('fs', 'sp', 'tp'), may hold values from -5 to 5
- added_log_decay: float32 [4, 1536, 32], P('fs', 'sp', 'tp'), may hold values from -0.7 to 0
- logarithm_rates: float32 [32], replicated, may hold values from -20 to -2.9
- head_channel_taps: bfloat16 [4, 2048], replicated, may hold values from -3 to 3
- input_projection_taps: bfloat16 [4, 512], replicated, may hold values from -3 to 3
- output_projection_taps: bfloat16 [4, 512], replicated, may hold values from -3 to 3
- input_projection_bias: bfloat16 [512], replicated, may hold values from -0.59765625 to -0.19921875
- group_norm_gain: bfloat16 [2048], replicated, may hold values from 0.099609375 to 1.8984375
- pooling_input: bfloat16 [4, 1536, 1024], P('fs', 'sp', 'tp'), may hold values from -6 to 6
- pooling_group_weight: bfloat16 [4, 256, 256], replicated, may hold values from -0.375 to 0.375
- pooling_channel_scale: bfloat16 [1024], replicated, may hold values from 0.099609375 to 1.8984375
- statespace_output_weight: bfloat16 [2048, 4096], P('tp', ('sp', 'fs')), may hold values from -8 to 8
- pooling_output_weight: bfloat16 [1024, 4096], P('tp', ('sp', 'fs')), may hold values from -8 to 8
- output_norm_gain: bfloat16 [4096], replicated, may hold values from 0.099609375 to 1.8984375
Outputs:
- output: bfloat16 [4, 1536, 4096], P('fs', 'sp', 'tp')
The draws below stay inside these ranges and needn't reach their ends.
All inputs are finite; a program needn't handle non-finite values.
Results may differ from the reference program's by a relative error of at most 0.02.
Values may be sent and summed in bfloat16 or wider, within the bound.
A program may use at most 128 MiB of HBM per device.

```python
import jax
import jax.numpy as jnp
from jax import lax

D = 4096
HEADS = 32
HEAD_DIM = 64
GROUPS = 4
STATE = 128
CONV = 4
BLOCK = 128
POOL_GROUPS = 4
POOL_GROUP = 256
TOK_DEV = 384
INNER = 2048
POOL = 1024
SEQUENCE_TOKENS = 1536
SEQS = 4
N_TP = 2


def draw_step_size_input(key, part):
    noise_key, level_key = jax.random.split(jax.random.fold_in(key, 3))
    blocks = SEQUENCE_TOKENS // TOK_DEV
    levels = jax.random.uniform(level_key, (SEQS, blocks, 1, HEADS), jnp.float32, -1.2, 1.2)
    noise_part = 0.7 * jax.random.normal(noise_key, (SEQS, blocks, TOK_DEV, HEADS), jnp.float32)
    values = jnp.clip(levels + noise_part, -5.0, 5.0)
    return values.reshape(SEQS, SEQUENCE_TOKENS, HEADS).astype(jnp.bfloat16)


def draw_logarithm_rates(key, part):
    order_key, fast_key, slow_key = jax.random.split(jax.random.fold_in(key, 5), 3)
    shuffled = jax.random.permutation(order_key, HEADS)
    fast_heads = shuffled < HEADS // 2
    fast_rate = jnp.exp(jax.random.uniform(fast_key, (HEADS,), jnp.float32, jnp.log(0.02), jnp.log(0.05)))
    slow_rate = jax.random.uniform(slow_key, (HEADS,), jnp.float32, 0.15, 0.45) / SEQUENCE_TOKENS
    return jnp.log(jnp.where(fast_heads, fast_rate, slow_rate)).astype(jnp.float32)


def draw_added_log_decay(key, part):
    first_key, second_key, size_key = jax.random.split(jax.random.fold_in(key, 9), 3)
    half_len = SEQUENCE_TOKENS // 2
    first_position = jax.random.randint(first_key, (SEQS, 1), 0, half_len)
    second_position = jax.random.randint(second_key, (SEQS, 1), 0, SEQUENCE_TOKENS - half_len) + half_len
    spike_positions = jnp.concatenate([first_position, second_position], axis=1)
    retained_fraction = jax.random.uniform(size_key, (SEQS, 2, HEADS), jnp.float32, 0.5, 0.8)
    spike_hits = (jnp.arange(SEQUENCE_TOKENS, dtype=jnp.int32)[None, :, None] == spike_positions[:, None, :]).astype(jnp.float32)
    return jnp.einsum('lga,lab->lgb', spike_hits, jnp.log(retained_fraction)).astype(jnp.float32)


def column_scales(key):
    noise_part = jnp.clip(jax.random.normal(jax.random.fold_in(key, 17), (D,), jnp.float32), -2.0, 2.0)
    column_ramp = jnp.arange(D, dtype=jnp.float32) / D
    log_scale = jnp.log(0.3) + jnp.log(10.0) * column_ramp
    return jnp.exp(log_scale + 0.3 * noise_part)


def draw_statespace_output_weight(key, part):
    values = jnp.clip(jax.random.normal(jax.random.fold_in(key, 21), (INNER, D), jnp.float32), -6.0, 6.0)
    scaled = values * column_scales(key)[None, :] / jnp.sqrt(jnp.float32(INNER + POOL))
    return jnp.clip(scaled, -8.0, 8.0).astype(jnp.bfloat16)


def draw_pooling_output_weight(key, part):
    values = jnp.clip(jax.random.normal(jax.random.fold_in(key, 23), (POOL, D), jnp.float32), -6.0, 6.0)
    scaled = values * column_scales(key)[None, :] / jnp.sqrt(jnp.float32(INNER + POOL))
    return jnp.clip(scaled, -8.0, 8.0).astype(jnp.bfloat16)


def steps_of(key, dims, cuts, smallest, high):
    level = 1.0
    for axis_at, shards_of in cuts:
        draws = jax.random.uniform(jax.random.fold_in(jax.random.fold_in(key, 6), axis_at), (shards_of,), jnp.float32, smallest / len(cuts), high / len(cuts))
        level = level * jnp.repeat(jnp.exp(draws), dims[axis_at] // shards_of).reshape((-1,) + (1,) * (len(dims) - 1 - axis_at))
    return level


def noise(own_key, shape, width, most, cuts=(), kind=jnp.bfloat16):
    loudness = steps_of(own_key, shape, cuts, -0.22, 0.18) if cuts else 1.0
    entries = jax.random.normal(own_key, shape, jnp.float32) * width * loudness
    return jnp.minimum(jnp.maximum(entries, -most), most).astype(kind)


def setup_inputs(seed: int = 0) -> dict:
    arg_keys = jax.random.split(jax.random.key(seed), 19)
    statespace_input = noise(arg_keys[0], (SEQS, SEQUENCE_TOKENS, INNER), 1.0, 6.0, ((0, 4), (1, 4), (2, 2)))
    output_gate_input = noise(arg_keys[1], (SEQS, SEQUENCE_TOKENS, INNER), 1.0, 6.0, ((0, 4), (1, 4), (2, 2)))
    state_input_projection = noise(arg_keys[2], (SEQS, SEQUENCE_TOKENS, GROUPS * STATE), 1.0, 6.0, ((0, 4), (1, 4), (2, 2)))
    state_output_projection = noise(arg_keys[3], (SEQS, SEQUENCE_TOKENS, GROUPS * STATE), 1.0, 6.0, ((0, 4), (1, 4), (2, 2)))
    step_size_input = draw_step_size_input(jax.random.fold_in(arg_keys[18], 71), 0)
    added_log_decay = draw_added_log_decay(jax.random.fold_in(arg_keys[18], 71), 0)
    logarithm_rates = draw_logarithm_rates(jax.random.fold_in(arg_keys[18], 71), 0)
    head_channel_taps = noise(arg_keys[7], (CONV, INNER), CONV ** -0.5, 3.0)
    input_projection_taps = noise(arg_keys[8], (CONV, GROUPS * STATE), CONV ** -0.5, 3.0)
    output_projection_taps = noise(arg_keys[9], (CONV, GROUPS * STATE), CONV ** -0.5, 3.0)
    input_projection_bias = jnp.clip(jax.random.uniform(arg_keys[10], (GROUPS * STATE,), jnp.float32, -0.59765625, -0.19921875), -0.59765625, -0.19921875).astype(jnp.bfloat16)
    group_norm_gain = jnp.clip(1.0 + 0.18 * jax.random.normal(arg_keys[11], (INNER,), jnp.float32), 0.099609375, 1.8984375).astype(jnp.bfloat16)
    pooling_input = noise(arg_keys[12], (SEQS, SEQUENCE_TOKENS, POOL), 1.0, 6.0, ((0, 4), (1, 4), (2, 2)))
    pooling_group_weight = noise(arg_keys[13], (POOL_GROUPS, POOL_GROUP, POOL_GROUP), POOL_GROUP ** -0.5, 0.375)
    pooling_channel_scale = jnp.clip(1.0 + 0.18 * jax.random.normal(arg_keys[14], (POOL,), jnp.float32), 0.099609375, 1.8984375).astype(jnp.bfloat16)
    statespace_output_weight = draw_statespace_output_weight(jax.random.fold_in(arg_keys[18], 71), 0)
    pooling_output_weight = draw_pooling_output_weight(jax.random.fold_in(arg_keys[18], 71), 0)
    output_norm_gain = jnp.clip(1.0 + 0.18 * jax.random.normal(arg_keys[17], (D,), jnp.float32), 0.099609375, 1.8984375).astype(jnp.bfloat16)
    return {"statespace_input": statespace_input, "output_gate_input": output_gate_input, "state_input_projection": state_input_projection, "state_output_projection": state_output_projection, "step_size_input": step_size_input, "added_log_decay": added_log_decay, "logarithm_rates": logarithm_rates, "head_channel_taps": head_channel_taps, "input_projection_taps": input_projection_taps, "output_projection_taps": output_projection_taps, "input_projection_bias": input_projection_bias, "group_norm_gain": group_norm_gain, "pooling_input": pooling_input, "pooling_group_weight": pooling_group_weight, "pooling_channel_scale": pooling_channel_scale, "statespace_output_weight": statespace_output_weight, "pooling_output_weight": pooling_output_weight, "output_norm_gain": output_norm_gain}


eps = 1e-06

def causal_taps(input_rows, prior_rows, tap_weights, offset_bias):
    padded = jnp.concatenate([prior_rows, input_rows], axis=1).astype(jnp.float32)
    tok_rows = input_rows.shape[1]
    running = jnp.zeros(input_rows.shape, jnp.float32) + offset_bias
    for tap_index in range(tap_weights.shape[0]):
        running = running + tap_weights[tap_index].astype(jnp.float32) * padded[:, tap_index:tap_index + tok_rows]
    return jax.nn.silu(running).astype(jnp.bfloat16)

def pool_mix(input_rows, prior_rows, positions, group_ids, pooling_group_weight, pooling_channel_scale):
    tail_rows = prior_rows.shape[1]
    tok_rows = input_rows.shape[1]
    padded = jnp.concatenate([prior_rows, input_rows], axis=1).astype(jnp.float32)
    window_reach = jnp.left_shift(jnp.int32(2), group_ids)
    running = jnp.zeros(input_rows.shape, jnp.float32)
    for offset_back in range(tail_rows + 1):
        start_row = tail_rows - offset_back
        running = running + padded[:, start_row:start_row + tok_rows] * (offset_back < window_reach).astype(jnp.float32)
    window_count = jnp.minimum(positions[:, None] + 1.0, window_reach.astype(jnp.float32)[None, :])
    pooled = (running / window_count - input_rows.astype(jnp.float32)).astype(jnp.bfloat16)
    grouped = pooled.reshape(input_rows.shape[:2] + (pooling_group_weight.shape[0], pooling_group_weight.shape[1]))
    mixed = jnp.einsum('slgc,gcd->slgd', grouped.astype(jnp.float32), pooling_group_weight.astype(jnp.float32))
    return (mixed.reshape(input_rows.shape) * pooling_channel_scale.astype(jnp.float32)).astype(jnp.bfloat16)

def reference(statespace_input, output_gate_input, state_input_projection, state_output_projection, step_size_input, added_log_decay, logarithm_rates, head_channel_taps, input_projection_taps, output_projection_taps, input_projection_bias, group_norm_gain, pooling_input, pooling_group_weight, pooling_channel_scale, statespace_output_weight, pooling_output_weight, output_norm_gain):
    seq_count = statespace_input.shape[0]
    number_of_blocks = SEQUENCE_TOKENS // BLOCK
    per_group = HEADS // GROUPS
    pool_tail = 2 ** POOL_GROUPS - 1

    def block_split(source):
        return jnp.moveaxis(source.reshape((seq_count, number_of_blocks, BLOCK) + source.shape[2:]), 1, 0)
    mixer_inputs = (block_split(statespace_input), block_split(output_gate_input), block_split(state_input_projection), block_split(state_output_projection), block_split(step_size_input), block_split(added_log_decay), block_split(pooling_input), jnp.arange(number_of_blocks, dtype=jnp.int32))
    group_ids = jnp.arange(POOL, dtype=jnp.int32) // POOL_GROUP
    head_decay_rates = jnp.exp(logarithm_rates)
    causal = jnp.arange(BLOCK)[:, None] >= jnp.arange(BLOCK)[None, :]
    share_ssd = INNER // N_TP
    share_pool = POOL // N_TP

    def advance(carried, current_inputs):
        state_now, prior_x, prior_b, prior_c, prior_pool = carried
        head_channel_rows, output_gate_rows, input_projection_rows, output_projection_rows, step_size_rows, decay_spikes, pooling_rows, current_block_index = current_inputs
        x_conv = causal_taps(head_channel_rows, prior_x, head_channel_taps, 0.0)
        b_conv = causal_taps(input_projection_rows, prior_b, input_projection_taps, input_projection_bias.astype(jnp.float32))
        c_conv = causal_taps(output_projection_rows, prior_c, output_projection_taps, 0.0)
        discrete_step_size = jax.nn.softplus(step_size_rows.astype(jnp.float32))
        cumulative_decay = jnp.cumsum(-discrete_step_size * head_decay_rates + decay_spikes, axis=1)
        cumulative_decay = cumulative_decay.reshape(seq_count, BLOCK, GROUPS, per_group)
        cum_t = cumulative_decay.transpose(0, 2, 3, 1)
        step_t = discrete_step_size.reshape(seq_count, BLOCK, GROUPS, per_group).transpose(0, 2, 3, 1)
        heads_x = x_conv.reshape(seq_count, BLOCK, GROUPS, per_group, HEAD_DIM).astype(jnp.float32)
        group_b = b_conv.reshape(seq_count, BLOCK, GROUPS, STATE).astype(jnp.float32)
        group_c = c_conv.reshape(seq_count, BLOCK, GROUPS, STATE).astype(jnp.float32)
        scores = jnp.einsum('stgn,sugn->sgtu', group_c, group_b)
        decay_gap = cum_t[..., :, None] - cum_t[..., None, :]
        decay_factor = jnp.where(causal, jnp.exp(jnp.where(causal, decay_gap, 0.0)), 0.0)
        weights = (scores[:, :, None] * decay_factor * step_t[..., None, :]).astype(jnp.bfloat16)
        within = jnp.einsum('sgetu,sugep->stgep', weights.astype(jnp.float32), heads_x)
        entering = lax.optimization_barrier(state_now.astype(jnp.bfloat16))
        carried_out = jnp.einsum('stgn,sgepn->stgep', group_c, entering.astype(jnp.float32))
        carried_out = carried_out * jnp.exp(cumulative_decay)[..., None]
        block_end = cum_t[..., -1]
        end_weight = jnp.exp(block_end[..., None] - cum_t) * step_t
        scaled_x = lax.optimization_barrier((heads_x * end_weight.transpose(0, 3, 1, 2)[..., None]).astype(jnp.bfloat16))
        block_state = jnp.einsum('sugep,sugn->sgepn', scaled_x.astype(jnp.float32), group_b)
        next_state = state_now * jnp.exp(block_end)[..., None, None] + block_state
        mixed_ssd = (within + carried_out).reshape(seq_count, BLOCK, INNER) * jax.nn.silu(output_gate_rows.astype(jnp.float32))
        grouped = mixed_ssd.reshape(seq_count, BLOCK, GROUPS, INNER // GROUPS)
        normed = grouped * lax.rsqrt(lax.optimization_barrier(jnp.mean(grouped * grouped, axis=-1, keepdims=True)) + eps)
        ssd_out = (normed.reshape(seq_count, BLOCK, INNER) * group_norm_gain.astype(jnp.float32)).astype(jnp.bfloat16)
        positions = (current_block_index * BLOCK + jnp.arange(BLOCK, dtype=jnp.int32)).astype(jnp.float32)
        pool_out = pool_mix(pooling_rows, prior_pool, positions, group_ids, pooling_group_weight, pooling_channel_scale)
        flat_ssd = ssd_out.reshape(seq_count * BLOCK, INNER)
        flat_pool = pool_out.reshape(seq_count * BLOCK, POOL)
        total = jnp.zeros((seq_count * BLOCK, D), jnp.float32)
        for part_index in range(N_TP):
            partial_value = jnp.dot(flat_ssd[:, part_index * share_ssd:(part_index + 1) * share_ssd], statespace_output_weight[part_index * share_ssd:(part_index + 1) * share_ssd], preferred_element_type=jnp.float32)
            partial_value = partial_value + jnp.dot(flat_pool[:, part_index * share_pool:(part_index + 1) * share_pool], pooling_output_weight[part_index * share_pool:(part_index + 1) * share_pool], preferred_element_type=jnp.float32)
            rounded = lax.optimization_barrier(partial_value.astype(jnp.bfloat16))
            total = total + rounded.astype(jnp.float32)
        inv_root = lax.rsqrt(lax.optimization_barrier(jnp.mean(total * total, axis=1, keepdims=True)) + eps)
        output = (total * inv_root * output_norm_gain.astype(jnp.float32)).astype(jnp.bfloat16)
        next_carry = (next_state, head_channel_rows[:, BLOCK - CONV + 1:], input_projection_rows[:, BLOCK - CONV + 1:], output_projection_rows[:, BLOCK - CONV + 1:], pooling_rows[:, BLOCK - pool_tail:])
        return (next_carry, output.reshape(seq_count, BLOCK, D))
    start_carry = (jnp.zeros((seq_count, GROUPS, per_group, HEAD_DIM, STATE), jnp.float32), jnp.zeros((seq_count, CONV - 1, INNER), jnp.bfloat16), jnp.zeros((seq_count, CONV - 1, GROUPS * STATE), jnp.bfloat16), jnp.zeros((seq_count, CONV - 1, GROUPS * STATE), jnp.bfloat16), jnp.zeros((seq_count, pool_tail, POOL), jnp.bfloat16))
    final_carry, outputs = lax.scan(advance, start_carry, mixer_inputs)
    return jnp.moveaxis(outputs, 0, 1).reshape(seq_count, SEQUENCE_TOKENS, D)
```

```python
import functools

import jax
import jax.numpy as jnp
from jax import lax
from jax.experimental import pallas as pl
from jax.experimental.pallas import tpu as pltpu
from jax.sharding import PartitionSpec as P

D = 4096
HEAD_DIM = 64
STATE = 128
CONV = 4
BLOCK = 128
POOL_GROUPS = 4
POOL_GROUP = 256


eps = 1e-06


def passed_along(block, axis, distance):
    devices = range(lax.axis_size(axis))
    route = [(i - distance, i) for i in devices if i - distance in devices]
    return lax.ppermute(block, axis, route)


def entering_2(array, axis, join, neutral):
    place = lax.axis_index(axis)
    gathered = jax.tree.map(
        lambda a, kind: lax.all_gather(a.astype(kind), axis), array, (jnp.bfloat16, jnp.bfloat16)
    )
    state = jax.tree.map(lambda a, e: jnp.zeros_like(a) + jnp.asarray(e, a.dtype), array, neutral)

    def one(lap, state):
        return join(
            state,
            jax.tree.map(
                lambda a, own: lax.dynamic_index_in_dim(a, lap, 0, False).astype(own.dtype),
                gathered,
                array,
            ),
        )

    return lax.fori_loop(0, place, one, state)


MESH_IDS = pl.DeviceIdType.MESH
EXACT = lax.Precision.HIGHEST
CHUNKS = 6
PAUSE = 0


class Links:
    def __init__(self, sp_size, fs_size):
        self.n = sp_size
        self.z = lax.axis_index("sp")
        self.fs = lax.axis_index("fs")
        self.core = lax.axis_index("tp")
        self.x = lax.rem(self.fs, 2)
        self.y = self.fs // 2
        self.beside = {"fs": self.fs + 1 - 2 * self.x}
        self.across = {"fs": self.fs + 2 - 4 * self.y}
        self.sibling = {"tp": 1 - self.core}

    def barrier(self):
        barrier = pltpu.get_barrier_semaphore()
        near = [{"sp": lax.rem(self.z + far, self.n)} for far in (1, self.n - 1)]
        for other in (*near, self.beside, self.across, self.sibling):
            pl.semaphore_signal(barrier, inc=1, device_id=other, device_id_type=MESH_IDS)
        pl.semaphore_wait(barrier, len(near) + 3)

    def within(self, place):
        return jnp.logical_and(place >= 0, place < self.n)

    def nearest(self, turn):
        if turn == 0:
            return self.z
        low, high = self.z, self.n - 1 - self.z
        small = jnp.minimum(low, high)
        both = turn <= 2 * small
        far = jnp.where(both, (turn + 1) // 2, turn - small)
        sign = jnp.where(both, 1 - 2 * (turn % 2), jnp.where(high > low, 1, -1))
        return self.z + sign * far


def remote(src, dst, sends, arrivals, spot, device):
    return pltpu.make_async_remote_copy(
        src_ref=src,
        dst_ref=dst,
        send_sem=sends.at[spot],
        recv_sem=arrivals.at[spot],
        device_id=device,
        device_id_type=MESH_IDS,
    )


class Weights:
    def __init__(self, links, whole, width, z_sems, y_sems):
        self.links, self.whole, self.width = links, whole, width
        self.z_sems, self.y_sems = z_sems, y_sems
        self.rows = whole.shape[0] // CHUNKS
        self.direct = range(CHUNKS - 1)
        self.turned = (CHUNKS - 1,)
        self.sent = []

    def region(self, chunk, z, y):
        at = pl.multiple_of((z * 2 + y) * self.width, self.width)
        return self.whole.at[pl.ds(chunk * self.rows, self.rows), pl.ds(at, self.width)]

    def along(self, chunk, step, way, side, arriving):
        links = self.links
        origin = links.z - way * (step if arriving else step - 1)
        y = links.y if side == 0 else 1 - links.y
        spot = ((chunk * (links.n - 1) + step - 1) * 2 + (way < 0)) * 2 + side
        place = self.region(chunk, jnp.clip(origin, 0, links.n - 1), y)
        copy = remote(place, place, *self.z_sems, spot, {"sp": links.z + way})
        far = links.z if arriving else links.z + way
        return copy, jnp.logical_and(links.within(origin), links.within(far))

    def over(self, chunk, offset, arriving):
        links = self.links
        y = 1 - links.y if arriving else links.y
        origin = links.z + offset
        place = self.region(chunk, jnp.clip(origin, 0, links.n - 1), y)
        spot = chunk * (2 * links.n - 1) + offset + links.n - 1
        copy = remote(place, place, *self.y_sems, spot, links.across)
        return copy, links.within(origin)

    def go(self, kind, *key):
        copy, here = kind(*key, False)
        self.sent.append((kind, key))
        pl.when(here)(copy.start)

    def take(self, kind, *key):
        copy, here = kind(*key, True)
        pl.when(here)(copy.wait_recv)

    def pass_on(self, chunk, step, way, side):
        if step < self.links.n:
            self.go(self.along, chunk, step, way, side)

    def begin(self):
        for chunk in self.turned:
            self.go(self.over, chunk, 0)
        for chunk in self.direct:
            for way in (1, -1):
                self.pass_on(chunk, 1, way, 0)
            self.go(self.over, chunk, 0)
        for chunk in self.turned:
            for way in (1, -1):
                self.pass_on(chunk, 1, way, 0)

    def turn(self):
        for chunk in self.turned:
            self.take(self.over, chunk, 0)
            for way in (1, -1):
                self.pass_on(chunk, 1, way, 1)

    def hop(self, step, chunk):
        for way in (1, -1):
            if chunk in self.turned:
                for side in (0, 1):
                    self.take(self.along, chunk, step, way, side)
                    self.pass_on(chunk, step + 1, way, side)
            else:
                self.take(self.along, chunk, step, way, 0)
                self.pass_on(chunk, step + 1, way, 0)
                self.go(self.over, chunk, -way * step)

    def settle(self, step):
        for chunk in self.direct:
            for offset in (0,) if step == 0 else (step, -step):
                self.take(self.over, chunk, offset)

    def finish(self):
        for kind, key in self.sent:
            copy, here = kind(*key, False)
            pl.when(here)(copy.wait_send)


def silu(rows):
    return rows / (1.0 + jnp.exp(-rows))


def softplus(rows):
    return jnp.maximum(rows, 0.0) + jnp.log(1.0 + jnp.exp(-jnp.abs(rows)))


def chosen(core, options):
    best = options[0]
    for at in range(1, len(options)):
        best = jnp.where(core == at, options[at], best)
    return best


def mixers(links, tail, cores, refs, sems):
    (x_in, gate, b_in, c_in, dt, added, rates, x_taps, b_taps, c_taps, bias, gain, pool_in,
     pool_weight, pool_scale, prior_x, prior_b, prior_c, prior_pool, x_pad, bc_pad, pool_pad,
     pool_two, pool_four, x_split, bc_conv, b_turned, cum_all, step_all, within, grown, local_in,
     state, before, carry_in, carry_out, channels, far_channels) = refs
    sends, arrivals = sems
    rows, inner = x_in.shape[1:]
    heads = dt.shape[2]
    wide = b_in.shape[2]
    pool = pool_in.shape[2]
    groups = wide // STATE
    span = inner // groups
    blocks = rows // BLOCK
    z, core = links.z, links.core
    lead = 8
    sources = ((x_in, prior_x), (b_in, prior_b), (c_in, prior_c), (pool_in, prior_pool))

    def tails(at):
        source, target = sources[at]
        return remote(
            source.at[0, pl.ds(rows - tail, tail)], target, sends, arrivals, at, {"sp": z + 1}
        )

    def chain(group):
        return remote(
            carry_out.at[group], carry_in.at[group], sends, arrivals, 4 + group, {"sp": z + 1}
        )

    def pool_letter():
        cols = pl.ds(inner, pool)
        return remote(
            channels.at[:, cols], far_channels.at[:, cols], sends, arrivals, 4 + groups, links.beside
        )

    def block_letter(at):
        place = (pl.ds(at * BLOCK, BLOCK), pl.ds(0, inner))
        return remote(
            channels.at[place], far_channels.at[place], sends, arrivals, 5 + groups + at, links.beside
        )

    follows = z + 1 < links.n

    @pl.when(follows)
    def _():
        for at in range(4):
            tails(at).start()

    yield
    x_pad[tail:] = x_in[0].astype(jnp.float32)
    bc_pad[tail:, 0:wide] = b_in[0].astype(jnp.float32)
    bc_pad[tail:, wide:] = c_in[0].astype(jnp.float32)
    pool_pad[0:lead] = jnp.zeros((lead, pool), jnp.float32)
    pool_pad[lead + tail :] = pool_in[0].astype(jnp.float32)
    cum_all[...] = jnp.zeros_like(cum_all)
    step_all[...] = jnp.zeros_like(step_all)
    steps = softplus(dt[0].astype(jnp.float32))
    step_all[:, 0:heads] = steps
    own_rates = chosen(core, [rates[:, c * heads : (c + 1) * heads] for c in range(cores)])
    logs = -steps * jnp.exp(own_rates) + added[0]
    down = lax.broadcasted_iota(jnp.int32, (BLOCK, BLOCK), 0)
    over = lax.broadcasted_iota(jnp.int32, (BLOCK, BLOCK), 1)
    causal = down >= over
    lower = causal.astype(jnp.float32)
    first_half = lax.broadcasted_iota(jnp.int32, (BLOCK, 2 * HEAD_DIM), 1) < HEAD_DIM

    def mine(ref, size):
        at = pl.multiple_of(core * size, size)
        return ref[:, pl.ds(at, size)].astype(jnp.float32)

    taps_x = mine(x_taps, inner)
    taps_bc = jnp.concatenate([mine(b_taps, wide), mine(c_taps, wide)], axis=1)
    bias_b = mine(bias, wide)
    bias_bc = jnp.concatenate([bias_b, jnp.zeros_like(bias_b)], axis=1)

    @pl.when(z == 0)
    def _():
        x_pad[0:tail] = jnp.zeros((tail, inner), jnp.float32)
        bc_pad[0:tail] = jnp.zeros((tail, 2 * wide), jnp.float32)
        pool_pad[lead : lead + tail] = jnp.zeros((tail, pool), jnp.float32)

    @pl.when(z > 0)
    def _():
        for at in range(4):
            tails(at).wait_recv()
        x_pad[0:tail] = prior_x[...].astype(jnp.float32)
        bc_pad[0:tail, 0:wide] = prior_b[...].astype(jnp.float32)
        bc_pad[0:tail, wide:] = prior_c[...].astype(jnp.float32)
        pool_pad[lead : lead + tail] = prior_pool[...].astype(jnp.float32)

    def taps(pad, weights, at, cols):
        total = None
        for tap in range(CONV):
            begin = at * BLOCK + tail - CONV + 1 + tap
            term = pad[begin : begin + BLOCK, cols] * weights[tap : tap + 1, cols]
            total = term if total is None else total + term
        return total

    def spread(narrow, head):
        shape = (BLOCK, 2 * HEAD_DIM)
        return jnp.where(
            first_half,
            jnp.broadcast_to(narrow[:, head : head + 1], shape),
            jnp.broadcast_to(narrow[:, head + 1 : head + 2], shape),
        )

    yield
    pairs = span // (2 * HEAD_DIM)
    ends = []
    state[...] = jnp.zeros_like(state)
    for at in range(blocks):
        now = slice(at * BLOCK, (at + 1) * BLOCK)
        bc_conv[now] = silu(taps(bc_pad, taps_bc, at, slice(0, 2 * wide)) + bias_bc).astype(
            jnp.bfloat16
        )
        cum = jnp.dot(lower, logs[now], precision=EXACT, preferred_element_type=jnp.float32)
        cum_all[now, 0:heads] = cum
        decayed = jnp.exp(cum)
        closing = jnp.exp(cum[BLOCK - 1 : BLOCK] - cum) * steps[now]
        ended = []
        for group in range(groups):
            cols = slice(group * span, (group + 1) * span)
            x_now = silu(taps(x_pad, taps_x, at, cols))
            b_now = bc_conv[now, group * STATE : (group + 1) * STATE]
            b_flat = jnp.transpose(b_now.astype(jnp.float32)).astype(jnp.bfloat16)
            b_turned[at * groups + group] = b_flat
            scaled = []
            for pair in range(pairs):
                head = group * (span // HEAD_DIM) + 2 * pair
                lanes = slice(pair * 2 * HEAD_DIM, (pair + 1) * 2 * HEAD_DIM)
                here = slice(head * HEAD_DIM, (head + 2) * HEAD_DIM)
                x_pair = x_now[:, lanes]
                x_split[at, 0:BLOCK, here] = jnp.where(first_half, x_pair, 0.0).astype(jnp.bfloat16)
                x_split[at, BLOCK : 2 * BLOCK, here] = jnp.where(first_half, 0.0, x_pair).astype(
                    jnp.bfloat16
                )
                x_half = x_pair.astype(jnp.bfloat16).astype(jnp.float32)
                scaled.append((x_half * spread(closing, head)).astype(jnp.bfloat16))
                grown[now, here] = spread(decayed, head)
            end = grown[(at + 1) * BLOCK - 1 : (at + 1) * BLOCK, cols]
            ended.append(end)
            local_in[at, :, cols] = state[:, cols]
            state[:, cols] = state[:, cols] * end + jnp.dot(
                b_flat, jnp.concatenate(scaled, axis=1), preferred_element_type=jnp.float32
            )
            yield
        ends.append(ended)

    def hand_on():
        @pl.when(z == 0)
        def _():
            before[...] = jnp.zeros_like(before)

        for group in range(groups):
            cols = slice(group * span, (group + 1) * span)

            @pl.when(z > 0)
            def _(group=group, cols=cols):
                chain(group).wait_recv()
                before[:, cols] = carry_in[group].astype(jnp.float32)

            @pl.when(follows)
            def _(group=group, cols=cols):
                falling = ends[0][group]
                for at in range(1, blocks):
                    falling = falling * ends[at][group]
                carry_out[group] = (before[:, cols] * falling + state[:, cols]).astype(jnp.bfloat16)
                chain(group).start()

    def chain_point(place, last=False):
        pl.when(z >= place if last else z == place)(hand_on)

    chain_point(0)
    yield
    place = z * rows
    position = (place + lax.broadcasted_iota(jnp.int32, (rows, 1), 0)).astype(jnp.float32) + 1.0
    pool_groups = pool // POOL_GROUP
    for group in range(pool_groups):
        cols = slice(group * POOL_GROUP, (group + 1) * POOL_GROUP)
        size = rows + tail
        two = pool_pad[lead:, cols] + pool_pad[lead - 1 : lead - 1 + size, cols]
        pool_two[0:lead] = jnp.zeros((lead, POOL_GROUP), jnp.float32)
        pool_two[lead:] = two
        four = two + pool_two[lead - 2 : lead - 2 + size]
        pool_four[0:lead] = jnp.zeros((lead, POOL_GROUP), jnp.float32)
        pool_four[lead:] = four
        eight = four + pool_four[lead - 4 : lead - 4 + size]
        sixteen = eight[tail:] + eight[tail - 8 : size - 8]
        sums = [two[tail:], four[tail:], eight[tail:], sixteen]
        picks = [c * pool_groups + group for c in range(cores)]
        running = chosen(core, [sums[pick] for pick in picks])
        reach = chosen(core, [jnp.float32(2 ** (pick + 1)) for pick in picks])
        share = 1.0 / jnp.minimum(position, reach)
        pooled = running * share - pool_in[0, :, cols].astype(jnp.float32)
        mixed = jnp.dot(
            pooled.astype(jnp.bfloat16),
            pool_weight[core * pool_groups + group],
            preferred_element_type=jnp.float32,
        )
        at = pl.multiple_of(core * pool + group * POOL_GROUP, POOL_GROUP)
        scale = pool_scale[:, pl.ds(at, POOL_GROUP)].astype(jnp.float32)
        out = inner + group * POOL_GROUP
        channels[:, out : out + POOL_GROUP] = (mixed * scale).astype(jnp.bfloat16)
        yield
    pool_letter().start()
    chain_point(1)
    for at in range(blocks):
        now = slice(at * BLOCK, (at + 1) * BLOCK)
        cum = cum_all[now, 0:heads]
        cum_flat = jnp.transpose(cum_all[now])
        step_flat = jnp.transpose(step_all[now])
        for group in range(groups):
            c_now = bc_conv[now, wide + group * STATE : wide + (group + 1) * STATE]
            scores = jnp.dot(
                c_now, b_turned[at * groups + group], preferred_element_type=jnp.float32
            )
            for pair in range(pairs):
                first = group * (span // HEAD_DIM) + 2 * pair
                both = []
                for head in (first, first + 1):
                    gap = cum[:, head : head + 1] - cum_flat[head : head + 1]
                    decay = jnp.exp(jnp.where(causal, gap, -1e30))
                    both.append((scores * decay * step_flat[head : head + 1]).astype(jnp.bfloat16))
                here = slice(first * HEAD_DIM, (first + 2) * HEAD_DIM)
                within[now, here] = jnp.dot(
                    jnp.concatenate(both, axis=1),
                    x_split[at, :, here],
                    preferred_element_type=jnp.float32,
                )
            yield
        if at == 0:
            chain_point(2)
    chain_point(3, True)
    yield
    falling = [None] * groups
    for at in range(blocks):
        now = slice(at * BLOCK, (at + 1) * BLOCK)
        for group in range(groups):
            cols = slice(group * span, (group + 1) * span)
            earlier = before[:, cols]
            if at:
                earlier = earlier * falling[group]
            entering = local_in[at, :, cols] + earlier
            c_now = bc_conv[now, wide + group * STATE : wide + (group + 1) * STATE]
            carried = jnp.dot(
                c_now, entering.astype(jnp.bfloat16), preferred_element_type=jnp.float32
            )
            mixed = (within[now, cols] + carried * grown[now, cols]) * silu(
                gate[0, now, cols].astype(jnp.float32)
            )
            root = lax.rsqrt(jnp.mean(mixed * mixed, axis=1, keepdims=True) + eps)
            at_gain = pl.multiple_of(core * inner + group * span, span)
            channels[now, cols] = (
                mixed * root * gain[:, pl.ds(at_gain, span)].astype(jnp.float32)
            ).astype(jnp.bfloat16)
            end = ends[at][group]
            falling[group] = end if at == 0 else falling[group] * end
        block_letter(at).start()
        yield
    letters = [pool_letter(), *(block_letter(at) for at in range(blocks))]

    def received():
        for letter in letters:
            letter.wait_recv()

    def finish():
        for letter in letters:
            letter.wait_send()

        @pl.when(follows)
        def _():
            for at in range(4):
                tails(at).wait_send()
            for group in range(groups):
                chain(group).wait_send()

    return received, finish


def whole_kernel(sp_size, fs_size, cores, tail, *refs):
    inputs, ssd_weight, pool_rows, out_gain, out = refs[:15], refs[15], refs[16], refs[17], refs[18]
    (z_sends, z_arrivals, y_sends, y_arrivals, m_sends, m_arrivals, p_sends, p_arrivals, o_sends,
     o_arrivals, local_sems, whole, parts, part_in, returned, return_in, squares, squares_in,
     *rest) = refs[19:]
    channels, far_channels = rest[-2:]
    links = Links(sp_size, fs_size)
    width = ssd_weight.shape[1]
    inner = ssd_weight.shape[0]
    rows = channels.shape[0]
    half = sp_size // cores
    core = links.core
    own_at = pl.multiple_of((links.z * 2 + links.y) * width, width)
    loads = [
        pltpu.make_async_copy(
            source, whole.at[pl.ds(begin, source.shape[0]), pl.ds(own_at, width)], local_sems.at[at]
        )
        for at, (source, begin) in enumerate(((ssd_weight, 0), (pool_rows, inner)))
    ]
    for load in loads:
        load.start()
    links.barrier()
    weights = Weights(links, whole, width, (z_sends, z_arrivals), (y_sends, y_arrivals))
    work = mixers(links, tail, cores, (*inputs, *rest), (m_sends, m_arrivals))

    def moves():
        for load in loads:
            load.wait()
        weights.begin()
        yield
        yield
        yield
        weights.turn()
        for step in range(1, sp_size):
            if step == 1:
                for _ in range(PAUSE):
                    yield
            for chunk in range(CHUNKS):
                yield
                weights.hop(step, chunk)
            yield step

    flow = moves()
    mixed = None
    hops = 0
    while mixed is None:
        try:
            next(work)
        except StopIteration as ended:
            mixed = ended.value
        else:
            hops = next(flow, None) or hops
    received, finish_mixers = mixed

    def reach(step):
        nonlocal hops
        while hops < step:
            hops = next(flow) or hops

    def multiply(turn, far):
        z = links.nearest(turn)
        source = far_channels if far else channels

        @pl.loop(0, 2)
        def _(y):
            slab = z * 2 + y
            at = pl.multiple_of(slab * width, width)
            parts[far, slab] = jnp.dot(
                source[...], whole[:, pl.ds(at, width)], preferred_element_type=jnp.float32
            ).astype(jnp.bfloat16)

            @pl.when(z // half != core)
            def _():
                part_letter(z, y, far).start()

    def part_letter(z, y, far):
        slab = z * 2 + y
        return remote(
            parts.at[far, slab],
            part_in.at[far, lax.rem(z, half) * 2 + y],
            p_sends,
            p_arrivals,
            far * 2 * sp_size + slab,
            links.sibling,
        )

    def return_letter(slot):
        return remote(
            returned.at[slot], return_in.at[slot], o_sends, o_arrivals, slot, links.beside
        )

    def give_back(turn):
        z = links.nearest(turn)

        @pl.when(z // half == core)
        def _():
            @pl.loop(0, 2)
            def _(y):
                part_letter(z, y, 1).wait_recv()
                slot = lax.rem(z, half) * 2 + y
                returned[slot] = (
                    parts[1, z * 2 + y].astype(jnp.float32) + part_in[1, slot].astype(jnp.float32)
                ).astype(jnp.bfloat16)
                return_letter(slot).start()

    weights.settle(0)
    multiply(0, 0)
    reach(1)
    weights.settle(1)
    multiply(1, 0)
    for step in range(2, sp_size):
        if step == sp_size - 1:
            received()
            for turn in range(step):
                multiply(turn, 1)
                if turn:
                    give_back(turn - 1)
            give_back(step - 1)
        reach(step)
        weights.settle(step)
        if step == sp_size - 1:
            multiply(step, 1)
            multiply(step, 0)
            give_back(step)
        else:
            multiply(step, 0)
    own_half = core * half
    slots = 2 * half

    def lane_squares(values):
        values = values * values
        total = values[:, 0:128]
        for at in range(1, width // 128):
            total = total + values[:, at * 128 : (at + 1) * 128]
        return total

    def own_total(slot):
        return parts[0, own_half * 2 + slot].astype(jnp.float32) + part_in[0, slot].astype(
            jnp.float32
        )

    squares[...] = jnp.zeros_like(squares)

    @pl.loop(0, slots)
    def _(slot):
        part_letter(own_half + slot // 2, lax.rem(slot, 2), 0).wait_recv()
        squares[...] += lane_squares(own_total(slot))

    @pl.loop(0, slots)
    def _(slot):
        return_letter(slot).wait_recv()
        squares[...] += lane_squares(return_in[slot].astype(jnp.float32))

    exchange = remote(squares, squares_in, o_sends, o_arrivals, slots, links.sibling)
    exchange.start()
    exchange.wait_recv()
    row_squares = jnp.sum(squares[...] + squares_in[...], axis=1, keepdims=True)
    root = lax.rsqrt(row_squares / out_gain.shape[1] + eps)

    @pl.loop(0, slots)
    def _(slot):
        first = (slot // 2) * fs_size + 2 * lax.rem(slot, 2)
        for values, x in (
            (own_total(slot), links.x),
            (return_in[slot].astype(jnp.float32), 1 - links.x),
        ):
            at = pl.multiple_of((first + x) * width, width)
            at_gain = pl.multiple_of(core * out.shape[2] + at, width)
            out[0, :, pl.ds(at, width)] = (
                values * root * out_gain[:, pl.ds(at_gain, width)].astype(jnp.float32)
            ).astype(jnp.bfloat16)

    exchange.wait_send()
    weights.finish()
    finish_mixers()

    @pl.loop(0, 2 * half)
    def _(slot):
        return_letter(slot).wait_send()
        other = (1 - core) * half
        for far in range(2):
            part_letter(other + slot // 2, lax.rem(slot, 2), far).wait_send()


def mixed_and_projected(inputs, ssd_weight, pool_rows, out_gain, tail):
    sp_size, fs_size, cores = lax.axis_size("sp"), lax.axis_size("fs"), lax.axis_size("tp")
    width = ssd_weight.shape[1]
    x_in, b_in, pool_in = inputs[0], inputs[2], inputs[12]
    tok_rows, inner = x_in.shape[1:]
    wide, pool = b_in.shape[2], pool_in.shape[2]
    groups = wide // STATE
    span = inner // groups
    blocks = tok_rows // BLOCK
    half = sp_size // cores
    slots = 2 * half
    vmem = pl.BlockSpec(memory_space=pltpu.VMEM)
    hbm = pl.BlockSpec(memory_space=pl.ANY)
    dma = pltpu.SemaphoreType.DMA
    half_type, full_type = jnp.bfloat16, jnp.float32
    z_spots, y_spots = CHUNKS * (sp_size - 1) * 4, CHUNKS * (2 * sp_size - 1)
    letters = 5 + groups + blocks
    return pl.pallas_call(
        functools.partial(whole_kernel, sp_size, fs_size, cores, tail),
        out_shape=jax.ShapeDtypeStruct((1, tok_rows, out_gain.shape[1] // cores), half_type),
        in_specs=[vmem] * len(inputs) + [hbm, hbm, vmem],
        out_specs=vmem,
        scratch_shapes=[
            dma((z_spots,)),
            dma((z_spots,)),
            dma((y_spots,)),
            dma((y_spots,)),
            dma((letters,)),
            dma((letters,)),
            dma((4 * sp_size,)),
            dma((4 * sp_size,)),
            dma((slots + 1,)),
            dma((slots + 1,)),
            dma((2,)),
            pltpu.VMEM((inner + pool, width * 2 * sp_size), half_type),
            pltpu.VMEM((2, 2 * sp_size, tok_rows, width), half_type),
            pltpu.VMEM((2, slots, tok_rows, width), half_type),
            pltpu.VMEM((slots, tok_rows, width), half_type),
            pltpu.VMEM((slots, tok_rows, width), half_type),
            pltpu.VMEM((tok_rows, 128), full_type),
            pltpu.VMEM((tok_rows, 128), full_type),
            pltpu.VMEM((tail, inner), half_type),
            pltpu.VMEM((tail, wide), half_type),
            pltpu.VMEM((tail, wide), half_type),
            pltpu.VMEM((tail, pool), half_type),
            pltpu.VMEM((tail + tok_rows, inner), full_type),
            pltpu.VMEM((tail + tok_rows, 2 * wide), full_type),
            pltpu.VMEM((8 + tail + tok_rows, pool), full_type),
            pltpu.VMEM((8 + tail + tok_rows, POOL_GROUP), full_type),
            pltpu.VMEM((8 + tail + tok_rows, POOL_GROUP), full_type),
            pltpu.VMEM((blocks, 2 * BLOCK, inner), half_type),
            pltpu.VMEM((tok_rows, 2 * wide), half_type),
            pltpu.VMEM((blocks * groups, STATE, BLOCK), half_type),
            pltpu.VMEM((tok_rows, 128), full_type),
            pltpu.VMEM((tok_rows, 128), full_type),
            pltpu.VMEM((tok_rows, inner), full_type),
            pltpu.VMEM((tok_rows, inner), full_type),
            pltpu.VMEM((blocks, STATE, inner), full_type),
            pltpu.VMEM((STATE, inner), full_type),
            pltpu.VMEM((STATE, inner), full_type),
            pltpu.VMEM((groups, STATE, span), half_type),
            pltpu.VMEM((groups, STATE, span), half_type),
            pltpu.VMEM((tok_rows, inner + pool), half_type),
            pltpu.VMEM((tok_rows, inner + pool), half_type),
        ],
        compiler_params=pltpu.CompilerParams(
            collective_id=0, has_side_effects=True, vmem_limit_bytes=56 * 2**20
        ),
        name="paired_mixers",
    )(*inputs, ssd_weight, pool_rows, out_gain)


def causal_taps(input_rows, prior_rows, tap_weights, offset_bias):
    padded = jnp.concatenate([prior_rows, input_rows], axis=0).astype(jnp.float32)
    tok_rows = input_rows.shape[0]
    running = jnp.zeros(input_rows.shape, jnp.float32) + offset_bias
    for tap_index in range(tap_weights.shape[0]):
        running = (
            running
            + tap_weights[tap_index].astype(jnp.float32) * padded[tap_index : tap_index + tok_rows]
        )
    return jax.nn.silu(running).astype(jnp.bfloat16)


def pool_mix(input_rows, prior_rows, positions, group_ids, local_weight, local_scale):
    tail_rows = prior_rows.shape[0]
    tok_rows = input_rows.shape[0]
    padded = jnp.concatenate([prior_rows, input_rows], axis=0).astype(jnp.float32)
    window_reach = jnp.left_shift(jnp.int32(2), group_ids)
    running = jnp.zeros(input_rows.shape, jnp.float32)
    for offset_back in range(tail_rows + 1):
        start_row = tail_rows - offset_back
        running = running + padded[start_row : start_row + tok_rows] * (
            offset_back < window_reach
        ).astype(jnp.float32)
    window_count = jnp.minimum(positions[:, None] + 1.0, window_reach.astype(jnp.float32)[None, :])
    pooled = (running / window_count - input_rows.astype(jnp.float32)).astype(jnp.bfloat16)
    grouped = pooled.reshape(tok_rows, local_weight.shape[0], local_weight.shape[1])
    mixed = jnp.einsum("lgc,gcd->lgd", grouped, local_weight, preferred_element_type=jnp.float32)
    return (mixed.reshape(input_rows.shape) * local_scale.astype(jnp.float32)).astype(jnp.bfloat16)


def join_states(earlier, later_part):
    return (
        earlier[0] + later_part[0],
        earlier[1] * jnp.exp(later_part[0])[..., None, None] + later_part[1],
    )


def body(
    statespace_input,
    output_gate_input,
    state_input_projection,
    state_output_projection,
    step_size_input,
    added_log_decay,
    logarithm_rates,
    head_channel_taps,
    input_projection_taps,
    output_projection_taps,
    input_projection_bias,
    group_norm_gain,
    pooling_input,
    pooling_group_weight,
    pooling_channel_scale,
    statespace_output_weight,
    pooling_output_weight,
    output_norm_gain,
):
    core_count = lax.axis_size("tp")
    sp_size, fs_size = lax.axis_size("sp"), lax.axis_size("fs")
    pool_tail = 2**POOL_GROUPS - 1
    paired = (
        statespace_output_weight.shape[1] % 128 == 0
        and fs_size == 4
        and core_count == 2
        and sp_size in (4, 8)
    )
    if paired:
        return mixed_and_projected(
            (
                statespace_input,
                output_gate_input,
                state_input_projection,
                state_output_projection,
                step_size_input,
                added_log_decay,
                logarithm_rates[None],
                head_channel_taps,
                input_projection_taps,
                output_projection_taps,
                input_projection_bias[None],
                group_norm_gain[None],
                pooling_input,
                pooling_group_weight,
                pooling_channel_scale[None],
            ),
            statespace_output_weight,
            pooling_output_weight,
            output_norm_gain[None],
            pool_tail + 1,
        )
    core_index = lax.axis_index("tp")
    seq_index = lax.axis_index("sp")
    head_channel_rows = statespace_input[0]
    output_gate_rows = output_gate_input[0]
    input_projection_rows = state_input_projection[0]
    output_projection_rows = state_output_projection[0]
    step_size_rows = step_size_input[0]
    decay_spikes = added_log_decay[0]
    pooling_rows = pooling_input[0]
    tok_rows = head_channel_rows.shape[0]
    inner_local = head_channel_rows.shape[1]
    heads_local = step_size_rows.shape[1]
    state_local = input_projection_rows.shape[1]
    pool_local = pooling_rows.shape[1]
    groups_local = state_local // STATE
    per_group = heads_local // groups_local
    groups_pool = pool_local // POOL_GROUP
    conv_tail = CONV - 1
    own_columns = jnp.concatenate([statespace_output_weight, pooling_output_weight], axis=0)
    tails = jnp.concatenate(
        [
            jnp.pad(rows[tok_rows - tail :], ((pool_tail - tail, 0), (0, 0)))
            for rows, tail in (
                (head_channel_rows, conv_tail),
                (input_projection_rows, conv_tail),
                (output_projection_rows, conv_tail),
                (pooling_rows, pool_tail),
            )
        ],
        axis=1,
    )
    prior = passed_along(tails, "sp", 1)
    widths = (inner_local, state_local, state_local, pool_local)
    prior_x, prior_b, prior_c, prior_pool = (
        prior[pool_tail - tail :, sum(widths[:at]) : sum(widths[: at + 1])]
        for at, tail in enumerate((conv_tail, conv_tail, conv_tail, pool_tail))
    )
    taps_x = lax.dynamic_slice_in_dim(head_channel_taps, core_index * inner_local, inner_local, 1)
    taps_b = lax.dynamic_slice_in_dim(
        input_projection_taps, core_index * state_local, state_local, 1
    )
    taps_c = lax.dynamic_slice_in_dim(
        output_projection_taps, core_index * state_local, state_local, 1
    )
    bias_b = lax.dynamic_slice_in_dim(
        input_projection_bias, core_index * state_local, state_local, 0
    )
    gain_ssd = lax.dynamic_slice_in_dim(group_norm_gain, core_index * inner_local, inner_local, 0)
    head_decay_rates = jnp.exp(
        lax.dynamic_slice_in_dim(logarithm_rates, core_index * heads_local, heads_local, 0)
    )
    gain_pool = lax.dynamic_slice_in_dim(
        pooling_channel_scale, core_index * pool_local, pool_local, 0
    )
    weight_pool = lax.dynamic_slice_in_dim(
        pooling_group_weight, core_index * groups_pool, groups_pool, 0
    )
    whole_columns = lax.all_gather(own_columns, ("sp", "fs"), axis=1, tiled=True)
    x_conv = causal_taps(head_channel_rows, prior_x, taps_x, 0.0)
    b_conv = causal_taps(input_projection_rows, prior_b, taps_b, bias_b.astype(jnp.float32))
    c_conv = causal_taps(output_projection_rows, prior_c, taps_c, 0.0)
    blocks = tok_rows // BLOCK
    discrete_step_size = jax.nn.softplus(step_size_rows.astype(jnp.float32))
    logarithm_decay = -discrete_step_size * head_decay_rates + decay_spikes
    cumulative_decay = jnp.cumsum(
        logarithm_decay.reshape(blocks, BLOCK, groups_local, per_group), axis=1
    )
    cum_t = cumulative_decay.transpose(0, 2, 3, 1)
    step_t = discrete_step_size.reshape(blocks, BLOCK, groups_local, per_group).transpose(
        0, 2, 3, 1
    )
    heads_x = x_conv.reshape(blocks, BLOCK, groups_local, per_group, HEAD_DIM)
    group_b = b_conv.reshape(blocks, BLOCK, groups_local, STATE)
    group_c = c_conv.reshape(blocks, BLOCK, groups_local, STATE)
    scores = jnp.einsum("ktgn,kugn->kgtu", group_c, group_b, preferred_element_type=jnp.float32)
    causal = jnp.arange(BLOCK)[:, None] >= jnp.arange(BLOCK)[None, :]
    decay_gap = cum_t[..., :, None] - cum_t[..., None, :]
    decay_factor = jnp.where(causal, jnp.exp(jnp.where(causal, decay_gap, 0.0)), 0.0)
    weights = (scores[:, :, None] * decay_factor * step_t[..., None, :]).astype(jnp.bfloat16)
    within = jnp.einsum("kgetu,kugep->ktgep", weights, heads_x, preferred_element_type=jnp.float32)
    block_end = cum_t[..., -1]
    end_weight = jnp.exp(block_end[..., None] - cum_t) * step_t
    scaled_x = (heads_x * end_weight.transpose(0, 3, 1, 2)[..., None]).astype(jnp.bfloat16)
    block_state = jnp.einsum(
        "kugep,kugn->kgepn", scaled_x, group_b, preferred_element_type=jnp.float32
    )

    def local_chain(state_now, current_inputs):
        piece_state, piece_fall = current_inputs
        return (state_now * jnp.exp(piece_fall)[..., None, None] + piece_state, state_now)

    final_state, local_entering = lax.scan(
        local_chain, jnp.zeros(block_state.shape[1:], jnp.float32), (block_state, block_end)
    )
    log_total = jnp.sum(block_end, axis=0)
    prefix_log = jnp.cumsum(block_end, axis=0) - block_end
    log_before, state_before = entering_2(
        (log_total, final_state),
        "sp",
        join_states,
        (jnp.zeros_like(log_total), jnp.zeros_like(final_state)),
    )
    entering = (local_entering + jnp.exp(prefix_log)[..., None, None] * state_before[None]).astype(
        jnp.bfloat16
    )
    carried_out = jnp.einsum(
        "ktgn,kgepn->ktgep", group_c, entering, preferred_element_type=jnp.float32
    )
    carried_out = carried_out * jnp.exp(cumulative_decay)[..., None]
    mixed_ssd = (within + carried_out).reshape(tok_rows, inner_local) * jax.nn.silu(
        output_gate_rows.astype(jnp.float32)
    )
    grouped = mixed_ssd.reshape(tok_rows, groups_local, inner_local // groups_local)
    normed = grouped * lax.rsqrt(jnp.mean(grouped * grouped, axis=-1, keepdims=True) + eps)
    ssd_out = (normed.reshape(tok_rows, inner_local) * gain_ssd.astype(jnp.float32)).astype(
        jnp.bfloat16
    )
    positions = (seq_index * tok_rows + jnp.arange(tok_rows, dtype=jnp.int32)).astype(jnp.float32)
    group_ids = core_index * groups_pool + jnp.arange(pool_local, dtype=jnp.int32) // POOL_GROUP
    pool_out = pool_mix(pooling_rows, prior_pool, positions, group_ids, weight_pool, gain_pool)
    channels = jnp.concatenate([ssd_out, pool_out], axis=1)
    half_width = D // core_count
    gain_out = lax.dynamic_slice_in_dim(
        output_norm_gain, core_index * half_width, half_width, 0
    ).astype(jnp.float32)
    partial = jnp.dot(channels, whole_columns, preferred_element_type=jnp.float32).astype(
        jnp.bfloat16
    )
    own_half = lax.dynamic_slice_in_dim(partial, core_index * half_width, half_width, 1).astype(
        jnp.float32
    )
    for hop in range(1, core_count):
        target = lax.rem(core_index + hop, core_count)
        leaving = lax.dynamic_slice_in_dim(partial, target * half_width, half_width, 1)
        route = [(i, (i + hop) % core_count) for i in range(core_count)]
        own_half = own_half + lax.ppermute(leaving, "tp", route).astype(jnp.float32)
    row_squares = lax.psum(jnp.sum(own_half * own_half, axis=1), "tp")
    result = own_half * lax.rsqrt(row_squares / D + eps)[:, None] * gain_out
    return result.astype(jnp.bfloat16)[None]


def solution(mesh):
    in_specs = (
        P("fs", "sp", "tp"),
        P("fs", "sp", "tp"),
        P("fs", "sp", "tp"),
        P("fs", "sp", "tp"),
        P("fs", "sp", "tp"),
        P("fs", "sp", "tp"),
        P(),
        P(),
        P(),
        P(),
        P(),
        P(),
        P("fs", "sp", "tp"),
        P(),
        P(),
        P("tp", ("sp", "fs")),
        P("tp", ("sp", "fs")),
        P(),
    )
    out_specs = P("fs", "sp", "tp")
    return jax.shard_map(body, mesh=mesh, in_specs=in_specs, out_specs=out_specs, check_vma=False)
```

```python
import functools

import jax
import jax.numpy as jnp
from jax import lax
from jax.experimental import pallas as pl
from jax.experimental.pallas import tpu as pltpu
from jax.sharding import PartitionSpec as P

D = 4096
HEAD_DIM = 64
STATE = 128
CONV = 4
BLOCK = 128
POOL_GROUPS = 4
POOL_GROUP = 256


eps = 1e-06


def passed_along(block, axis, distance):
    devices = range(lax.axis_size(axis))
    route = [(i - distance, i) for i in devices if i - distance in devices]
    return lax.ppermute(block, axis, route)


def entering_2(array, axis, join, neutral):
    place = lax.axis_index(axis)
    gathered = jax.tree.map(
        lambda a, kind: lax.all_gather(a.astype(kind), axis), array, (jnp.bfloat16, jnp.bfloat16)
    )
    state = jax.tree.map(lambda a, e: jnp.zeros_like(a) + jnp.asarray(e, a.dtype), array, neutral)

    def one(lap, state):
        return join(
            state,
            jax.tree.map(
                lambda a, own: lax.dynamic_index_in_dim(a, lap, 0, False).astype(own.dtype),
                gathered,
                array,
            ),
        )

    return lax.fori_loop(0, place, one, state)


MESH_IDS = pl.DeviceIdType.MESH
EXACT = lax.Precision.HIGHEST
CHUNKS = 6
INPUTS, GATE, VECTORS = 13, 1, 10
SOURCES, OTHERS = (0, 2, 3, 11), (4, 5, 6, 7, 8, 9, 10, 12)
ORDER = (*SOURCES, *OTHERS, GATE)


class Links:
    def __init__(self, sp_size, fs_size):
        self.n = sp_size
        self.z = lax.axis_index("sp")
        self.fs = lax.axis_index("fs")
        self.core = lax.axis_index("tp")
        self.x = lax.rem(self.fs, 2)
        self.y = self.fs // 2
        self.beside = {"fs": self.fs + 1 - 2 * self.x}
        self.across = {"fs": self.fs + 2 - 4 * self.y}
        self.sibling = {"tp": 1 - self.core}

    def barrier(self):
        barrier = pltpu.get_barrier_semaphore()
        near = [{"sp": lax.rem(self.z + far, self.n)} for far in (1, self.n - 1)]
        for other in (*near, self.beside, self.across, self.sibling):
            pl.semaphore_signal(barrier, inc=1, device_id=other, device_id_type=MESH_IDS)
        pl.semaphore_wait(barrier, len(near) + 3)

    def within(self, place):
        return jnp.logical_and(place >= 0, place < self.n)

    def nearest(self, turn):
        if turn == 0:
            return self.z
        low, high = self.z, self.n - 1 - self.z
        small = jnp.minimum(low, high)
        both = turn <= 2 * small
        far = jnp.where(both, (turn + 1) // 2, turn - small)
        sign = jnp.where(both, 1 - 2 * (turn % 2), jnp.where(high > low, 1, -1))
        return self.z + sign * far


def remote(src, dst, sends, arrivals, spot, device):
    return pltpu.make_async_remote_copy(
        src_ref=src,
        dst_ref=dst,
        send_sem=sends.at[spot],
        recv_sem=arrivals.at[spot],
        device_id=device,
        device_id_type=MESH_IDS,
    )


class Weights:
    def __init__(self, links, whole, width, z_sems, y_sems):
        self.links, self.whole, self.width = links, whole, width
        self.z_sems, self.y_sems = z_sems, y_sems
        self.rows = whole.shape[0] // CHUNKS
        self.direct = range(CHUNKS - 1)
        self.turned = (CHUNKS - 1,)
        self.sent = {}

    def region(self, chunk, z, y):
        at = pl.multiple_of((z * 2 + y) * self.width, self.width)
        return self.whole.at[pl.ds(chunk * self.rows, self.rows), pl.ds(at, self.width)]

    def along(self, chunk, step, way, side, arriving):
        links = self.links
        origin = links.z - way * (step if arriving else step - 1)
        y = links.y if side == 0 else 1 - links.y
        spot = ((chunk * (links.n - 1) + step - 1) * 2 + (way < 0)) * 2 + side
        place = self.region(chunk, jnp.clip(origin, 0, links.n - 1), y)
        copy = remote(place, place, *self.z_sems, spot, {"sp": links.z + way})
        far = links.z if arriving else links.z + way
        return copy, jnp.logical_and(links.within(origin), links.within(far))

    def over(self, chunk, offset, arriving):
        links = self.links
        y = 1 - links.y if arriving else links.y
        origin = links.z + offset
        place = self.region(chunk, jnp.clip(origin, 0, links.n - 1), y)
        spot = chunk * (2 * links.n - 1) + offset + links.n - 1
        copy = remote(place, place, *self.y_sems, spot, links.across)
        return copy, links.within(origin)

    def go(self, kind, *key):
        copy, here = kind(*key, False)
        self.sent[kind.__name__, key] = kind
        pl.when(here)(copy.start)

    def take(self, kind, *key):
        copy, here = kind(*key, True)
        pl.when(here)(copy.wait_recv)

    def pass_on(self, chunk, step, way, side):
        if step < self.links.n:
            self.go(self.along, chunk, step, way, side)

    def begin(self):
        for chunk in (*self.turned, *self.direct):
            self.go(self.over, chunk, 0)

    def own(self, chunks, side=0):
        for chunk in chunks:
            for way in (1, -1):
                self.pass_on(chunk, 1, way, side)

    def turn(self):
        for chunk in self.turned:
            self.take(self.over, chunk, 0)
        for side in (0, 1):
            self.own(self.turned, side)

    def hop(self, step, chunks):
        for chunk in chunks:
            for way in (1, -1):
                for side in (0, 1) if chunk in self.turned else (0,):
                    self.take(self.along, chunk, step, way, side)
                    self.pass_on(chunk, step + 1, way, side)
                if chunk in self.direct:
                    self.go(self.over, chunk, -way * step)

    def settle(self, step):
        for chunk in self.direct:
            for offset in (0,) if step == 0 else (step, -step):
                self.take(self.over, chunk, offset)

    def finish(self):
        for (_, key), kind in self.sent.items():
            copy, here = kind(*key, False)
            pl.when(here)(copy.wait_send)


def silu(rows):
    return rows / (1.0 + jnp.exp(-rows))


def softplus(rows):
    return jnp.maximum(rows, 0.0) + jnp.log(1.0 + jnp.exp(-jnp.abs(rows)))


def chosen(core, options):
    best = options[0]
    for at in range(1, len(options)):
        best = jnp.where(core == at, options[at], best)
    return best


def mixers(links, tail, cores, pieces, fetches, refs, sems):
    (x_in, gate, b_in, c_in, dt, added, rates, x_taps, b_taps, c_taps, vectors, pool_in,
     pool_weight, prior_x, prior_b, prior_c, prior_pool, x_pad, bc_pad, pool_pad,
     pool_two, pool_four, x_split, bc_conv, b_turned, flat, upright, within, grown, local_in,
     state, before, carry_in, carry_out, channels, far_channels) = refs
    sends, arrivals = sems
    rows, inner = x_in.shape[1:]
    heads = dt.shape[1]
    wide = b_in.shape[2]
    pool = pool_in.shape[2]
    groups = wide // STATE
    span = inner // groups
    blocks = rows // BLOCK
    z, core = links.z, links.core
    lead = 8
    sources = ((x_in, prior_x), (b_in, prior_b), (c_in, prior_c), (pool_in, prior_pool))

    def tails(at):
        source, target = sources[at]
        return remote(
            source.at[0, pl.ds(rows - tail, tail)], target, sends, arrivals, at, {"sp": z + 1}
        )

    def chain(group):
        return remote(
            carry_out.at[group], carry_in.at[group], sends, arrivals, 4 + group, {"sp": z + 1}
        )

    def pool_letter():
        cols = pl.ds(inner, pool)
        return remote(
            channels.at[:, cols], far_channels.at[:, cols], sends, arrivals, 4 + groups, links.beside
        )

    def block_letter(at):
        place = (pl.ds(at * BLOCK, BLOCK), pl.ds(0, inner))
        return remote(
            channels.at[place], far_channels.at[place], sends, arrivals, 5 + groups + at, links.beside
        )

    follows = z + 1 < links.n
    for at in SOURCES:
        fetches[at].wait()

    @pl.when(follows)
    def _():
        for at in range(4):
            tails(at).start()

    yield "start"
    for at in OTHERS:
        fetches[at].wait()
    x_pad[tail:] = x_in[0].astype(jnp.float32)
    bc_pad[tail:, 0:wide] = b_in[0].astype(jnp.float32)
    bc_pad[tail:, wide:] = c_in[0].astype(jnp.float32)
    pool_pad[0:lead] = jnp.zeros((lead, pool), jnp.float32)
    pool_pad[lead + tail :] = pool_in[0].astype(jnp.float32)
    steps_flat = softplus(dt[0].astype(jnp.float32))
    own_rates = rates[pl.ds(pl.multiple_of(core * heads, heads), heads)]
    logs_flat = -steps_flat * jnp.exp(own_rates) + added[0]
    flat[...] = jnp.zeros_like(flat)
    down = lax.broadcasted_iota(jnp.int32, (BLOCK, BLOCK), 0)
    over = lax.broadcasted_iota(jnp.int32, (BLOCK, BLOCK), 1)
    causal = down >= over
    upper = (down <= over).astype(jnp.float32)
    first_half = lax.broadcasted_iota(jnp.int32, (BLOCK, 2 * HEAD_DIM), 1) < HEAD_DIM

    def mine(ref, size):
        at = pl.multiple_of(core * size, size)
        return ref[:, pl.ds(at, size)].astype(jnp.float32)

    taps_x = mine(x_taps, inner)
    taps_bc = jnp.concatenate([mine(b_taps, wide), mine(c_taps, wide)], axis=1)
    bias_b = pieces(vectors, "bias", core * wide, wide)
    bias_bc = jnp.concatenate([bias_b, jnp.zeros_like(bias_b)], axis=1)

    @pl.when(z == 0)
    def _():
        x_pad[0:tail] = jnp.zeros((tail, inner), jnp.float32)
        bc_pad[0:tail] = jnp.zeros((tail, 2 * wide), jnp.float32)
        pool_pad[lead : lead + tail] = jnp.zeros((tail, pool), jnp.float32)

    @pl.when(z > 0)
    def _():
        for at in range(4):
            tails(at).wait_recv()
        x_pad[0:tail] = prior_x[...].astype(jnp.float32)
        bc_pad[0:tail, 0:wide] = prior_b[...].astype(jnp.float32)
        bc_pad[0:tail, wide:] = prior_c[...].astype(jnp.float32)
        pool_pad[lead : lead + tail] = prior_pool[...].astype(jnp.float32)

    def taps(pad, weights, at, cols):
        total = None
        for tap in range(CONV):
            begin = at * BLOCK + tail - CONV + 1 + tap
            term = pad[begin : begin + BLOCK, cols] * weights[tap : tap + 1, cols]
            total = term if total is None else total + term
        return total

    def spread(narrow, head):
        shape = (BLOCK, 2 * HEAD_DIM)
        return jnp.where(
            first_half,
            jnp.broadcast_to(narrow[:, head : head + 1], shape),
            jnp.broadcast_to(narrow[:, head + 1 : head + 2], shape),
        )

    place = z * rows
    position = (place + lax.broadcasted_iota(jnp.int32, (rows, 1), 0)).astype(jnp.float32) + 1.0
    pool_groups = pool // POOL_GROUP
    for group in range(pool_groups):
        cols = slice(group * POOL_GROUP, (group + 1) * POOL_GROUP)
        size = rows + tail
        two = pool_pad[lead:, cols] + pool_pad[lead - 1 : lead - 1 + size, cols]
        pool_two[0:lead] = jnp.zeros((lead, POOL_GROUP), jnp.float32)
        pool_two[lead:] = two
        four = two + pool_two[lead - 2 : lead - 2 + size]
        pool_four[0:lead] = jnp.zeros((lead, POOL_GROUP), jnp.float32)
        pool_four[lead:] = four
        eight = four + pool_four[lead - 4 : lead - 4 + size]
        sixteen = eight[tail:] + eight[tail - 8 : size - 8]
        sums = [two[tail:], four[tail:], eight[tail:], sixteen]
        picks = [c * pool_groups + group for c in range(cores)]
        running = chosen(core, [sums[pick] for pick in picks])
        reach = chosen(core, [jnp.float32(2 ** (pick + 1)) for pick in picks])
        share = 1.0 / jnp.minimum(position, reach)
        pooled = running * share - pool_in[0, :, cols].astype(jnp.float32)
        mixed = jnp.dot(
            pooled.astype(jnp.bfloat16),
            pool_weight[core * pool_groups + group],
            preferred_element_type=jnp.float32,
        )
        scale = pieces(vectors, "scale", core * pool + group * POOL_GROUP, POOL_GROUP)
        out = inner + group * POOL_GROUP
        channels[:, out : out + POOL_GROUP] = (mixed * scale).astype(jnp.bfloat16)
    pool_letter().start()
    pairs = span // (2 * HEAD_DIM)
    ends = []
    state[...] = jnp.zeros_like(state)
    for at in range(blocks):
        now = slice(at * BLOCK, (at + 1) * BLOCK)
        bc_conv[now] = silu(taps(bc_pad, taps_bc, at, slice(0, 2 * wide)) + bias_bc).astype(
            jnp.bfloat16
        )
        flat[at, 0:heads] = jnp.dot(
            logs_flat[:, now], upper, precision=EXACT, preferred_element_type=jnp.float32
        )
        flat[at, heads : 2 * heads] = steps_flat[:, now]
        upright[at] = jnp.transpose(flat[at])
        cum = upright[at, :, 0:heads]
        decayed = jnp.exp(cum)
        closing = jnp.exp(cum[BLOCK - 1 : BLOCK] - cum) * upright[at, :, heads : 2 * heads]
        ended = []
        for group in range(groups):
            cols = slice(group * span, (group + 1) * span)
            x_now = silu(taps(x_pad, taps_x, at, cols))
            b_now = bc_conv[now, group * STATE : (group + 1) * STATE]
            b_flat = jnp.transpose(b_now.astype(jnp.float32)).astype(jnp.bfloat16)
            b_turned[at * groups + group] = b_flat
            scaled = []
            for pair in range(pairs):
                head = group * (span // HEAD_DIM) + 2 * pair
                lanes = slice(pair * 2 * HEAD_DIM, (pair + 1) * 2 * HEAD_DIM)
                here = slice(head * HEAD_DIM, (head + 2) * HEAD_DIM)
                x_pair = x_now[:, lanes]
                x_split[at, 0:BLOCK, here] = jnp.where(first_half, x_pair, 0.0).astype(jnp.bfloat16)
                x_split[at, BLOCK : 2 * BLOCK, here] = jnp.where(first_half, 0.0, x_pair).astype(
                    jnp.bfloat16
                )
                x_half = x_pair.astype(jnp.bfloat16).astype(jnp.float32)
                scaled.append((x_half * spread(closing, head)).astype(jnp.bfloat16))
                grown[now, here] = spread(decayed, head)
            end = grown[(at + 1) * BLOCK - 1 : (at + 1) * BLOCK, cols]
            ended.append(end)
            local_in[at, :, cols] = state[:, cols]
            state[:, cols] = state[:, cols] * end + jnp.dot(
                b_flat, jnp.concatenate(scaled, axis=1), preferred_element_type=jnp.float32
            )
        yield at
        ends.append(ended)

    def hand_on():
        @pl.when(z == 0)
        def _():
            before[...] = jnp.zeros_like(before)

        for group in range(groups):
            cols = slice(group * span, (group + 1) * span)

            @pl.when(z > 0)
            def _(group=group, cols=cols):
                chain(group).wait_recv()
                before[:, cols] = carry_in[group].astype(jnp.float32)

            @pl.when(follows)
            def _(group=group, cols=cols):
                falling = ends[0][group]
                for at in range(1, blocks):
                    falling = falling * ends[at][group]
                carry_out[group] = (before[:, cols] * falling + state[:, cols]).astype(jnp.bfloat16)
                chain(group).start()

    def chain_point(place, last=False):
        pl.when(z >= place if last else z == place)(hand_on)

    chain_point(0)
    yield "states"
    for at in range(blocks):
        now = slice(at * BLOCK, (at + 1) * BLOCK)
        cum = upright[at, :, 0:heads]
        cum_flat = flat[at, 0:heads]
        step_flat = flat[at, heads : 2 * heads]
        for group in range(groups):
            c_now = bc_conv[now, wide + group * STATE : wide + (group + 1) * STATE]
            scores = jnp.dot(
                c_now, b_turned[at * groups + group], preferred_element_type=jnp.float32
            )
            for pair in range(pairs):
                first = group * (span // HEAD_DIM) + 2 * pair
                both = []
                for head in (first, first + 1):
                    gap = cum[:, head : head + 1] - cum_flat[head : head + 1]
                    decay = jnp.exp(jnp.where(causal, gap, -1e30))
                    both.append((scores * decay * step_flat[head : head + 1]).astype(jnp.bfloat16))
                here = slice(first * HEAD_DIM, (first + 2) * HEAD_DIM)
                within[now, here] = jnp.dot(
                    jnp.concatenate(both, axis=1),
                    x_split[at, :, here],
                    preferred_element_type=jnp.float32,
                )
    chain_point(1)
    yield "second"
    chain_point(2)
    yield "third"
    chain_point(3, True)
    falling = [None] * groups
    fetches[GATE].wait()
    for at in range(blocks):
        now = slice(at * BLOCK, (at + 1) * BLOCK)
        for group in range(groups):
            cols = slice(group * span, (group + 1) * span)
            earlier = before[:, cols]
            if at:
                earlier = earlier * falling[group]
            entering = local_in[at, :, cols] + earlier
            c_now = bc_conv[now, wide + group * STATE : wide + (group + 1) * STATE]
            carried = jnp.dot(
                c_now, entering.astype(jnp.bfloat16), preferred_element_type=jnp.float32
            )
            mixed = (within[now, cols] + carried * grown[now, cols]) * silu(
                gate[0, now, cols].astype(jnp.float32)
            )
            root = lax.rsqrt(jnp.mean(mixed * mixed, axis=1, keepdims=True) + eps)
            gain = pieces(vectors, "gain", core * inner + group * span, span)
            channels[now, cols] = (mixed * root * gain).astype(jnp.bfloat16)
            end = ends[at][group]
            falling[group] = end if at == 0 else falling[group] * end
        block_letter(at).start()
    letters = [pool_letter(), *(block_letter(at) for at in range(blocks))]

    def received():
        for letter in letters:
            letter.wait_recv()

    def finish():
        for letter in letters:
            letter.wait_send()

        @pl.when(follows)
        def _():
            for at in range(4):
                tails(at).wait_send()
            for group in range(groups):
                chain(group).wait_send()

    return received, finish


def whole_kernel(sp_size, fs_size, cores, tail, pieces, *refs):
    inputs, ssd_weight, pool_rows, out = refs[:INPUTS], *refs[INPUTS : INPUTS + 3]
    (z_sends, z_arrivals, y_sends, y_arrivals, m_sends, m_arrivals, p_sends, p_arrivals, o_sends,
     o_arrivals, local_sems, whole, parts, part_in, returned, return_in, squares, squares_in,
     *rest) = refs[INPUTS + 3 :]
    held, rest = rest[:INPUTS], rest[INPUTS:]
    vectors = held[VECTORS]
    channels, far_channels = rest[-2:]
    links = Links(sp_size, fs_size)
    width = ssd_weight.shape[1]
    inner = ssd_weight.shape[0]
    rows = channels.shape[0]
    half = sp_size // cores
    core = links.core
    own_at = pl.multiple_of((links.z * 2 + links.y) * width, width)
    loads = [
        pltpu.make_async_copy(
            source, whole.at[pl.ds(begin, source.shape[0]), pl.ds(own_at, width)], local_sems.at[at]
        )
        for at, (source, begin) in enumerate(((ssd_weight, 0), (pool_rows, inner)))
    ]
    fetches = [
        pltpu.make_async_copy(source, place, local_sems.at[2 + at])
        for at, (source, place) in enumerate(zip(inputs, held))
    ]
    for at in ORDER:
        fetches[at].start()
    for load in loads:
        load.start()
    links.barrier()
    weights = Weights(links, whole, width, (z_sends, z_arrivals), (y_sends, y_arrivals))
    work = mixers(links, tail, cores, pieces, fetches, (*held, *rest), (m_sends, m_arrivals))

    direct, turned = weights.direct, weights.turned
    late = links.z >= sp_size // 2
    mixed = None
    while mixed is None:
        try:
            mark = next(work)
        except StopIteration as ended:
            mixed = ended.value
            break
        if mark == "start":
            for load in loads:
                load.wait()
            weights.begin()
            weights.own(direct[:3])
        elif mark == 1:
            weights.own(direct[3:4])
        elif mark == "states":
            weights.own(direct[4:])
            weights.hop(1, direct[:1])
        elif mark == "second":
            pl.when(late)(lambda: weights.hop(1, direct[1:3]))
        elif mark == "third":
            pl.when(late)(lambda: weights.hop(1, direct[3:]))
    received, finish_mixers = mixed
    pl.when(jnp.logical_not(late))(lambda: weights.hop(1, direct[1:]))

    def multiply(turn, far):
        z = links.nearest(turn)
        source = far_channels if far else channels

        @pl.loop(0, 2)
        def _(y):
            slab = z * 2 + y
            at = pl.multiple_of(slab * width, width)
            parts[far, slab] = jnp.dot(
                source[...], whole[:, pl.ds(at, width)], preferred_element_type=jnp.float32
            ).astype(jnp.bfloat16)

            @pl.when(z // half != core)
            def _():
                part_letter(z, y, far).start()

    def part_letter(z, y, far):
        slab = z * 2 + y
        return remote(
            parts.at[far, slab],
            part_in.at[far, lax.rem(z, half) * 2 + y],
            p_sends,
            p_arrivals,
            far * 2 * sp_size + slab,
            links.sibling,
        )

    def return_letter(slot):
        return remote(
            returned.at[slot], return_in.at[slot], o_sends, o_arrivals, slot, links.beside
        )

    def give_back(turn):
        z = links.nearest(turn)

        @pl.when(z // half == core)
        def _():
            @pl.loop(0, 2)
            def _(y):
                part_letter(z, y, 1).wait_recv()
                slot = lax.rem(z, half) * 2 + y
                returned[slot] = (
                    parts[1, z * 2 + y].astype(jnp.float32) + part_in[1, slot].astype(jnp.float32)
                ).astype(jnp.bfloat16)
                return_letter(slot).start()

    last = sp_size - 1
    weights.turn()
    weights.settle(0)
    multiply(0, 0)
    for step in range(2, sp_size):
        weights.hop(step, direct)
        if step < last:
            weights.hop(step - 1, turned)
            weights.settle(step - 1)
            multiply(step - 1, 0)
    received()
    for turn in range(last - 1):
        multiply(turn, 1)
        if turn:
            give_back(turn - 1)
    weights.hop(last - 1, turned)
    weights.settle(last - 1)
    multiply(last - 1, 1)
    give_back(last - 2)
    multiply(last - 1, 0)
    give_back(last - 1)
    weights.hop(last, turned)
    weights.settle(last)
    multiply(last, 1)
    multiply(last, 0)
    give_back(last)
    own_half = core * half
    slots = 2 * half

    def lane_squares(values):
        values = values * values
        total = values[:, 0:128]
        for at in range(1, width // 128):
            total = total + values[:, at * 128 : (at + 1) * 128]
        return total

    def own_total(slot):
        return parts[0, own_half * 2 + slot].astype(jnp.float32) + part_in[0, slot].astype(
            jnp.float32
        )

    squares[...] = jnp.zeros_like(squares)

    @pl.loop(0, slots)
    def _(slot):
        part_letter(own_half + slot // 2, lax.rem(slot, 2), 0).wait_recv()
        squares[...] += lane_squares(own_total(slot))

    @pl.loop(0, slots)
    def _(slot):
        return_letter(slot).wait_recv()
        squares[...] += lane_squares(return_in[slot].astype(jnp.float32))

    exchange = remote(squares, squares_in, o_sends, o_arrivals, slots, links.sibling)
    exchange.start()
    exchange.wait_recv()
    row_squares = jnp.sum(squares[...] + squares_in[...], axis=1, keepdims=True)
    features = cores * out.shape[2]
    root = lax.rsqrt(row_squares / features + eps)

    @pl.loop(0, slots)
    def _(slot):
        first = (slot // 2) * fs_size + 2 * lax.rem(slot, 2)
        for values, x in (
            (own_total(slot), links.x),
            (return_in[slot].astype(jnp.float32), 1 - links.x),
        ):
            at = pl.multiple_of((first + x) * width, width)
            gain = pieces(vectors, "out", core * out.shape[2] + at, width)
            out[0, :, pl.ds(at, width)] = (values * root * gain).astype(jnp.bfloat16)

    exchange.wait_send()
    weights.finish()
    finish_mixers()

    @pl.loop(0, 2 * half)
    def _(slot):
        return_letter(slot).wait_send()
        other = (1 - core) * half
        for far in range(2):
            part_letter(other + slot // 2, lax.rem(slot, 2), far).wait_send()


def mixed_and_projected(inputs, vectors, ssd_weight, pool_rows, tail):
    sp_size, fs_size, cores = lax.axis_size("sp"), lax.axis_size("fs"), lax.axis_size("tp")
    width = ssd_weight.shape[1]
    x_in, b_in, pool_in = inputs[0], inputs[2], inputs[10]
    starts, features = {}, vectors["out"].shape[0]
    for name, vector in vectors.items():
        starts[name] = sum(vectors[other].shape[0] for other in starts)

    def pieces(ref, name, offset, size):
        at = pl.multiple_of(starts[name] + offset, 128)
        return ref[:, pl.ds(at, size)].astype(jnp.float32)

    joined = jnp.concatenate(list(vectors.values()))[None]
    inputs = (*inputs[:10], joined, *inputs[10:])
    tok_rows, inner = x_in.shape[1:]
    wide, pool = b_in.shape[2], pool_in.shape[2]
    groups = wide // STATE
    span = inner // groups
    blocks = tok_rows // BLOCK
    half = sp_size // cores
    slots = 2 * half
    vmem = pl.BlockSpec(memory_space=pltpu.VMEM)
    hbm = pl.BlockSpec(memory_space=pltpu.HBM)
    dma = pltpu.SemaphoreType.DMA
    half_type, full_type = jnp.bfloat16, jnp.float32
    z_spots, y_spots = CHUNKS * (sp_size - 1) * 4, CHUNKS * (2 * sp_size - 1)
    letters = 5 + groups + blocks
    return pl.pallas_call(
        functools.partial(whole_kernel, sp_size, fs_size, cores, tail, pieces),
        out_shape=jax.ShapeDtypeStruct((1, tok_rows, features // cores), half_type),
        in_specs=[hbm] * (len(inputs) + 2),
        out_specs=vmem,
        scratch_shapes=[
            dma((z_spots,)),
            dma((z_spots,)),
            dma((y_spots,)),
            dma((y_spots,)),
            dma((letters,)),
            dma((letters,)),
            dma((4 * sp_size,)),
            dma((4 * sp_size,)),
            dma((slots + 1,)),
            dma((slots + 1,)),
            dma((2 + len(inputs),)),
            pltpu.VMEM((inner + pool, width * 2 * sp_size), half_type),
            pltpu.VMEM((2, 2 * sp_size, tok_rows, width), half_type),
            pltpu.VMEM((2, slots, tok_rows, width), half_type),
            pltpu.VMEM((slots, tok_rows, width), half_type),
            pltpu.VMEM((slots, tok_rows, width), half_type),
            pltpu.VMEM((tok_rows, 128), full_type),
            pltpu.VMEM((tok_rows, 128), full_type),
            *(pltpu.VMEM(array.shape, array.dtype) for array in inputs),
            pltpu.VMEM((tail, inner), half_type),
            pltpu.VMEM((tail, wide), half_type),
            pltpu.VMEM((tail, wide), half_type),
            pltpu.VMEM((tail, pool), half_type),
            pltpu.VMEM((tail + tok_rows, inner), full_type),
            pltpu.VMEM((tail + tok_rows, 2 * wide), full_type),
            pltpu.VMEM((8 + tail + tok_rows, pool), full_type),
            pltpu.VMEM((8 + tail + tok_rows, POOL_GROUP), full_type),
            pltpu.VMEM((8 + tail + tok_rows, POOL_GROUP), full_type),
            pltpu.VMEM((blocks, 2 * BLOCK, inner), half_type),
            pltpu.VMEM((tok_rows, 2 * wide), half_type),
            pltpu.VMEM((blocks * groups, STATE, BLOCK), half_type),
            pltpu.VMEM((blocks, 128, BLOCK), full_type),
            pltpu.VMEM((blocks, BLOCK, 128), full_type),
            pltpu.VMEM((tok_rows, inner), full_type),
            pltpu.VMEM((tok_rows, inner), full_type),
            pltpu.VMEM((blocks, STATE, inner), full_type),
            pltpu.VMEM((STATE, inner), full_type),
            pltpu.VMEM((STATE, inner), full_type),
            pltpu.VMEM((groups, STATE, span), half_type),
            pltpu.VMEM((groups, STATE, span), half_type),
            pltpu.VMEM((tok_rows, inner + pool), half_type),
            pltpu.VMEM((tok_rows, inner + pool), half_type),
        ],
        compiler_params=pltpu.CompilerParams(
            collective_id=0, has_side_effects=True, vmem_limit_bytes=54 * 2**20
        ),
        name="paired_mixers",
    )(*inputs, ssd_weight, pool_rows)


def causal_taps(input_rows, prior_rows, tap_weights, offset_bias):
    padded = jnp.concatenate([prior_rows, input_rows], axis=0).astype(jnp.float32)
    tok_rows = input_rows.shape[0]
    running = jnp.zeros(input_rows.shape, jnp.float32) + offset_bias
    for tap_index in range(tap_weights.shape[0]):
        running = (
            running
            + tap_weights[tap_index].astype(jnp.float32) * padded[tap_index : tap_index + tok_rows]
        )
    return jax.nn.silu(running).astype(jnp.bfloat16)


def pool_mix(input_rows, prior_rows, positions, group_ids, local_weight, local_scale):
    tail_rows = prior_rows.shape[0]
    tok_rows = input_rows.shape[0]
    padded = jnp.concatenate([prior_rows, input_rows], axis=0).astype(jnp.float32)
    window_reach = jnp.left_shift(jnp.int32(2), group_ids)
    running = jnp.zeros(input_rows.shape, jnp.float32)
    for offset_back in range(tail_rows + 1):
        start_row = tail_rows - offset_back
        running = running + padded[start_row : start_row + tok_rows] * (
            offset_back < window_reach
        ).astype(jnp.float32)
    window_count = jnp.minimum(positions[:, None] + 1.0, window_reach.astype(jnp.float32)[None, :])
    pooled = (running / window_count - input_rows.astype(jnp.float32)).astype(jnp.bfloat16)
    grouped = pooled.reshape(tok_rows, local_weight.shape[0], local_weight.shape[1])
    mixed = jnp.einsum("lgc,gcd->lgd", grouped, local_weight, preferred_element_type=jnp.float32)
    return (mixed.reshape(input_rows.shape) * local_scale.astype(jnp.float32)).astype(jnp.bfloat16)


def join_states(earlier, later_part):
    return (
        earlier[0] + later_part[0],
        earlier[1] * jnp.exp(later_part[0])[..., None, None] + later_part[1],
    )


def body(
    statespace_input,
    output_gate_input,
    state_input_projection,
    state_output_projection,
    step_size_input,
    added_log_decay,
    logarithm_rates,
    head_channel_taps,
    input_projection_taps,
    output_projection_taps,
    input_projection_bias,
    group_norm_gain,
    pooling_input,
    pooling_group_weight,
    pooling_channel_scale,
    statespace_output_weight,
    pooling_output_weight,
    output_norm_gain,
):
    core_count = lax.axis_size("tp")
    sp_size, fs_size = lax.axis_size("sp"), lax.axis_size("fs")
    pool_tail = 2**POOL_GROUPS - 1
    paired = (
        statespace_output_weight.shape[1] % 128 == 0
        and fs_size == 4
        and core_count == 2
        and sp_size in (4, 8)
    )
    if paired:
        return mixed_and_projected(
            (
                statespace_input,
                output_gate_input,
                state_input_projection,
                state_output_projection,
                jnp.swapaxes(step_size_input, 1, 2),
                jnp.swapaxes(added_log_decay, 1, 2),
                logarithm_rates[:, None],
                head_channel_taps,
                input_projection_taps,
                output_projection_taps,
                pooling_input,
                pooling_group_weight,
            ),
            {
                "out": output_norm_gain,
                "gain": group_norm_gain,
                "scale": pooling_channel_scale,
                "bias": input_projection_bias,
            },
            statespace_output_weight,
            pooling_output_weight,
            pool_tail + 1,
        )
    core_index = lax.axis_index("tp")
    seq_index = lax.axis_index("sp")
    head_channel_rows = statespace_input[0]
    output_gate_rows = output_gate_input[0]
    input_projection_rows = state_input_projection[0]
    output_projection_rows = state_output_projection[0]
    step_size_rows = step_size_input[0]
    decay_spikes = added_log_decay[0]
    pooling_rows = pooling_input[0]
    tok_rows = head_channel_rows.shape[0]
    inner_local = head_channel_rows.shape[1]
    heads_local = step_size_rows.shape[1]
    state_local = input_projection_rows.shape[1]
    pool_local = pooling_rows.shape[1]
    groups_local = state_local // STATE
    per_group = heads_local // groups_local
    groups_pool = pool_local // POOL_GROUP
    conv_tail = CONV - 1
    own_columns = jnp.concatenate([statespace_output_weight, pooling_output_weight], axis=0)
    tails = jnp.concatenate(
        [
            jnp.pad(rows[tok_rows - tail :], ((pool_tail - tail, 0), (0, 0)))
            for rows, tail in (
                (head_channel_rows, conv_tail),
                (input_projection_rows, conv_tail),
                (output_projection_rows, conv_tail),
                (pooling_rows, pool_tail),
            )
        ],
        axis=1,
    )
    prior = passed_along(tails, "sp", 1)
    widths = (inner_local, state_local, state_local, pool_local)
    prior_x, prior_b, prior_c, prior_pool = (
        prior[pool_tail - tail :, sum(widths[:at]) : sum(widths[: at + 1])]
        for at, tail in enumerate((conv_tail, conv_tail, conv_tail, pool_tail))
    )
    taps_x = lax.dynamic_slice_in_dim(head_channel_taps, core_index * inner_local, inner_local, 1)
    taps_b = lax.dynamic_slice_in_dim(
        input_projection_taps, core_index * state_local, state_local, 1
    )
    taps_c = lax.dynamic_slice_in_dim(
        output_projection_taps, core_index * state_local, state_local, 1
    )
    bias_b = lax.dynamic_slice_in_dim(
        input_projection_bias, core_index * state_local, state_local, 0
    )
    gain_ssd = lax.dynamic_slice_in_dim(group_norm_gain, core_index * inner_local, inner_local, 0)
    head_decay_rates = jnp.exp(
        lax.dynamic_slice_in_dim(logarithm_rates, core_index * heads_local, heads_local, 0)
    )
    gain_pool = lax.dynamic_slice_in_dim(
        pooling_channel_scale, core_index * pool_local, pool_local, 0
    )
    weight_pool = lax.dynamic_slice_in_dim(
        pooling_group_weight, core_index * groups_pool, groups_pool, 0
    )
    whole_columns = lax.all_gather(own_columns, ("sp", "fs"), axis=1, tiled=True)
    x_conv = causal_taps(head_channel_rows, prior_x, taps_x, 0.0)
    b_conv = causal_taps(input_projection_rows, prior_b, taps_b, bias_b.astype(jnp.float32))
    c_conv = causal_taps(output_projection_rows, prior_c, taps_c, 0.0)
    blocks = tok_rows // BLOCK
    discrete_step_size = jax.nn.softplus(step_size_rows.astype(jnp.float32))
    logarithm_decay = -discrete_step_size * head_decay_rates + decay_spikes
    cumulative_decay = jnp.cumsum(
        logarithm_decay.reshape(blocks, BLOCK, groups_local, per_group), axis=1
    )
    cum_t = cumulative_decay.transpose(0, 2, 3, 1)
    step_t = discrete_step_size.reshape(blocks, BLOCK, groups_local, per_group).transpose(
        0, 2, 3, 1
    )
    heads_x = x_conv.reshape(blocks, BLOCK, groups_local, per_group, HEAD_DIM)
    group_b = b_conv.reshape(blocks, BLOCK, groups_local, STATE)
    group_c = c_conv.reshape(blocks, BLOCK, groups_local, STATE)
    scores = jnp.einsum("ktgn,kugn->kgtu", group_c, group_b, preferred_element_type=jnp.float32)
    causal = jnp.arange(BLOCK)[:, None] >= jnp.arange(BLOCK)[None, :]
    decay_gap = cum_t[..., :, None] - cum_t[..., None, :]
    decay_factor = jnp.where(causal, jnp.exp(jnp.where(causal, decay_gap, 0.0)), 0.0)
    weights = (scores[:, :, None] * decay_factor * step_t[..., None, :]).astype(jnp.bfloat16)
    within = jnp.einsum("kgetu,kugep->ktgep", weights, heads_x, preferred_element_type=jnp.float32)
    block_end = cum_t[..., -1]
    end_weight = jnp.exp(block_end[..., None] - cum_t) * step_t
    scaled_x = (heads_x * end_weight.transpose(0, 3, 1, 2)[..., None]).astype(jnp.bfloat16)
    block_state = jnp.einsum(
        "kugep,kugn->kgepn", scaled_x, group_b, preferred_element_type=jnp.float32
    )

    def local_chain(state_now, current_inputs):
        piece_state, piece_fall = current_inputs
        return (state_now * jnp.exp(piece_fall)[..., None, None] + piece_state, state_now)

    final_state, local_entering = lax.scan(
        local_chain, jnp.zeros(block_state.shape[1:], jnp.float32), (block_state, block_end)
    )
    log_total = jnp.sum(block_end, axis=0)
    prefix_log = jnp.cumsum(block_end, axis=0) - block_end
    log_before, state_before = entering_2(
        (log_total, final_state),
        "sp",
        join_states,
        (jnp.zeros_like(log_total), jnp.zeros_like(final_state)),
    )
    entering = (local_entering + jnp.exp(prefix_log)[..., None, None] * state_before[None]).astype(
        jnp.bfloat16
    )
    carried_out = jnp.einsum(
        "ktgn,kgepn->ktgep", group_c, entering, preferred_element_type=jnp.float32
    )
    carried_out = carried_out * jnp.exp(cumulative_decay)[..., None]
    mixed_ssd = (within + carried_out).reshape(tok_rows, inner_local) * jax.nn.silu(
        output_gate_rows.astype(jnp.float32)
    )
    grouped = mixed_ssd.reshape(tok_rows, groups_local, inner_local // groups_local)
    normed = grouped * lax.rsqrt(jnp.mean(grouped * grouped, axis=-1, keepdims=True) + eps)
    ssd_out = (normed.reshape(tok_rows, inner_local) * gain_ssd.astype(jnp.float32)).astype(
        jnp.bfloat16
    )
    positions = (seq_index * tok_rows + jnp.arange(tok_rows, dtype=jnp.int32)).astype(jnp.float32)
    group_ids = core_index * groups_pool + jnp.arange(pool_local, dtype=jnp.int32) // POOL_GROUP
    pool_out = pool_mix(pooling_rows, prior_pool, positions, group_ids, weight_pool, gain_pool)
    channels = jnp.concatenate([ssd_out, pool_out], axis=1)
    half_width = D // core_count
    gain_out = lax.dynamic_slice_in_dim(
        output_norm_gain, core_index * half_width, half_width, 0
    ).astype(jnp.float32)
    partial = jnp.dot(channels, whole_columns, preferred_element_type=jnp.float32).astype(
        jnp.bfloat16
    )
    own_half = lax.dynamic_slice_in_dim(partial, core_index * half_width, half_width, 1).astype(
        jnp.float32
    )
    for hop in range(1, core_count):
        target = lax.rem(core_index + hop, core_count)
        leaving = lax.dynamic_slice_in_dim(partial, target * half_width, half_width, 1)
        route = [(i, (i + hop) % core_count) for i in range(core_count)]
        own_half = own_half + lax.ppermute(leaving, "tp", route).astype(jnp.float32)
    row_squares = lax.psum(jnp.sum(own_half * own_half, axis=1), "tp")
    result = own_half * lax.rsqrt(row_squares / D + eps)[:, None] * gain_out
    return result.astype(jnp.bfloat16)[None]


def solution(mesh):
    in_specs = (
        P("fs", "sp", "tp"),
        P("fs", "sp", "tp"),
        P("fs", "sp", "tp"),
        P("fs", "sp", "tp"),
        P("fs", "sp", "tp"),
        P("fs", "sp", "tp"),
        P(),
        P(),
        P(),
        P(),
        P(),
        P(),
        P("fs", "sp", "tp"),
        P(),
        P(),
        P("tp", ("sp", "fs")),
        P("tp", ("sp", "fs")),
        P(),
    )
    out_specs = P("fs", "sp", "tp")
    return jax.shard_map(body, mesh=mesh, in_specs=in_specs, out_specs=out_specs, check_vma=False)
```

```python
import functools

import jax
import jax.numpy as jnp
from jax import lax
from jax.experimental import pallas as pl
from jax.experimental.pallas import tpu as pltpu
from jax.sharding import PartitionSpec as P

D = 4096
HEAD_DIM = 64
STATE = 128
CONV = 4
BLOCK = 128
POOL_GROUPS = 4
POOL_GROUP = 256


eps = 1e-06


def passed_along(block, axis, distance):
    devices = range(lax.axis_size(axis))
    route = [(i - distance, i) for i in devices if i - distance in devices]
    return lax.ppermute(block, axis, route)


def entering_2(array, axis, join, neutral):
    place = lax.axis_index(axis)
    gathered = jax.tree.map(
        lambda a, kind: lax.all_gather(a.astype(kind), axis), array, (jnp.bfloat16, jnp.bfloat16)
    )
    state = jax.tree.map(lambda a, e: jnp.zeros_like(a) + jnp.asarray(e, a.dtype), array, neutral)

    def one(lap, state):
        return join(
            state,
            jax.tree.map(
                lambda a, own: lax.dynamic_index_in_dim(a, lap, 0, False).astype(own.dtype),
                gathered,
                array,
            ),
        )

    return lax.fori_loop(0, place, one, state)


MESH_IDS = pl.DeviceIdType.MESH
EXACT = lax.Precision.HIGHEST
CHUNKS, CHAINS = 6, 4
INPUTS, GATE, VECTORS = 13, 1, 10
SOURCES, OTHERS = (0, 2, 3, 11), (4, 5, 6, 7, 8, 9, 10, 12)


class Links:
    def __init__(self, sp_size, fs_size):
        self.n = sp_size
        self.z = lax.axis_index("sp")
        self.fs = lax.axis_index("fs")
        self.core = lax.axis_index("tp")
        self.x = lax.rem(self.fs, 2)
        self.y = self.fs // 2
        self.beside = {"fs": self.fs + 1 - 2 * self.x}
        self.across = {"fs": self.fs + 2 - 4 * self.y}
        self.sibling = {"tp": 1 - self.core}

    def barrier(self):
        barrier = pltpu.get_barrier_semaphore()
        near = [{"sp": lax.rem(self.z + far, self.n)} for far in (1, self.n - 1)]
        for other in (*near, self.beside, self.across, self.sibling):
            pl.semaphore_signal(barrier, inc=1, device_id=other, device_id_type=MESH_IDS)
        pl.semaphore_wait(barrier, len(near) + 3)

    def within(self, place):
        return jnp.logical_and(place >= 0, place < self.n)

    def nearest(self, turn):
        if turn == 0:
            return self.z
        low, high = self.z, self.n - 1 - self.z
        small = jnp.minimum(low, high)
        both = turn <= 2 * small
        far = jnp.where(both, (turn + 1) // 2, turn - small)
        sign = jnp.where(both, 1 - 2 * (turn % 2), jnp.where(high > low, 1, -1))
        return self.z + sign * far


def remote(src, dst, sends, arrivals, spot, device):
    return pltpu.make_async_remote_copy(
        src_ref=src,
        dst_ref=dst,
        send_sem=sends.at[spot],
        recv_sem=arrivals.at[spot],
        device_id=device,
        device_id_type=MESH_IDS,
    )


class Weights:
    def __init__(self, links, whole, width, z_sems, y_sems):
        self.links, self.whole, self.width = links, whole, width
        self.z_sems, self.y_sems = z_sems, y_sems
        self.rows = whole.shape[0] // CHUNKS
        self.direct = range(CHUNKS - 1)
        self.turned = (CHUNKS - 1,)
        self.sent = {}

    def region(self, chunk, z, y):
        at = pl.multiple_of((z * 2 + y) * self.width, self.width)
        return self.whole.at[pl.ds(chunk * self.rows, self.rows), pl.ds(at, self.width)]

    def along(self, chunk, step, way, side, arriving):
        links = self.links
        origin = links.z - way * (step if arriving else step - 1)
        y = links.y if side == 0 else 1 - links.y
        spot = ((chunk * (links.n - 1) + step - 1) * 2 + (way < 0)) * 2 + side
        place = self.region(chunk, jnp.clip(origin, 0, links.n - 1), y)
        copy = remote(place, place, *self.z_sems, spot, {"sp": links.z + way})
        far = links.z if arriving else links.z + way
        return copy, jnp.logical_and(links.within(origin), links.within(far))

    def over(self, chunk, offset, arriving):
        links = self.links
        y = 1 - links.y if arriving else links.y
        origin = links.z + offset
        place = self.region(chunk, jnp.clip(origin, 0, links.n - 1), y)
        spot = chunk * (2 * links.n - 1) + offset + links.n - 1
        copy = remote(place, place, *self.y_sems, spot, links.across)
        return copy, links.within(origin)

    def go(self, kind, *key):
        copy, here = kind(*key, False)
        self.sent[kind.__name__, key] = kind
        pl.when(here)(copy.start)

    def take(self, kind, *key):
        copy, here = kind(*key, True)
        pl.when(here)(copy.wait_recv)

    def pass_on(self, chunk, step, way, side):
        if step < self.links.n and not self.single(step, way, side):
            self.go(self.along, chunk, step, way, side)

    def single(self, step, way, side):
        return step >= self.links.n - 2 and way == 1 and side == 1

    def begin(self):
        for chunk in (*self.turned, *self.direct):
            self.go(self.over, chunk, 0)

    def own(self, chunks, sides=(0,), ways=(1, -1)):
        for chunk in chunks:
            for side in sides:
                for way in ways:
                    self.pass_on(chunk, 1, way, side)

    def turn(self):
        for chunk in self.turned:
            self.take(self.over, chunk, 0)

    def hop(self, step, chunks, sides=(0,), ways=(1, -1)):
        for chunk in chunks:
            for way in ways:
                for side in sides:
                    if not self.single(step, way, side):
                        self.take(self.along, chunk, step, way, side)
                        self.pass_on(chunk, step + 1, way, side)
                if chunk in self.direct or (0 in sides and self.single(step, way, 1)):
                    self.go(self.over, chunk, -way * step)

    def settle(self, step):
        for chunk in self.direct:
            for offset in (0,) if step == 0 else (step, -step):
                self.take(self.over, chunk, offset)
        if self.single(step, 1, 1):
            for chunk in self.turned:
                self.take(self.over, chunk, -step)

    def finish(self):
        for (_, key), kind in self.sent.items():
            copy, here = kind(*key, False)
            pl.when(here)(copy.wait_send)


def silu(rows):
    return rows / (1.0 + jnp.exp(-rows))


def softplus(rows):
    return jnp.maximum(rows, 0.0) + jnp.log(1.0 + jnp.exp(-jnp.abs(rows)))


def chosen(core, options):
    best = options[0]
    for at in range(1, len(options)):
        best = jnp.where(core == at, options[at], best)
    return best


def mixers(links, tail, cores, pieces, fetches, refs, sems):
    (x_in, gate, b_in, c_in, dt, added, rates, x_taps, b_taps, c_taps, vectors, pool_in,
     pool_weight, prior_x, prior_b, prior_c, prior_pool, x_pad, bc_pad, pool_pad,
     pool_two, pool_four, x_split, bc_conv, b_turned, flat, upright, within, grown, local_in,
     state, before, carry_in, carry_out, channels, far_channels) = refs
    sends, arrivals = sems
    rows, inner = x_in.shape[1:]
    heads = dt.shape[1]
    wide = b_in.shape[2]
    pool = pool_in.shape[2]
    groups = wide // STATE
    span = inner // groups
    blocks = rows // BLOCK
    z, core = links.z, links.core
    lead = 8
    parts = CHAINS
    length = inner // parts
    sources = ((x_in, prior_x), (b_in, prior_b), (c_in, prior_c), (pool_in, prior_pool))

    def tails(at):
        source, target = sources[at]
        return remote(
            source.at[0, pl.ds(rows - tail, tail)], target, sends, arrivals, at, {"sp": z + 1}
        )

    def chain(group):
        return remote(
            carry_out.at[group], carry_in.at[group], sends, arrivals, 4 + group, {"sp": z + 1}
        )

    def pool_letter():
        cols = pl.ds(inner, pool)
        return remote(
            channels.at[:, cols], far_channels.at[:, cols], sends, arrivals, 4 + parts, links.beside
        )

    def block_letter(at):
        place = (pl.ds(at * BLOCK, BLOCK), pl.ds(0, inner))
        return remote(
            channels.at[place], far_channels.at[place], sends, arrivals, 5 + parts + at, links.beside
        )

    follows = z + 1 < links.n
    for at in SOURCES:
        fetches[at].wait()

    @pl.when(follows)
    def _():
        for at in range(4):
            tails(at).start()

    yield "start"
    for at in OTHERS:
        fetches[at].wait()
    x_pad[tail:] = x_in[0].astype(jnp.float32)
    bc_pad[tail:, 0:wide] = b_in[0].astype(jnp.float32)
    bc_pad[tail:, wide:] = c_in[0].astype(jnp.float32)
    pool_pad[0:lead] = jnp.zeros((lead, pool), jnp.float32)
    pool_pad[lead + tail :] = pool_in[0].astype(jnp.float32)
    steps_flat = softplus(dt[0].astype(jnp.float32))
    table = (heads, rates.shape[1])
    picked = lax.broadcasted_iota(jnp.int32, table, 1) == (
        core * heads + lax.broadcasted_iota(jnp.int32, table, 0)
    )
    own_rates = jnp.sum(
        jnp.where(picked, jnp.broadcast_to(rates[...], table), 0.0), axis=1, keepdims=True
    )
    logs_flat = -steps_flat * jnp.exp(own_rates) + added[0]
    flat[...] = jnp.zeros_like(flat)
    down = lax.broadcasted_iota(jnp.int32, (BLOCK, BLOCK), 0)
    over = lax.broadcasted_iota(jnp.int32, (BLOCK, BLOCK), 1)
    causal = down >= over
    upper = (down <= over).astype(jnp.float32)
    first_half = lax.broadcasted_iota(jnp.int32, (BLOCK, 2 * HEAD_DIM), 1) < HEAD_DIM

    def mine(ref, size):
        at = pl.multiple_of(core * size, size)
        return ref[:, pl.ds(at, size)].astype(jnp.float32)

    taps_x = mine(x_taps, inner)
    taps_bc = jnp.concatenate([mine(b_taps, wide), mine(c_taps, wide)], axis=1)
    bias_b = pieces(vectors, "bias", core * wide, wide)
    bias_bc = jnp.concatenate([bias_b, jnp.zeros_like(bias_b)], axis=1)

    @pl.when(z == 0)
    def _():
        x_pad[0:tail] = jnp.zeros((tail, inner), jnp.float32)
        bc_pad[0:tail] = jnp.zeros((tail, 2 * wide), jnp.float32)
        pool_pad[lead : lead + tail] = jnp.zeros((tail, pool), jnp.float32)

    @pl.when(z > 0)
    def _():
        for at in range(4):
            tails(at).wait_recv()
        x_pad[0:tail] = prior_x[...].astype(jnp.float32)
        bc_pad[0:tail, 0:wide] = prior_b[...].astype(jnp.float32)
        bc_pad[0:tail, wide:] = prior_c[...].astype(jnp.float32)
        pool_pad[lead : lead + tail] = prior_pool[...].astype(jnp.float32)

    def taps(pad, weights, at, cols):
        total = None
        for tap in range(CONV):
            begin = at * BLOCK + tail - CONV + 1 + tap
            term = pad[begin : begin + BLOCK, cols] * weights[tap : tap + 1, cols]
            total = term if total is None else total + term
        return total

    def spread(narrow, head):
        shape = (BLOCK, 2 * HEAD_DIM)
        return jnp.where(
            first_half,
            jnp.broadcast_to(narrow[:, head : head + 1], shape),
            jnp.broadcast_to(narrow[:, head + 1 : head + 2], shape),
        )

    pairs = span // (2 * HEAD_DIM)
    ends = []
    state[...] = jnp.zeros_like(state)
    for at in range(blocks):
        now = slice(at * BLOCK, (at + 1) * BLOCK)
        bc_conv[now] = silu(taps(bc_pad, taps_bc, at, slice(0, 2 * wide)) + bias_bc).astype(
            jnp.bfloat16
        )
        flat[at, 0:heads] = jnp.dot(
            logs_flat[:, now], upper, precision=EXACT, preferred_element_type=jnp.float32
        )
        flat[at, heads : 2 * heads] = steps_flat[:, now]
        upright[at] = jnp.transpose(flat[at])
        cum = upright[at, :, 0:heads]
        decayed = jnp.exp(cum)
        closing = jnp.exp(cum[BLOCK - 1 : BLOCK] - cum) * upright[at, :, heads : 2 * heads]
        ended = []
        for group in range(groups):
            cols = slice(group * span, (group + 1) * span)
            x_now = silu(taps(x_pad, taps_x, at, cols))
            b_now = bc_conv[now, group * STATE : (group + 1) * STATE]
            b_flat = jnp.transpose(b_now.astype(jnp.float32)).astype(jnp.bfloat16)
            b_turned[at * groups + group] = b_flat
            scaled = []
            for pair in range(pairs):
                head = group * (span // HEAD_DIM) + 2 * pair
                lanes = slice(pair * 2 * HEAD_DIM, (pair + 1) * 2 * HEAD_DIM)
                here = slice(head * HEAD_DIM, (head + 2) * HEAD_DIM)
                x_pair = x_now[:, lanes]
                x_split[at, 0:BLOCK, here] = jnp.where(first_half, x_pair, 0.0).astype(jnp.bfloat16)
                x_split[at, BLOCK : 2 * BLOCK, here] = jnp.where(first_half, 0.0, x_pair).astype(
                    jnp.bfloat16
                )
                x_half = x_pair.astype(jnp.bfloat16).astype(jnp.float32)
                scaled.append((x_half * spread(closing, head)).astype(jnp.bfloat16))
                grown[now, here] = spread(decayed, head)
            end = grown[(at + 1) * BLOCK - 1 : (at + 1) * BLOCK, cols]
            ended.append(end)
            local_in[at, :, cols] = state[:, cols]
            state[:, cols] = state[:, cols] * end + jnp.dot(
                b_flat, jnp.concatenate(scaled, axis=1), preferred_element_type=jnp.float32
            )
        yield at
        ends.append(ended)

    def hand_on():
        @pl.when(z == 0)
        def _():
            before[...] = jnp.zeros_like(before)

        for link in range(parts):
            cols = slice(link * length, (link + 1) * length)
            group, at_end = link * length // span, slice(link * length % span, link * length % span + length)

            @pl.when(z > 0)
            def _(link=link, cols=cols):
                chain(link).wait_recv()
                before[:, cols] = carry_in[link].astype(jnp.float32)

            @pl.when(follows)
            def _(link=link, cols=cols, group=group, at_end=at_end):
                falling = ends[0][group][:, at_end]
                for at in range(1, blocks):
                    falling = falling * ends[at][group][:, at_end]
                carry_out[link] = (before[:, cols] * falling + state[:, cols]).astype(jnp.bfloat16)
                chain(link).start()

    def chain_point(place, last=False):
        pl.when(z >= place if last else z == place)(hand_on)

    chain_point(0)
    yield "states"
    place = z * rows
    position = (place + lax.broadcasted_iota(jnp.int32, (rows, 1), 0)).astype(jnp.float32) + 1.0
    pool_groups = pool // POOL_GROUP
    for group in range(pool_groups):
        cols = slice(group * POOL_GROUP, (group + 1) * POOL_GROUP)
        size = rows + tail
        two = pool_pad[lead:, cols] + pool_pad[lead - 1 : lead - 1 + size, cols]
        pool_two[0:lead] = jnp.zeros((lead, POOL_GROUP), jnp.float32)
        pool_two[lead:] = two
        four = two + pool_two[lead - 2 : lead - 2 + size]
        pool_four[0:lead] = jnp.zeros((lead, POOL_GROUP), jnp.float32)
        pool_four[lead:] = four
        eight = four + pool_four[lead - 4 : lead - 4 + size]
        sixteen = eight[tail:] + eight[tail - 8 : size - 8]
        sums = [two[tail:], four[tail:], eight[tail:], sixteen]
        picks = [c * pool_groups + group for c in range(cores)]
        running = chosen(core, [sums[pick] for pick in picks])
        reach = chosen(core, [jnp.float32(2 ** (pick + 1)) for pick in picks])
        pooled = running / jnp.minimum(position, reach) - pool_in[0, :, cols].astype(jnp.float32)
        mixed = jnp.dot(
            pooled.astype(jnp.bfloat16),
            pool_weight[core * pool_groups + group],
            preferred_element_type=jnp.float32,
        )
        scale = pieces(vectors, "scale", core * pool + group * POOL_GROUP, POOL_GROUP)
        out = inner + group * POOL_GROUP
        channels[:, out : out + POOL_GROUP] = (mixed * scale).astype(jnp.bfloat16)
    pool_letter().start()
    for at in range(blocks):
        now = slice(at * BLOCK, (at + 1) * BLOCK)
        cum = upright[at, :, 0:heads]
        cum_flat = flat[at, 0:heads]
        step_flat = flat[at, heads : 2 * heads]
        for group in range(groups):
            c_now = bc_conv[now, wide + group * STATE : wide + (group + 1) * STATE]
            scores = jnp.dot(
                c_now, b_turned[at * groups + group], preferred_element_type=jnp.float32
            )
            for pair in range(pairs):
                first = group * (span // HEAD_DIM) + 2 * pair
                both = []
                for head in (first, first + 1):
                    gap = cum[:, head : head + 1] - cum_flat[head : head + 1]
                    decay = jnp.exp(jnp.where(causal, gap, -1e30))
                    both.append((scores * decay * step_flat[head : head + 1]).astype(jnp.bfloat16))
                here = slice(first * HEAD_DIM, (first + 2) * HEAD_DIM)
                within[now, here] = jnp.dot(
                    jnp.concatenate(both, axis=1),
                    x_split[at, :, here],
                    preferred_element_type=jnp.float32,
                )
    chain_point(1)
    yield "second"
    chain_point(2)
    yield "third"
    chain_point(3, True)
    falling = [None] * groups
    fetches[GATE].wait()
    for at in range(blocks):
        now = slice(at * BLOCK, (at + 1) * BLOCK)
        for group in range(groups):
            cols = slice(group * span, (group + 1) * span)
            earlier = before[:, cols]
            if at:
                earlier = earlier * falling[group]
            entering = local_in[at, :, cols] + earlier
            c_now = bc_conv[now, wide + group * STATE : wide + (group + 1) * STATE]
            carried = jnp.dot(
                c_now, entering.astype(jnp.bfloat16), preferred_element_type=jnp.float32
            )
            mixed = (within[now, cols] + carried * grown[now, cols]) * silu(
                gate[0, now, cols].astype(jnp.float32)
            )
            root = lax.rsqrt(jnp.mean(mixed * mixed, axis=1, keepdims=True) + eps)
            gain = pieces(vectors, "gain", core * inner + group * span, span)
            channels[now, cols] = (mixed * root * gain).astype(jnp.bfloat16)
            end = ends[at][group]
            falling[group] = end if at == 0 else falling[group] * end
        block_letter(at).start()
    letters = [pool_letter(), *(block_letter(at) for at in range(blocks))]

    def received():
        for letter in letters:
            letter.wait_recv()

    def finish():
        for letter in letters:
            letter.wait_send()

        @pl.when(follows)
        def _():
            for at in range(4):
                tails(at).wait_send()
            for link in range(parts):
                chain(link).wait_send()

    return received, finish


def whole_kernel(sp_size, fs_size, cores, tail, pieces, *refs):
    inputs, ssd_weight, pool_rows, out = refs[:INPUTS], *refs[INPUTS : INPUTS + 3]
    (z_sends, z_arrivals, y_sends, y_arrivals, m_sends, m_arrivals, p_sends, p_arrivals, o_sends,
     o_arrivals, local_sems, whole, parts, part_in, returned, return_in, squares, squares_in,
     *rest) = refs[INPUTS + 3 :]
    held, rest = rest[:INPUTS], rest[INPUTS:]
    vectors = held[VECTORS]
    channels, far_channels = rest[-2:]
    links = Links(sp_size, fs_size)
    width = ssd_weight.shape[1]
    inner = ssd_weight.shape[0]
    rows = channels.shape[0]
    half = sp_size // cores
    core = links.core
    own_at = pl.multiple_of((links.z * 2 + links.y) * width, width)
    loads = [
        pltpu.make_async_copy(
            source, whole.at[pl.ds(begin, source.shape[0]), pl.ds(own_at, width)], local_sems.at[at]
        )
        for at, (source, begin) in enumerate(((ssd_weight, 0), (pool_rows, inner)))
    ]
    fetches = [
        pltpu.make_async_copy(source, place, local_sems.at[2 + at])
        for at, (source, place) in enumerate(zip(inputs, held))
    ]
    for at in SOURCES:
        fetches[at].start()
    for load in loads:
        load.start()
    for at in (*OTHERS, GATE):
        fetches[at].start()
    links.barrier()
    weights = Weights(links, whole, width, (z_sends, z_arrivals), (y_sends, y_arrivals))
    work = mixers(links, tail, cores, pieces, fetches, (*held, *rest), (m_sends, m_arrivals))

    direct, turned = weights.direct, weights.turned
    both = (0, 1)
    last = sp_size - 1
    mixed = None
    while mixed is None:
        try:
            mark = next(work)
        except StopIteration as ended:
            mixed = ended.value
            break
        if mark == "start":
            for load in loads:
                load.wait()
            weights.begin()
            weights.own(direct[:3])
        elif mark == 1:
            weights.own(direct[3:4])
        elif mark == "states":
            weights.own(direct[4:])
            weights.turn()
            weights.own(turned, both, (-1,))
            pl.when(links.z >= 2)(lambda: weights.own(turned, both, (1,)))
            weights.hop(1, direct[:1], ways=(-1,))
        elif mark == "second":
            weights.hop(1, direct[1:3], ways=(-1,))
            pl.when(links.z == 1)(lambda: weights.own(turned, both, (1,)))
            pl.when(links.z == 1)(lambda: weights.hop(1, direct[:4], ways=(1,)))
            pl.when(links.z == last)(lambda: weights.hop(1, direct, ways=(1,)))
            inner_late = jnp.logical_and(links.z >= 2, links.z < last)
            pl.when(inner_late)(lambda: weights.hop(1, direct[:2], ways=(1,)))
        elif mark == "third":
            pl.when(inner_late)(lambda: weights.hop(1, direct[2:], ways=(1,)))
            pl.when(links.z == last)(lambda: weights.hop(2, direct[:2], ways=(1,)))
            pl.when(links.z >= 2)(lambda: weights.hop(1, direct[3:], ways=(-1,)))
    received, finish_mixers = mixed
    pl.when(links.z == 0)(lambda: weights.own(turned, both, (1,)))
    pl.when(links.z == 1)(lambda: weights.hop(1, direct[4:], ways=(1,)))
    pl.when(links.z <= 1)(lambda: weights.hop(1, direct[3:], ways=(-1,)))

    def multiply(turn, far, sides=both):
        z = links.nearest(turn)
        source = far_channels if far else channels

        @pl.loop(0, len(sides))
        def _(at):
            y = lax.rem(links.y + sides[0] + at, 2)
            slab = z * 2 + y
            lanes = pl.ds(pl.multiple_of(slab * width, width), width)
            parts[far, slab] = jnp.dot(
                source[...], whole[:, lanes], preferred_element_type=jnp.float32
            ).astype(jnp.bfloat16)

            @pl.when(z // half != core)
            def _():
                part_letter(z, y, far).start()

    def part_letter(z, y, far):
        slab = z * 2 + y
        return remote(
            parts.at[far, slab],
            part_in.at[far, lax.rem(z, half) * 2 + y],
            p_sends,
            p_arrivals,
            far * 2 * sp_size + slab,
            links.sibling,
        )

    def return_letter(slot):
        return remote(
            returned.at[slot], return_in.at[slot], o_sends, o_arrivals, slot, links.beside
        )

    def give_back(turn, sides=both):
        z = links.nearest(turn)

        @pl.when(z // half == core)
        def _():
            @pl.loop(0, len(sides))
            def _(at):
                y = lax.rem(links.y + sides[0] + at, 2)
                part_letter(z, y, 1).wait_recv()
                slot = lax.rem(z, half) * 2 + y
                returned[slot] = (
                    parts[1, z * 2 + y].astype(jnp.float32) + part_in[1, slot].astype(jnp.float32)
                ).astype(jnp.bfloat16)
                return_letter(slot).start()

    edge = jnp.logical_or(links.z == 0, links.z == last)
    weights.settle(0)
    multiply(0, 0)
    for step in range(1, last):
        weights.hop(step, turned, both)
        if step + 1 < last:
            if step == 1:
                pl.when(links.z == last)(lambda: weights.hop(2, direct[2:]))
                pl.when(links.z != last)(lambda: weights.hop(2, direct))
            else:
                weights.hop(step + 1, direct)
            weights.settle(step)
            multiply(step, 0)
    received()
    share = -(-len(direct) // last)

    def ahead(turn):
        multiply(turn, 1)
        give_back(turn)
        multiply(turn, 0)

    for turn in range(last):
        pieces_now = direct[turn * share : (turn + 1) * share]
        if turn == last - 1:
            pl.when(jnp.logical_not(edge))(lambda: ahead(turn))
            weights.settle(turn)
            weights.hop(last, pieces_now)
            pl.when(edge)(lambda: ahead(turn))
        else:
            multiply(turn, 1)
            weights.hop(last, pieces_now)
            give_back(turn)
    weights.hop(last, turned, (0,))
    multiply(last, 1, (0,))
    multiply(last, 0, (0,))
    give_back(last, (0,))
    weights.hop(last, turned, (1,))
    weights.settle(last)
    multiply(last, 1, (1,))
    multiply(last, 0, (1,))
    give_back(last, (1,))
    own_half = core * half
    slots = 2 * half

    def lane_squares(values):
        values = values * values
        total = values[:, 0:128]
        for at in range(1, width // 128):
            total = total + values[:, at * 128 : (at + 1) * 128]
        return total

    def own_total(slot):
        return parts[0, own_half * 2 + slot].astype(jnp.float32) + part_in[0, slot].astype(
            jnp.float32
        )

    squares[...] = jnp.zeros_like(squares)

    @pl.loop(0, slots)
    def _(slot):
        part_letter(own_half + slot // 2, lax.rem(slot, 2), 0).wait_recv()
        squares[...] += lane_squares(own_total(slot))

    @pl.loop(0, slots)
    def _(slot):
        return_letter(slot).wait_recv()
        squares[...] += lane_squares(return_in[slot].astype(jnp.float32))

    exchange = remote(squares, squares_in, o_sends, o_arrivals, slots, links.sibling)
    exchange.start()
    exchange.wait_recv()
    row_squares = jnp.sum(squares[...] + squares_in[...], axis=1, keepdims=True)
    features = cores * out.shape[2]
    root = lax.rsqrt(row_squares / features + eps)

    @pl.loop(0, slots)
    def _(slot):
        first = (slot // 2) * fs_size + 2 * lax.rem(slot, 2)
        for values, x in (
            (own_total(slot), links.x),
            (return_in[slot].astype(jnp.float32), 1 - links.x),
        ):
            at = pl.multiple_of((first + x) * width, width)
            gain = pieces(vectors, "out", core * out.shape[2] + at, width)
            out[0, :, pl.ds(at, width)] = (values * root * gain).astype(jnp.bfloat16)

    exchange.wait_send()
    weights.finish()
    finish_mixers()

    @pl.loop(0, 2 * half)
    def _(slot):
        return_letter(slot).wait_send()
        other = (1 - core) * half
        for far in range(2):
            part_letter(other + slot // 2, lax.rem(slot, 2), far).wait_send()


def mixed_and_projected(inputs, vectors, ssd_weight, pool_rows, tail):
    sp_size, fs_size, cores = lax.axis_size("sp"), lax.axis_size("fs"), lax.axis_size("tp")
    width = ssd_weight.shape[1]
    x_in, b_in, pool_in = inputs[0], inputs[2], inputs[10]
    starts, features = {}, vectors["out"].shape[0]
    for name, vector in vectors.items():
        starts[name] = sum(vectors[other].shape[0] for other in starts)

    def pieces(ref, name, offset, size):
        at = pl.multiple_of(starts[name] + offset, 128)
        return ref[:, pl.ds(at, size)].astype(jnp.float32)

    joined = jnp.concatenate(list(vectors.values()))[None]
    inputs = (*inputs[:10], joined, *inputs[10:])
    tok_rows, inner = x_in.shape[1:]
    wide, pool = b_in.shape[2], pool_in.shape[2]
    groups = wide // STATE
    blocks = tok_rows // BLOCK
    half = sp_size // cores
    slots = 2 * half
    vmem = pl.BlockSpec(memory_space=pltpu.VMEM)
    hbm = pl.BlockSpec(memory_space=pltpu.HBM)
    dma = pltpu.SemaphoreType.DMA
    half_type, full_type = jnp.bfloat16, jnp.float32
    z_spots, y_spots = CHUNKS * (sp_size - 1) * 4, CHUNKS * (2 * sp_size - 1)
    letters = 5 + CHAINS + blocks
    return pl.pallas_call(
        functools.partial(whole_kernel, sp_size, fs_size, cores, tail, pieces),
        out_shape=pltpu.VMEM((1, tok_rows, features // cores), half_type),
        in_specs=[hbm] * (len(inputs) + 2),
        out_specs=vmem,
        scratch_shapes=[
            dma((z_spots,)),
            dma((z_spots,)),
            dma((y_spots,)),
            dma((y_spots,)),
            dma((letters,)),
            dma((letters,)),
            dma((4 * sp_size,)),
            dma((4 * sp_size,)),
            dma((slots + 1,)),
            dma((slots + 1,)),
            dma((2 + len(inputs),)),
            pltpu.VMEM((inner + pool, width * 2 * sp_size), half_type),
            pltpu.VMEM((2, 2 * sp_size, tok_rows, width), half_type),
            pltpu.VMEM((2, slots, tok_rows, width), half_type),
            pltpu.VMEM((slots, tok_rows, width), half_type),
            pltpu.VMEM((slots, tok_rows, width), half_type),
            pltpu.VMEM((tok_rows, 128), full_type),
            pltpu.VMEM((tok_rows, 128), full_type),
            *(pltpu.VMEM(array.shape, array.dtype) for array in inputs),
            pltpu.VMEM((tail, inner), half_type),
            pltpu.VMEM((tail, wide), half_type),
            pltpu.VMEM((tail, wide), half_type),
            pltpu.VMEM((tail, pool), half_type),
            pltpu.VMEM((tail + tok_rows, inner), full_type),
            pltpu.VMEM((tail + tok_rows, 2 * wide), full_type),
            pltpu.VMEM((8 + tail + tok_rows, pool), full_type),
            pltpu.VMEM((8 + tail + tok_rows, POOL_GROUP), full_type),
            pltpu.VMEM((8 + tail + tok_rows, POOL_GROUP), full_type),
            pltpu.VMEM((blocks, 2 * BLOCK, inner), half_type),
            pltpu.VMEM((tok_rows, 2 * wide), half_type),
            pltpu.VMEM((blocks * groups, STATE, BLOCK), half_type),
            pltpu.VMEM((blocks, 128, BLOCK), full_type),
            pltpu.VMEM((blocks, BLOCK, 128), full_type),
            pltpu.VMEM((tok_rows, inner), full_type),
            pltpu.VMEM((tok_rows, inner), full_type),
            pltpu.VMEM((blocks, STATE, inner), full_type),
            pltpu.VMEM((STATE, inner), full_type),
            pltpu.VMEM((STATE, inner), full_type),
            pltpu.VMEM((CHAINS, STATE, inner // CHAINS), half_type),
            pltpu.VMEM((CHAINS, STATE, inner // CHAINS), half_type),
            pltpu.VMEM((tok_rows, inner + pool), half_type),
            pltpu.VMEM((tok_rows, inner + pool), half_type),
        ],
        compiler_params=pltpu.CompilerParams(
            collective_id=0, has_side_effects=True, vmem_limit_bytes=48 * 2**20
        ),
        name="paired_mixers",
    )(*(pltpu.with_memory_space_constraint(array, pltpu.HBM) for array in (*inputs, ssd_weight, pool_rows)))


def causal_taps(input_rows, prior_rows, tap_weights, offset_bias):
    padded = jnp.concatenate([prior_rows, input_rows], axis=0).astype(jnp.float32)
    tok_rows = input_rows.shape[0]
    running = jnp.zeros(input_rows.shape, jnp.float32) + offset_bias
    for tap_index in range(tap_weights.shape[0]):
        running = (
            running
            + tap_weights[tap_index].astype(jnp.float32) * padded[tap_index : tap_index + tok_rows]
        )
    return jax.nn.silu(running).astype(jnp.bfloat16)


def pool_mix(input_rows, prior_rows, positions, group_ids, local_weight, local_scale):
    tail_rows = prior_rows.shape[0]
    tok_rows = input_rows.shape[0]
    padded = jnp.concatenate([prior_rows, input_rows], axis=0).astype(jnp.float32)
    window_reach = jnp.left_shift(jnp.int32(2), group_ids)
    running = jnp.zeros(input_rows.shape, jnp.float32)
    for offset_back in range(tail_rows + 1):
        start_row = tail_rows - offset_back
        running = running + padded[start_row : start_row + tok_rows] * (
            offset_back < window_reach
        ).astype(jnp.float32)
    window_count = jnp.minimum(positions[:, None] + 1.0, window_reach.astype(jnp.float32)[None, :])
    pooled = (running / window_count - input_rows.astype(jnp.float32)).astype(jnp.bfloat16)
    grouped = pooled.reshape(tok_rows, local_weight.shape[0], local_weight.shape[1])
    mixed = jnp.einsum("lgc,gcd->lgd", grouped, local_weight, preferred_element_type=jnp.float32)
    return (mixed.reshape(input_rows.shape) * local_scale.astype(jnp.float32)).astype(jnp.bfloat16)


def join_states(earlier, later_part):
    return (
        earlier[0] + later_part[0],
        earlier[1] * jnp.exp(later_part[0])[..., None, None] + later_part[1],
    )


def body(
    statespace_input,
    output_gate_input,
    state_input_projection,
    state_output_projection,
    step_size_input,
    added_log_decay,
    logarithm_rates,
    head_channel_taps,
    input_projection_taps,
    output_projection_taps,
    input_projection_bias,
    group_norm_gain,
    pooling_input,
    pooling_group_weight,
    pooling_channel_scale,
    statespace_output_weight,
    pooling_output_weight,
    output_norm_gain,
):
    core_count = lax.axis_size("tp")
    sp_size, fs_size = lax.axis_size("sp"), lax.axis_size("fs")
    pool_tail = 2**POOL_GROUPS - 1
    paired = (
        statespace_output_weight.shape[1] % 128 == 0
        and fs_size == 4
        and core_count == 2
        and sp_size in (4, 8)
    )
    if paired:
        return mixed_and_projected(
            (
                statespace_input,
                output_gate_input,
                state_input_projection,
                state_output_projection,
                jnp.swapaxes(step_size_input, 1, 2),
                jnp.swapaxes(added_log_decay, 1, 2),
                logarithm_rates[None],
                head_channel_taps,
                input_projection_taps,
                output_projection_taps,
                pooling_input,
                pooling_group_weight,
            ),
            {
                "out": output_norm_gain,
                "gain": group_norm_gain,
                "scale": pooling_channel_scale,
                "bias": input_projection_bias,
            },
            statespace_output_weight,
            pooling_output_weight,
            pool_tail + 1,
        )
    core_index = lax.axis_index("tp")
    seq_index = lax.axis_index("sp")
    head_channel_rows = statespace_input[0]
    output_gate_rows = output_gate_input[0]
    input_projection_rows = state_input_projection[0]
    output_projection_rows = state_output_projection[0]
    step_size_rows = step_size_input[0]
    decay_spikes = added_log_decay[0]
    pooling_rows = pooling_input[0]
    tok_rows = head_channel_rows.shape[0]
    inner_local = head_channel_rows.shape[1]
    heads_local = step_size_rows.shape[1]
    state_local = input_projection_rows.shape[1]
    pool_local = pooling_rows.shape[1]
    groups_local = state_local // STATE
    per_group = heads_local // groups_local
    groups_pool = pool_local // POOL_GROUP
    conv_tail = CONV - 1
    own_columns = jnp.concatenate([statespace_output_weight, pooling_output_weight], axis=0)
    tails = jnp.concatenate(
        [
            jnp.pad(rows[tok_rows - tail :], ((pool_tail - tail, 0), (0, 0)))
            for rows, tail in (
                (head_channel_rows, conv_tail),
                (input_projection_rows, conv_tail),
                (output_projection_rows, conv_tail),
                (pooling_rows, pool_tail),
            )
        ],
        axis=1,
    )
    prior = passed_along(tails, "sp", 1)
    widths = (inner_local, state_local, state_local, pool_local)
    prior_x, prior_b, prior_c, prior_pool = (
        prior[pool_tail - tail :, sum(widths[:at]) : sum(widths[: at + 1])]
        for at, tail in enumerate((conv_tail, conv_tail, conv_tail, pool_tail))
    )
    taps_x = lax.dynamic_slice_in_dim(head_channel_taps, core_index * inner_local, inner_local, 1)
    taps_b = lax.dynamic_slice_in_dim(
        input_projection_taps, core_index * state_local, state_local, 1
    )
    taps_c = lax.dynamic_slice_in_dim(
        output_projection_taps, core_index * state_local, state_local, 1
    )
    bias_b = lax.dynamic_slice_in_dim(
        input_projection_bias, core_index * state_local, state_local, 0
    )
    gain_ssd = lax.dynamic_slice_in_dim(group_norm_gain, core_index * inner_local, inner_local, 0)
    head_decay_rates = jnp.exp(
        lax.dynamic_slice_in_dim(logarithm_rates, core_index * heads_local, heads_local, 0)
    )
    gain_pool = lax.dynamic_slice_in_dim(
        pooling_channel_scale, core_index * pool_local, pool_local, 0
    )
    weight_pool = lax.dynamic_slice_in_dim(
        pooling_group_weight, core_index * groups_pool, groups_pool, 0
    )
    whole_columns = lax.all_gather(own_columns, ("sp", "fs"), axis=1, tiled=True)
    x_conv = causal_taps(head_channel_rows, prior_x, taps_x, 0.0)
    b_conv = causal_taps(input_projection_rows, prior_b, taps_b, bias_b.astype(jnp.float32))
    c_conv = causal_taps(output_projection_rows, prior_c, taps_c, 0.0)
    blocks = tok_rows // BLOCK
    discrete_step_size = jax.nn.softplus(step_size_rows.astype(jnp.float32))
    logarithm_decay = -discrete_step_size * head_decay_rates + decay_spikes
    cumulative_decay = jnp.cumsum(
        logarithm_decay.reshape(blocks, BLOCK, groups_local, per_group), axis=1
    )
    cum_t = cumulative_decay.transpose(0, 2, 3, 1)
    step_t = discrete_step_size.reshape(blocks, BLOCK, groups_local, per_group).transpose(
        0, 2, 3, 1
    )
    heads_x = x_conv.reshape(blocks, BLOCK, groups_local, per_group, HEAD_DIM)
    group_b = b_conv.reshape(blocks, BLOCK, groups_local, STATE)
    group_c = c_conv.reshape(blocks, BLOCK, groups_local, STATE)
    scores = jnp.einsum("ktgn,kugn->kgtu", group_c, group_b, preferred_element_type=jnp.float32)
    causal = jnp.arange(BLOCK)[:, None] >= jnp.arange(BLOCK)[None, :]
    decay_gap = cum_t[..., :, None] - cum_t[..., None, :]
    decay_factor = jnp.where(causal, jnp.exp(jnp.where(causal, decay_gap, 0.0)), 0.0)
    weights = (scores[:, :, None] * decay_factor * step_t[..., None, :]).astype(jnp.bfloat16)
    within = jnp.einsum("kgetu,kugep->ktgep", weights, heads_x, preferred_element_type=jnp.float32)
    block_end = cum_t[..., -1]
    end_weight = jnp.exp(block_end[..., None] - cum_t) * step_t
    scaled_x = (heads_x * end_weight.transpose(0, 3, 1, 2)[..., None]).astype(jnp.bfloat16)
    block_state = jnp.einsum(
        "kugep,kugn->kgepn", scaled_x, group_b, preferred_element_type=jnp.float32
    )

    def local_chain(state_now, current_inputs):
        piece_state, piece_fall = current_inputs
        return (state_now * jnp.exp(piece_fall)[..., None, None] + piece_state, state_now)

    final_state, local_entering = lax.scan(
        local_chain, jnp.zeros(block_state.shape[1:], jnp.float32), (block_state, block_end)
    )
    log_total = jnp.sum(block_end, axis=0)
    prefix_log = jnp.cumsum(block_end, axis=0) - block_end
    log_before, state_before = entering_2(
        (log_total, final_state),
        "sp",
        join_states,
        (jnp.zeros_like(log_total), jnp.zeros_like(final_state)),
    )
    entering = (local_entering + jnp.exp(prefix_log)[..., None, None] * state_before[None]).astype(
        jnp.bfloat16
    )
    carried_out = jnp.einsum(
        "ktgn,kgepn->ktgep", group_c, entering, preferred_element_type=jnp.float32
    )
    carried_out = carried_out * jnp.exp(cumulative_decay)[..., None]
    mixed_ssd = (within + carried_out).reshape(tok_rows, inner_local) * jax.nn.silu(
        output_gate_rows.astype(jnp.float32)
    )
    grouped = mixed_ssd.reshape(tok_rows, groups_local, inner_local // groups_local)
    normed = grouped * lax.rsqrt(jnp.mean(grouped * grouped, axis=-1, keepdims=True) + eps)
    ssd_out = (normed.reshape(tok_rows, inner_local) * gain_ssd.astype(jnp.float32)).astype(
        jnp.bfloat16
    )
    positions = (seq_index * tok_rows + jnp.arange(tok_rows, dtype=jnp.int32)).astype(jnp.float32)
    group_ids = core_index * groups_pool + jnp.arange(pool_local, dtype=jnp.int32) // POOL_GROUP
    pool_out = pool_mix(pooling_rows, prior_pool, positions, group_ids, weight_pool, gain_pool)
    channels = jnp.concatenate([ssd_out, pool_out], axis=1)
    half_width = D // core_count
    gain_out = lax.dynamic_slice_in_dim(
        output_norm_gain, core_index * half_width, half_width, 0
    ).astype(jnp.float32)
    partial = jnp.dot(channels, whole_columns, preferred_element_type=jnp.float32).astype(
        jnp.bfloat16
    )
    own_half = lax.dynamic_slice_in_dim(partial, core_index * half_width, half_width, 1).astype(
        jnp.float32
    )
    for hop in range(1, core_count):
        target = lax.rem(core_index + hop, core_count)
        leaving = lax.dynamic_slice_in_dim(partial, target * half_width, half_width, 1)
        route = [(i, (i + hop) % core_count) for i in range(core_count)]
        own_half = own_half + lax.ppermute(leaving, "tp", route).astype(jnp.float32)
    row_squares = lax.psum(jnp.sum(own_half * own_half, axis=1), "tp")
    result = own_half * lax.rsqrt(row_squares / D + eps)[:, None] * gain_out
    return result.astype(jnp.bfloat16)[None]


def solution(mesh):
    in_specs = (
        P("fs", "sp", "tp"),
        P("fs", "sp", "tp"),
        P("fs", "sp", "tp"),
        P("fs", "sp", "tp"),
        P("fs", "sp", "tp"),
        P("fs", "sp", "tp"),
        P(),
        P(),
        P(),
        P(),
        P(),
        P(),
        P("fs", "sp", "tp"),
        P(),
        P(),
        P("tp", ("sp", "fs")),
        P("tp", ("sp", "fs")),
        P(),
    )
    out_specs = P("fs", "sp", "tp")
    return jax.shard_map(body, mesh=mesh, in_specs=in_specs, out_specs=out_specs, check_vma=False)
```

```python
import functools

import jax
import jax.numpy as jnp
from jax import lax
from jax.experimental import pallas as pl
from jax.experimental.pallas import tpu as pltpu
from jax.sharding import PartitionSpec as P

D = 4096
HEAD_DIM = 64
STATE = 128
CONV = 4
BLOCK = 128
POOL_GROUPS = 4
POOL_GROUP = 256


eps = 1e-06


def passed_along(block, axis, distance):
    devices = range(lax.axis_size(axis))
    route = [(i - distance, i) for i in devices if i - distance in devices]
    return lax.ppermute(block, axis, route)


def entering_2(array, axis, join, neutral):
    place = lax.axis_index(axis)
    gathered = jax.tree.map(
        lambda a, kind: lax.all_gather(a.astype(kind), axis), array, (jnp.bfloat16, jnp.bfloat16)
    )
    state = jax.tree.map(lambda a, e: jnp.zeros_like(a) + jnp.asarray(e, a.dtype), array, neutral)

    def one(lap, state):
        return join(
            state,
            jax.tree.map(
                lambda a, own: lax.dynamic_index_in_dim(a, lap, 0, False).astype(own.dtype),
                gathered,
                array,
            ),
        )

    return lax.fori_loop(0, place, one, state)


MESH_IDS = pl.DeviceIdType.MESH
EXACT = lax.Precision.HIGHEST
CHUNKS, CHAINS = 6, 4
NAMES = ("out", "gain", "scale", "bias")
INPUTS, GATE, VECTORS = 16, 1, 12
SOURCES, OTHERS = (0, 2, 3, 10), (4, 5, 6, 7, 8, 9, 11, 12, 13, 14, 15)


class Links:
    def __init__(self, sp_size, fs_size):
        self.n = sp_size
        self.z = lax.axis_index("sp")
        self.fs = lax.axis_index("fs")
        self.core = lax.axis_index("tp")
        self.x = lax.rem(self.fs, 2)
        self.y = self.fs // 2
        self.beside = {"fs": self.fs + 1 - 2 * self.x}
        self.across = {"fs": self.fs + 2 - 4 * self.y}
        self.sibling = {"tp": 1 - self.core}

    def barrier(self):
        barrier = pltpu.get_barrier_semaphore()
        near = [{"sp": lax.rem(self.z + far, self.n)} for far in (1, self.n - 1)]
        for other in (*near, self.beside, self.across, self.sibling):
            pl.semaphore_signal(barrier, inc=1, device_id=other, device_id_type=MESH_IDS)
        pl.semaphore_wait(barrier, len(near) + 3)

    def within(self, place):
        return jnp.logical_and(place >= 0, place < self.n)

    def nearest(self, turn):
        if turn == 0:
            return self.z
        low, high = self.z, self.n - 1 - self.z
        small = jnp.minimum(low, high)
        both = turn <= 2 * small
        far = jnp.where(both, (turn + 1) // 2, turn - small)
        sign = jnp.where(both, 1 - 2 * (turn % 2), jnp.where(high > low, 1, -1))
        return self.z + sign * far


def remote(src, dst, sends, arrivals, spot, device):
    return pltpu.make_async_remote_copy(
        src_ref=src,
        dst_ref=dst,
        send_sem=sends.at[spot],
        recv_sem=arrivals.at[spot],
        device_id=device,
        device_id_type=MESH_IDS,
    )


class Weights:
    def __init__(self, links, whole, width, z_sems, y_sems):
        self.links, self.whole, self.width = links, whole, width
        self.z_sems, self.y_sems = z_sems, y_sems
        self.rows = whole.shape[0] // CHUNKS
        self.direct = range(CHUNKS - 1)
        self.turned = (CHUNKS - 1,)
        self.sent = {}

    def region(self, chunk, z, y):
        at = pl.multiple_of((z * 2 + y) * self.width, self.width)
        return self.whole.at[pl.ds(chunk * self.rows, self.rows), pl.ds(at, self.width)]

    def along(self, chunk, step, way, side, arriving):
        links = self.links
        origin = links.z - way * (step if arriving else step - 1)
        y = links.y if side == 0 else 1 - links.y
        spot = ((chunk * (links.n - 1) + step - 1) * 2 + (way < 0)) * 2 + side
        place = self.region(chunk, jnp.clip(origin, 0, links.n - 1), y)
        copy = remote(place, place, *self.z_sems, spot, {"sp": links.z + way})
        far = links.z if arriving else links.z + way
        return copy, jnp.logical_and(links.within(origin), links.within(far))

    def over(self, chunk, offset, arriving):
        links = self.links
        y = 1 - links.y if arriving else links.y
        origin = links.z + offset
        place = self.region(chunk, jnp.clip(origin, 0, links.n - 1), y)
        spot = chunk * (2 * links.n - 1) + offset + links.n - 1
        copy = remote(place, place, *self.y_sems, spot, links.across)
        return copy, links.within(origin)

    def go(self, kind, *key):
        copy, here = kind(*key, False)
        self.sent[kind.__name__, key] = kind
        pl.when(here)(copy.start)

    def take(self, kind, *key):
        copy, here = kind(*key, True)
        pl.when(here)(copy.wait_recv)

    def pass_on(self, chunk, step, way, side):
        if step < self.links.n and not self.single(step, way, side):
            self.go(self.along, chunk, step, way, side)

    def single(self, step, way, side):
        return step >= self.links.n - 2 and way == 1 and side == 1

    def begin(self):
        for chunk in (*self.turned, *self.direct):
            self.go(self.over, chunk, 0)

    def own(self, chunks, sides=(0,), ways=(1, -1)):
        for chunk in chunks:
            for side in sides:
                for way in ways:
                    self.pass_on(chunk, 1, way, side)

    def turn(self):
        for chunk in self.turned:
            self.take(self.over, chunk, 0)

    def hop(self, step, chunks, sides=(0,), ways=(1, -1)):
        for chunk in chunks:
            for way in ways:
                for side in sides:
                    if not self.single(step, way, side):
                        self.take(self.along, chunk, step, way, side)
                        self.pass_on(chunk, step + 1, way, side)
                if chunk in self.direct or (0 in sides and self.single(step, way, 1)):
                    self.go(self.over, chunk, -way * step)

    def settle(self, step):
        for chunk in self.direct:
            for offset in (0,) if step == 0 else (step, -step):
                self.take(self.over, chunk, offset)
        if self.single(step, 1, 1):
            for chunk in self.turned:
                self.take(self.over, chunk, -step)

    def finish(self):
        for (_, key), kind in self.sent.items():
            copy, here = kind(*key, False)
            pl.when(here)(copy.wait_send)


def silu(rows):
    return rows / (1.0 + jnp.exp(-rows))


def softplus(rows):
    return jnp.maximum(rows, 0.0) + jnp.log(1.0 + jnp.exp(-jnp.abs(rows)))


def piece(vector, offset, size):
    at = pl.multiple_of(offset, 128)
    return vector[pl.ds(at, size)].astype(jnp.float32)[None]


def chosen(core, options):
    best = options[0]
    for at in range(1, len(options)):
        best = jnp.where(core == at, options[at], best)
    return best


def mixers(links, tail, cores, vectors, fetches, refs, sems):
    (x_in, gate, b_in, c_in, dt, added, rates, x_taps, b_taps, c_taps, pool_in,
     pool_weight, prior_x, prior_b, prior_c, prior_pool, x_pad, bc_pad, pool_pad,
     pool_two, pool_four, x_split, bc_conv, b_turned, flat, upright, within, grown, local_in,
     state, before, carry_in, carry_out, channels, far_channels) = refs
    sends, arrivals = sems
    rows, inner = x_in.shape[1:]
    heads = dt.shape[1]
    wide = b_in.shape[2]
    pool = pool_in.shape[2]
    groups = wide // STATE
    span = inner // groups
    blocks = rows // BLOCK
    z, core = links.z, links.core
    lead = 8
    parts = CHAINS
    length = inner // parts
    sources = ((x_in, prior_x), (b_in, prior_b), (c_in, prior_c), (pool_in, prior_pool))

    def tails(at):
        source, target = sources[at]
        return remote(
            source.at[0, pl.ds(rows - tail, tail)], target, sends, arrivals, at, {"sp": z + 1}
        )

    def chain(group):
        return remote(
            carry_out.at[group], carry_in.at[group], sends, arrivals, 4 + group, {"sp": z + 1}
        )

    def pool_letter():
        cols = pl.ds(inner, pool)
        return remote(
            channels.at[:, cols], far_channels.at[:, cols], sends, arrivals, 4 + parts, links.beside
        )

    def block_letter(at):
        place = (pl.ds(at * BLOCK, BLOCK), pl.ds(0, inner))
        return remote(
            channels.at[place], far_channels.at[place], sends, arrivals, 5 + parts + at, links.beside
        )

    follows = z + 1 < links.n
    yield "loaded"
    for at in SOURCES:
        fetches[at].wait()

    @pl.when(follows)
    def _():
        for at in range(4):
            tails(at).start()

    yield "start"
    for at in OTHERS:
        fetches[at].wait()
    x_pad[tail:] = x_in[0].astype(jnp.float32)
    bc_pad[tail:, 0:wide] = b_in[0].astype(jnp.float32)
    bc_pad[tail:, wide:] = c_in[0].astype(jnp.float32)
    pool_pad[0:lead] = jnp.zeros((lead, pool), jnp.float32)
    pool_pad[lead + tail :] = pool_in[0].astype(jnp.float32)
    steps_flat = softplus(dt[0].astype(jnp.float32))
    table = (heads, rates.shape[1])
    picked = lax.broadcasted_iota(jnp.int32, table, 1) == (
        core * heads + lax.broadcasted_iota(jnp.int32, table, 0)
    )
    own_rates = jnp.sum(
        jnp.where(picked, jnp.broadcast_to(rates[...], table), 0.0), axis=1, keepdims=True
    )
    logs_flat = -steps_flat * jnp.exp(own_rates) + added[0]
    flat[...] = jnp.zeros_like(flat)
    down = lax.broadcasted_iota(jnp.int32, (BLOCK, BLOCK), 0)
    over = lax.broadcasted_iota(jnp.int32, (BLOCK, BLOCK), 1)
    causal = down >= over
    upper = (down <= over).astype(jnp.float32)
    first_half = lax.broadcasted_iota(jnp.int32, (BLOCK, 2 * HEAD_DIM), 1) < HEAD_DIM

    def mine(ref, size):
        at = pl.multiple_of(core * size, size)
        return ref[:, pl.ds(at, size)].astype(jnp.float32)

    taps_x = mine(x_taps, inner)
    taps_bc = jnp.concatenate([mine(b_taps, wide), mine(c_taps, wide)], axis=1)
    bias_b = piece(vectors["bias"], core * wide, wide)
    bias_bc = jnp.concatenate([bias_b, jnp.zeros_like(bias_b)], axis=1)

    @pl.when(z == 0)
    def _():
        x_pad[0:tail] = jnp.zeros((tail, inner), jnp.float32)
        bc_pad[0:tail] = jnp.zeros((tail, 2 * wide), jnp.float32)
        pool_pad[lead : lead + tail] = jnp.zeros((tail, pool), jnp.float32)

    @pl.when(z > 0)
    def _():
        for at in range(4):
            tails(at).wait_recv()
        x_pad[0:tail] = prior_x[...].astype(jnp.float32)
        bc_pad[0:tail, 0:wide] = prior_b[...].astype(jnp.float32)
        bc_pad[0:tail, wide:] = prior_c[...].astype(jnp.float32)
        pool_pad[lead : lead + tail] = prior_pool[...].astype(jnp.float32)

    def taps(pad, weights, at, cols):
        total = None
        for tap in range(CONV):
            begin = at * BLOCK + tail - CONV + 1 + tap
            term = pad[begin : begin + BLOCK, cols] * weights[tap : tap + 1, cols]
            total = term if total is None else total + term
        return total

    def spread(narrow, head):
        shape = (BLOCK, 2 * HEAD_DIM)
        return jnp.where(
            first_half,
            jnp.broadcast_to(narrow[:, head : head + 1], shape),
            jnp.broadcast_to(narrow[:, head + 1 : head + 2], shape),
        )

    pairs = span // (2 * HEAD_DIM)
    ends = []
    state[...] = jnp.zeros_like(state)
    for at in range(blocks):
        now = slice(at * BLOCK, (at + 1) * BLOCK)
        bc_conv[now] = silu(taps(bc_pad, taps_bc, at, slice(0, 2 * wide)) + bias_bc).astype(
            jnp.bfloat16
        )
        flat[at, 0:heads] = jnp.dot(
            logs_flat[:, now], upper, precision=EXACT, preferred_element_type=jnp.float32
        )
        flat[at, heads : 2 * heads] = steps_flat[:, now]
        upright[at] = jnp.transpose(flat[at])
        cum = upright[at, :, 0:heads]
        decayed = jnp.exp(cum)
        closing = jnp.exp(cum[BLOCK - 1 : BLOCK] - cum) * upright[at, :, heads : 2 * heads]
        ended = []
        for group in range(groups):
            cols = slice(group * span, (group + 1) * span)
            x_now = silu(taps(x_pad, taps_x, at, cols))
            b_now = bc_conv[now, group * STATE : (group + 1) * STATE]
            b_flat = jnp.transpose(b_now.astype(jnp.float32)).astype(jnp.bfloat16)
            b_turned[at * groups + group] = b_flat
            scaled = []
            for pair in range(pairs):
                head = group * (span // HEAD_DIM) + 2 * pair
                lanes = slice(pair * 2 * HEAD_DIM, (pair + 1) * 2 * HEAD_DIM)
                here = slice(head * HEAD_DIM, (head + 2) * HEAD_DIM)
                x_pair = x_now[:, lanes]
                x_split[at, 0:BLOCK, here] = jnp.where(first_half, x_pair, 0.0).astype(jnp.bfloat16)
                x_split[at, BLOCK : 2 * BLOCK, here] = jnp.where(first_half, 0.0, x_pair).astype(
                    jnp.bfloat16
                )
                x_half = x_pair.astype(jnp.bfloat16).astype(jnp.float32)
                scaled.append((x_half * spread(closing, head)).astype(jnp.bfloat16))
                grown[now, here] = spread(decayed, head)
            end = grown[(at + 1) * BLOCK - 1 : (at + 1) * BLOCK, cols]
            ended.append(end)
            local_in[at, :, cols] = state[:, cols]
            state[:, cols] = state[:, cols] * end + jnp.dot(
                b_flat, jnp.concatenate(scaled, axis=1), preferred_element_type=jnp.float32
            )
        yield at
        ends.append(ended)

    def hand_on():
        @pl.when(z == 0)
        def _():
            before[...] = jnp.zeros_like(before)

        for link in range(parts):
            cols = slice(link * length, (link + 1) * length)
            group, at_end = link * length // span, slice(link * length % span, link * length % span + length)

            @pl.when(z > 0)
            def _(link=link, cols=cols):
                chain(link).wait_recv()
                before[:, cols] = carry_in[link].astype(jnp.float32)

            @pl.when(follows)
            def _(link=link, cols=cols, group=group, at_end=at_end):
                falling = ends[0][group][:, at_end]
                for at in range(1, blocks):
                    falling = falling * ends[at][group][:, at_end]
                carry_out[link] = (before[:, cols] * falling + state[:, cols]).astype(jnp.bfloat16)
                chain(link).start()

    def chain_point(place, last=False):
        pl.when(z >= place if last else z == place)(hand_on)

    chain_point(0)
    yield "states"
    place = z * rows
    position = (place + lax.broadcasted_iota(jnp.int32, (rows, 1), 0)).astype(jnp.float32) + 1.0
    pool_groups = pool // POOL_GROUP
    for group in range(pool_groups):
        cols = slice(group * POOL_GROUP, (group + 1) * POOL_GROUP)
        size = rows + tail
        two = pool_pad[lead:, cols] + pool_pad[lead - 1 : lead - 1 + size, cols]
        pool_two[0:lead] = jnp.zeros((lead, POOL_GROUP), jnp.float32)
        pool_two[lead:] = two
        four = two + pool_two[lead - 2 : lead - 2 + size]
        pool_four[0:lead] = jnp.zeros((lead, POOL_GROUP), jnp.float32)
        pool_four[lead:] = four
        eight = four + pool_four[lead - 4 : lead - 4 + size]
        sixteen = eight[tail:] + eight[tail - 8 : size - 8]
        sums = [two[tail:], four[tail:], eight[tail:], sixteen]
        picks = [c * pool_groups + group for c in range(cores)]
        running = chosen(core, [sums[pick] for pick in picks])
        reach = chosen(core, [jnp.float32(2 ** (pick + 1)) for pick in picks])
        pooled = running / jnp.minimum(position, reach) - pool_in[0, :, cols].astype(jnp.float32)
        mixed = jnp.dot(
            pooled.astype(jnp.bfloat16),
            pool_weight[core * pool_groups + group],
            preferred_element_type=jnp.float32,
        )
        scale = piece(vectors["scale"], core * pool + group * POOL_GROUP, POOL_GROUP)
        out = inner + group * POOL_GROUP
        channels[:, out : out + POOL_GROUP] = (mixed * scale).astype(jnp.bfloat16)
    pool_letter().start()
    for at in range(blocks):
        now = slice(at * BLOCK, (at + 1) * BLOCK)
        cum = upright[at, :, 0:heads]
        cum_flat = flat[at, 0:heads]
        step_flat = flat[at, heads : 2 * heads]
        for group in range(groups):
            c_now = bc_conv[now, wide + group * STATE : wide + (group + 1) * STATE]
            scores = jnp.dot(
                c_now, b_turned[at * groups + group], preferred_element_type=jnp.float32
            )
            for pair in range(pairs):
                first = group * (span // HEAD_DIM) + 2 * pair
                both = []
                for head in (first, first + 1):
                    gap = cum[:, head : head + 1] - cum_flat[head : head + 1]
                    decay = jnp.exp(jnp.where(causal, gap, -1e30))
                    both.append((scores * decay * step_flat[head : head + 1]).astype(jnp.bfloat16))
                here = slice(first * HEAD_DIM, (first + 2) * HEAD_DIM)
                within[now, here] = jnp.dot(
                    jnp.concatenate(both, axis=1),
                    x_split[at, :, here],
                    preferred_element_type=jnp.float32,
                )
    chain_point(1)
    yield "second"
    chain_point(2)
    yield "third"
    chain_point(3, True)
    falling = [None] * groups
    fetches[GATE].wait()
    for at in range(blocks):
        now = slice(at * BLOCK, (at + 1) * BLOCK)
        for group in range(groups):
            cols = slice(group * span, (group + 1) * span)
            earlier = before[:, cols]
            if at:
                earlier = earlier * falling[group]
            entering = local_in[at, :, cols] + earlier
            c_now = bc_conv[now, wide + group * STATE : wide + (group + 1) * STATE]
            carried = jnp.dot(
                c_now, entering.astype(jnp.bfloat16), preferred_element_type=jnp.float32
            )
            mixed = (within[now, cols] + carried * grown[now, cols]) * silu(
                gate[0, now, cols].astype(jnp.float32)
            )
            root = lax.rsqrt(jnp.mean(mixed * mixed, axis=1, keepdims=True) + eps)
            gain = piece(vectors["gain"], core * inner + group * span, span)
            channels[now, cols] = (mixed * root * gain).astype(jnp.bfloat16)
            end = ends[at][group]
            falling[group] = end if at == 0 else falling[group] * end
        block_letter(at).start()
    letters = [pool_letter(), *(block_letter(at) for at in range(blocks))]

    def received():
        for letter in letters:
            letter.wait_recv()

    def finish():
        for letter in letters:
            letter.wait_send()

        @pl.when(follows)
        def _():
            for at in range(4):
                tails(at).wait_send()
            for link in range(parts):
                chain(link).wait_send()

    return received, finish


def whole_kernel(sp_size, fs_size, cores, tail, *refs):
    inputs, ssd_weight, pool_rows, out = refs[:INPUTS], *refs[INPUTS : INPUTS + 3]
    (z_sends, z_arrivals, y_sends, y_arrivals, m_sends, m_arrivals, p_sends, p_arrivals, o_sends,
     o_arrivals, local_sems, whole, parts, part_in, returned, return_in, squares, squares_in,
     *rest) = refs[INPUTS + 3 :]
    held, rest = rest[:INPUTS], rest[INPUTS:]
    vectors = dict(zip(NAMES, held[VECTORS:]))
    held = held[:VECTORS]
    channels, far_channels = rest[-2:]
    links = Links(sp_size, fs_size)
    width = ssd_weight.shape[1]
    inner = ssd_weight.shape[0]
    rows = channels.shape[0]
    half = sp_size // cores
    core = links.core
    own_at = pl.multiple_of((links.z * 2 + links.y) * width, width)
    loads = [
        pltpu.make_async_copy(
            source, whole.at[pl.ds(begin, source.shape[0]), pl.ds(own_at, width)], local_sems.at[at]
        )
        for at, (source, begin) in enumerate(((ssd_weight, 0), (pool_rows, inner)))
    ]
    fetches = [
        pltpu.make_async_copy(source, place, local_sems.at[2 + at])
        for at, (source, place) in enumerate(zip(inputs, (*held, *vectors.values())))
    ]
    for load in loads:
        load.start()
    for at in (*SOURCES, *OTHERS, GATE):
        fetches[at].start()
    links.barrier()
    weights = Weights(links, whole, width, (z_sends, z_arrivals), (y_sends, y_arrivals))
    work = mixers(links, tail, cores, vectors, fetches, (*held, *rest), (m_sends, m_arrivals))

    direct, turned = weights.direct, weights.turned
    both = (0, 1)
    last = sp_size - 1
    mixed = None
    while mixed is None:
        try:
            mark = next(work)
        except StopIteration as ended:
            mixed = ended.value
            break
        if mark == "loaded":
            for load in loads:
                load.wait()
            weights.begin()
            weights.own(direct[:3], ways=(-1,))
        elif mark == "start":
            weights.own(direct[:3], ways=(1,))
        elif mark == 1:
            weights.own(direct[3:4])
        elif mark == "states":
            weights.own(direct[4:])
            weights.turn()
            weights.own(turned, both, (-1,))
            pl.when(links.z == last)(lambda: weights.own(turned, both, (1,)))
            weights.hop(1, direct[:1], ways=(-1,))
        elif mark == "second":
            weights.hop(1, direct[1:3], ways=(-1,))
            pl.when(links.z == 1)(lambda: weights.own(turned, both, (1,)))
            pl.when(links.z == 1)(lambda: weights.hop(1, direct[:4], ways=(1,)))
            pl.when(links.z == last)(lambda: weights.hop(1, direct, ways=(1,)))
            inner_late = jnp.logical_and(links.z >= 2, links.z < last)
            pl.when(inner_late)(lambda: weights.hop(1, direct[:3], ways=(1,)))
        elif mark == "third":
            pl.when(inner_late)(lambda: weights.own(turned, both, (1,)))
            pl.when(inner_late)(lambda: weights.hop(1, direct[3:], ways=(1,)))
            pl.when(links.z == last)(lambda: weights.hop(2, direct[:2], ways=(1,)))
            pl.when(links.z >= 2)(lambda: weights.hop(1, direct[3:], ways=(-1,)))
    received, finish_mixers = mixed
    pl.when(links.z == 0)(lambda: weights.own(turned, both, (1,)))
    pl.when(links.z == 1)(lambda: weights.hop(1, direct[4:], ways=(1,)))
    pl.when(links.z <= 1)(lambda: weights.hop(1, direct[3:], ways=(-1,)))

    def multiply(turn, far, sides=both):
        z = links.nearest(turn)
        source = far_channels if far else channels

        @pl.loop(0, len(sides))
        def _(at):
            y = lax.rem(links.y + sides[0] + at, 2)
            slab = z * 2 + y
            lanes = pl.ds(pl.multiple_of(slab * width, width), width)
            parts[far, slab] = jnp.dot(
                source[...], whole[:, lanes], preferred_element_type=jnp.float32
            ).astype(jnp.bfloat16)

            @pl.when(z // half != core)
            def _():
                part_letter(z, y, far).start()

    def part_letter(z, y, far):
        slab = z * 2 + y
        return remote(
            parts.at[far, slab],
            part_in.at[far, lax.rem(z, half) * 2 + y],
            p_sends,
            p_arrivals,
            far * 2 * sp_size + slab,
            links.sibling,
        )

    def return_letter(slot):
        return remote(
            returned.at[slot], return_in.at[slot], o_sends, o_arrivals, slot, links.beside
        )

    def give_back(turn, sides=both):
        z = links.nearest(turn)

        @pl.when(z // half == core)
        def _():
            @pl.loop(0, len(sides))
            def _(at):
                y = lax.rem(links.y + sides[0] + at, 2)
                part_letter(z, y, 1).wait_recv()
                slot = lax.rem(z, half) * 2 + y
                returned[slot] = (
                    parts[1, z * 2 + y].astype(jnp.float32) + part_in[1, slot].astype(jnp.float32)
                ).astype(jnp.bfloat16)
                return_letter(slot).start()

    edge = jnp.logical_or(links.z == 0, links.z == last)
    weights.settle(0)
    multiply(0, 0)
    for step in range(1, last):
        weights.hop(step, turned, both)
        if step + 1 < last:
            if step == 1:
                pl.when(links.z == last)(lambda: weights.hop(2, direct[2:]))
                pl.when(links.z != last)(lambda: weights.hop(2, direct))
            else:
                weights.hop(step + 1, direct)
            weights.settle(step)
            multiply(step, 0)
    received()
    share = -(-len(direct) // last)

    def ahead(turn):
        multiply(turn, 1)
        give_back(turn)
        multiply(turn, 0)

    for turn in range(last):
        pieces_now = direct[turn * share : (turn + 1) * share]
        if turn == last - 1:
            pl.when(jnp.logical_not(edge))(lambda: ahead(turn))
            weights.settle(turn)
            weights.hop(last, pieces_now)
            pl.when(edge)(lambda: ahead(turn))
        else:
            multiply(turn, 1)
            weights.hop(last, pieces_now)
            give_back(turn)
    weights.hop(last, turned, (0,))
    multiply(last, 1, (0,))
    multiply(last, 0, (0,))
    give_back(last, (0,))
    weights.hop(last, turned, (1,))
    weights.settle(last)
    multiply(last, 1, (1,))
    multiply(last, 0, (1,))
    give_back(last, (1,))
    own_half = core * half
    slots = 2 * half

    def lane_squares(values):
        values = values * values
        total = values[:, 0:128]
        for at in range(1, width // 128):
            total = total + values[:, at * 128 : (at + 1) * 128]
        return total

    def own_total(slot):
        return parts[0, own_half * 2 + slot].astype(jnp.float32) + part_in[0, slot].astype(
            jnp.float32
        )

    squares[...] = jnp.zeros_like(squares)

    @pl.loop(0, slots)
    def _(slot):
        part_letter(own_half + slot // 2, lax.rem(slot, 2), 0).wait_recv()
        squares[...] += lane_squares(own_total(slot))

    @pl.loop(0, slots)
    def _(slot):
        return_letter(slot).wait_recv()
        squares[...] += lane_squares(return_in[slot].astype(jnp.float32))

    exchange = remote(squares, squares_in, o_sends, o_arrivals, slots, links.sibling)
    exchange.start()
    exchange.wait_recv()
    row_squares = jnp.sum(squares[...] + squares_in[...], axis=1, keepdims=True)
    features = cores * out.shape[2]
    root = lax.rsqrt(row_squares / features + eps)

    @pl.loop(0, slots)
    def _(slot):
        first = (slot // 2) * fs_size + 2 * lax.rem(slot, 2)
        for values, x in (
            (own_total(slot), links.x),
            (return_in[slot].astype(jnp.float32), 1 - links.x),
        ):
            at = pl.multiple_of((first + x) * width, width)
            gain = piece(vectors["out"], core * out.shape[2] + at, width)
            out[0, :, pl.ds(at, width)] = (values * root * gain).astype(jnp.bfloat16)

    exchange.wait_send()
    weights.finish()
    finish_mixers()

    @pl.loop(0, 2 * half)
    def _(slot):
        return_letter(slot).wait_send()
        other = (1 - core) * half
        for far in range(2):
            part_letter(other + slot // 2, lax.rem(slot, 2), far).wait_send()


def mixed_and_projected(inputs, vectors, ssd_weight, pool_rows, tail):
    sp_size, fs_size, cores = lax.axis_size("sp"), lax.axis_size("fs"), lax.axis_size("tp")
    width = ssd_weight.shape[1]
    x_in, b_in, pool_in = inputs[0], inputs[2], inputs[10]
    features = vectors["out"].shape[0]
    inputs = (*inputs, *(vectors[name] for name in NAMES))
    tok_rows, inner = x_in.shape[1:]
    wide, pool = b_in.shape[2], pool_in.shape[2]
    groups = wide // STATE
    blocks = tok_rows // BLOCK
    half = sp_size // cores
    slots = 2 * half
    vmem = pl.BlockSpec(memory_space=pltpu.VMEM)
    hbm = pl.BlockSpec(memory_space=pltpu.HBM)
    dma = pltpu.SemaphoreType.DMA
    half_type, full_type = jnp.bfloat16, jnp.float32
    z_spots, y_spots = CHUNKS * (sp_size - 1) * 4, CHUNKS * (2 * sp_size - 1)
    letters = 5 + CHAINS + blocks
    return pl.pallas_call(
        functools.partial(whole_kernel, sp_size, fs_size, cores, tail),
        out_shape=pltpu.VMEM((1, tok_rows, features // cores), half_type),
        in_specs=[hbm] * (len(inputs) + 2),
        out_specs=vmem,
        scratch_shapes=[
            dma((z_spots,)),
            dma((z_spots,)),
            dma((y_spots,)),
            dma((y_spots,)),
            dma((letters,)),
            dma((letters,)),
            dma((4 * sp_size,)),
            dma((4 * sp_size,)),
            dma((slots + 1,)),
            dma((slots + 1,)),
            dma((2 + len(inputs),)),
            pltpu.VMEM((inner + pool, width * 2 * sp_size), half_type),
            pltpu.VMEM((2, 2 * sp_size, tok_rows, width), half_type),
            pltpu.VMEM((2, slots, tok_rows, width), half_type),
            pltpu.VMEM((slots, tok_rows, width), half_type),
            pltpu.VMEM((slots, tok_rows, width), half_type),
            pltpu.VMEM((tok_rows, 128), full_type),
            pltpu.VMEM((tok_rows, 128), full_type),
            *(pltpu.VMEM(array.shape, array.dtype) for array in inputs),
            pltpu.VMEM((tail, inner), half_type),
            pltpu.VMEM((tail, wide), half_type),
            pltpu.VMEM((tail, wide), half_type),
            pltpu.VMEM((tail, pool), half_type),
            pltpu.VMEM((tail + tok_rows, inner), full_type),
            pltpu.VMEM((tail + tok_rows, 2 * wide), full_type),
            pltpu.VMEM((8 + tail + tok_rows, pool), full_type),
            pltpu.VMEM((8 + tail + tok_rows, POOL_GROUP), full_type),
            pltpu.VMEM((8 + tail + tok_rows, POOL_GROUP), full_type),
            pltpu.VMEM((blocks, 2 * BLOCK, inner), half_type),
            pltpu.VMEM((tok_rows, 2 * wide), half_type),
            pltpu.VMEM((blocks * groups, STATE, BLOCK), half_type),
            pltpu.VMEM((blocks, 128, BLOCK), full_type),
            pltpu.VMEM((blocks, BLOCK, 128), full_type),
            pltpu.VMEM((tok_rows, inner), full_type),
            pltpu.VMEM((tok_rows, inner), full_type),
            pltpu.VMEM((blocks, STATE, inner), full_type),
            pltpu.VMEM((STATE, inner), full_type),
            pltpu.VMEM((STATE, inner), full_type),
            pltpu.VMEM((CHAINS, STATE, inner // CHAINS), half_type),
            pltpu.VMEM((CHAINS, STATE, inner // CHAINS), half_type),
            pltpu.VMEM((tok_rows, inner + pool), half_type),
            pltpu.VMEM((tok_rows, inner + pool), half_type),
        ],
        compiler_params=pltpu.CompilerParams(
            collective_id=0, has_side_effects=True, vmem_limit_bytes=48 * 2**20
        ),
        name="paired_mixers",
    )(*(pltpu.with_memory_space_constraint(array, pltpu.HBM) for array in (*inputs, ssd_weight, pool_rows)))


def causal_taps(input_rows, prior_rows, tap_weights, offset_bias):
    padded = jnp.concatenate([prior_rows, input_rows], axis=0).astype(jnp.float32)
    tok_rows = input_rows.shape[0]
    running = jnp.zeros(input_rows.shape, jnp.float32) + offset_bias
    for tap_index in range(tap_weights.shape[0]):
        running = (
            running
            + tap_weights[tap_index].astype(jnp.float32) * padded[tap_index : tap_index + tok_rows]
        )
    return jax.nn.silu(running).astype(jnp.bfloat16)


def pool_mix(input_rows, prior_rows, positions, group_ids, local_weight, local_scale):
    tail_rows = prior_rows.shape[0]
    tok_rows = input_rows.shape[0]
    padded = jnp.concatenate([prior_rows, input_rows], axis=0).astype(jnp.float32)
    window_reach = jnp.left_shift(jnp.int32(2), group_ids)
    running = jnp.zeros(input_rows.shape, jnp.float32)
    for offset_back in range(tail_rows + 1):
        start_row = tail_rows - offset_back
        running = running + padded[start_row : start_row + tok_rows] * (
            offset_back < window_reach
        ).astype(jnp.float32)
    window_count = jnp.minimum(positions[:, None] + 1.0, window_reach.astype(jnp.float32)[None, :])
    pooled = (running / window_count - input_rows.astype(jnp.float32)).astype(jnp.bfloat16)
    grouped = pooled.reshape(tok_rows, local_weight.shape[0], local_weight.shape[1])
    mixed = jnp.einsum("lgc,gcd->lgd", grouped, local_weight, preferred_element_type=jnp.float32)
    return (mixed.reshape(input_rows.shape) * local_scale.astype(jnp.float32)).astype(jnp.bfloat16)


def join_states(earlier, later_part):
    return (
        earlier[0] + later_part[0],
        earlier[1] * jnp.exp(later_part[0])[..., None, None] + later_part[1],
    )


def body(
    statespace_input,
    output_gate_input,
    state_input_projection,
    state_output_projection,
    step_size_input,
    added_log_decay,
    logarithm_rates,
    head_channel_taps,
    input_projection_taps,
    output_projection_taps,
    input_projection_bias,
    group_norm_gain,
    pooling_input,
    pooling_group_weight,
    pooling_channel_scale,
    statespace_output_weight,
    pooling_output_weight,
    output_norm_gain,
):
    core_count = lax.axis_size("tp")
    sp_size, fs_size = lax.axis_size("sp"), lax.axis_size("fs")
    pool_tail = 2**POOL_GROUPS - 1
    paired = (
        statespace_output_weight.shape[1] % 128 == 0
        and fs_size == 4
        and core_count == 2
        and sp_size in (4, 8)
    )
    if paired:
        return mixed_and_projected(
            (
                statespace_input,
                output_gate_input,
                state_input_projection,
                state_output_projection,
                jnp.swapaxes(step_size_input, 1, 2),
                jnp.swapaxes(added_log_decay, 1, 2),
                logarithm_rates[None],
                head_channel_taps,
                input_projection_taps,
                output_projection_taps,
                pooling_input,
                pooling_group_weight,
            ),
            {
                "out": output_norm_gain,
                "gain": group_norm_gain,
                "scale": pooling_channel_scale,
                "bias": input_projection_bias,
            },
            statespace_output_weight,
            pooling_output_weight,
            pool_tail + 1,
        )
    core_index = lax.axis_index("tp")
    seq_index = lax.axis_index("sp")
    head_channel_rows = statespace_input[0]
    output_gate_rows = output_gate_input[0]
    input_projection_rows = state_input_projection[0]
    output_projection_rows = state_output_projection[0]
    step_size_rows = step_size_input[0]
    decay_spikes = added_log_decay[0]
    pooling_rows = pooling_input[0]
    tok_rows = head_channel_rows.shape[0]
    inner_local = head_channel_rows.shape[1]
    heads_local = step_size_rows.shape[1]
    state_local = input_projection_rows.shape[1]
    pool_local = pooling_rows.shape[1]
    groups_local = state_local // STATE
    per_group = heads_local // groups_local
    groups_pool = pool_local // POOL_GROUP
    conv_tail = CONV - 1
    own_columns = jnp.concatenate([statespace_output_weight, pooling_output_weight], axis=0)
    tails = jnp.concatenate(
        [
            jnp.pad(rows[tok_rows - tail :], ((pool_tail - tail, 0), (0, 0)))
            for rows, tail in (
                (head_channel_rows, conv_tail),
                (input_projection_rows, conv_tail),
                (output_projection_rows, conv_tail),
                (pooling_rows, pool_tail),
            )
        ],
        axis=1,
    )
    prior = passed_along(tails, "sp", 1)
    widths = (inner_local, state_local, state_local, pool_local)
    prior_x, prior_b, prior_c, prior_pool = (
        prior[pool_tail - tail :, sum(widths[:at]) : sum(widths[: at + 1])]
        for at, tail in enumerate((conv_tail, conv_tail, conv_tail, pool_tail))
    )
    taps_x = lax.dynamic_slice_in_dim(head_channel_taps, core_index * inner_local, inner_local, 1)
    taps_b = lax.dynamic_slice_in_dim(
        input_projection_taps, core_index * state_local, state_local, 1
    )
    taps_c = lax.dynamic_slice_in_dim(
        output_projection_taps, core_index * state_local, state_local, 1
    )
    bias_b = lax.dynamic_slice_in_dim(
        input_projection_bias, core_index * state_local, state_local, 0
    )
    gain_ssd = lax.dynamic_slice_in_dim(group_norm_gain, core_index * inner_local, inner_local, 0)
    head_decay_rates = jnp.exp(
        lax.dynamic_slice_in_dim(logarithm_rates, core_index * heads_local, heads_local, 0)
    )
    gain_pool = lax.dynamic_slice_in_dim(
        pooling_channel_scale, core_index * pool_local, pool_local, 0
    )
    weight_pool = lax.dynamic_slice_in_dim(
        pooling_group_weight, core_index * groups_pool, groups_pool, 0
    )
    whole_columns = lax.all_gather(own_columns, ("sp", "fs"), axis=1, tiled=True)
    x_conv = causal_taps(head_channel_rows, prior_x, taps_x, 0.0)
    b_conv = causal_taps(input_projection_rows, prior_b, taps_b, bias_b.astype(jnp.float32))
    c_conv = causal_taps(output_projection_rows, prior_c, taps_c, 0.0)
    blocks = tok_rows // BLOCK
    discrete_step_size = jax.nn.softplus(step_size_rows.astype(jnp.float32))
    logarithm_decay = -discrete_step_size * head_decay_rates + decay_spikes
    cumulative_decay = jnp.cumsum(
        logarithm_decay.reshape(blocks, BLOCK, groups_local, per_group), axis=1
    )
    cum_t = cumulative_decay.transpose(0, 2, 3, 1)
    step_t = discrete_step_size.reshape(blocks, BLOCK, groups_local, per_group).transpose(
        0, 2, 3, 1
    )
    heads_x = x_conv.reshape(blocks, BLOCK, groups_local, per_group, HEAD_DIM)
    group_b = b_conv.reshape(blocks, BLOCK, groups_local, STATE)
    group_c = c_conv.reshape(blocks, BLOCK, groups_local, STATE)
    scores = jnp.einsum("ktgn,kugn->kgtu", group_c, group_b, preferred_element_type=jnp.float32)
    causal = jnp.arange(BLOCK)[:, None] >= jnp.arange(BLOCK)[None, :]
    decay_gap = cum_t[..., :, None] - cum_t[..., None, :]
    decay_factor = jnp.where(causal, jnp.exp(jnp.where(causal, decay_gap, 0.0)), 0.0)
    weights = (scores[:, :, None] * decay_factor * step_t[..., None, :]).astype(jnp.bfloat16)
    within = jnp.einsum("kgetu,kugep->ktgep", weights, heads_x, preferred_element_type=jnp.float32)
    block_end = cum_t[..., -1]
    end_weight = jnp.exp(block_end[..., None] - cum_t) * step_t
    scaled_x = (heads_x * end_weight.transpose(0, 3, 1, 2)[..., None]).astype(jnp.bfloat16)
    block_state = jnp.einsum(
        "kugep,kugn->kgepn", scaled_x, group_b, preferred_element_type=jnp.float32
    )

    def local_chain(state_now, current_inputs):
        piece_state, piece_fall = current_inputs
        return (state_now * jnp.exp(piece_fall)[..., None, None] + piece_state, state_now)

    final_state, local_entering = lax.scan(
        local_chain, jnp.zeros(block_state.shape[1:], jnp.float32), (block_state, block_end)
    )
    log_total = jnp.sum(block_end, axis=0)
    prefix_log = jnp.cumsum(block_end, axis=0) - block_end
    log_before, state_before = entering_2(
        (log_total, final_state),
        "sp",
        join_states,
        (jnp.zeros_like(log_total), jnp.zeros_like(final_state)),
    )
    entering = (local_entering + jnp.exp(prefix_log)[..., None, None] * state_before[None]).astype(
        jnp.bfloat16
    )
    carried_out = jnp.einsum(
        "ktgn,kgepn->ktgep", group_c, entering, preferred_element_type=jnp.float32
    )
    carried_out = carried_out * jnp.exp(cumulative_decay)[..., None]
    mixed_ssd = (within + carried_out).reshape(tok_rows, inner_local) * jax.nn.silu(
        output_gate_rows.astype(jnp.float32)
    )
    grouped = mixed_ssd.reshape(tok_rows, groups_local, inner_local // groups_local)
    normed = grouped * lax.rsqrt(jnp.mean(grouped * grouped, axis=-1, keepdims=True) + eps)
    ssd_out = (normed.reshape(tok_rows, inner_local) * gain_ssd.astype(jnp.float32)).astype(
        jnp.bfloat16
    )
    positions = (seq_index * tok_rows + jnp.arange(tok_rows, dtype=jnp.int32)).astype(jnp.float32)
    group_ids = core_index * groups_pool + jnp.arange(pool_local, dtype=jnp.int32) // POOL_GROUP
    pool_out = pool_mix(pooling_rows, prior_pool, positions, group_ids, weight_pool, gain_pool)
    channels = jnp.concatenate([ssd_out, pool_out], axis=1)
    half_width = D // core_count
    gain_out = lax.dynamic_slice_in_dim(
        output_norm_gain, core_index * half_width, half_width, 0
    ).astype(jnp.float32)
    partial = jnp.dot(channels, whole_columns, preferred_element_type=jnp.float32).astype(
        jnp.bfloat16
    )
    own_half = lax.dynamic_slice_in_dim(partial, core_index * half_width, half_width, 1).astype(
        jnp.float32
    )
    for hop in range(1, core_count):
        target = lax.rem(core_index + hop, core_count)
        leaving = lax.dynamic_slice_in_dim(partial, target * half_width, half_width, 1)
        route = [(i, (i + hop) % core_count) for i in range(core_count)]
        own_half = own_half + lax.ppermute(leaving, "tp", route).astype(jnp.float32)
    row_squares = lax.psum(jnp.sum(own_half * own_half, axis=1), "tp")
    result = own_half * lax.rsqrt(row_squares / D + eps)[:, None] * gain_out
    return result.astype(jnp.bfloat16)[None]


def solution(mesh):
    in_specs = (
        P("fs", "sp", "tp"),
        P("fs", "sp", "tp"),
        P("fs", "sp", "tp"),
        P("fs", "sp", "tp"),
        P("fs", "sp", "tp"),
        P("fs", "sp", "tp"),
        P(),
        P(),
        P(),
        P(),
        P(),
        P(),
        P("fs", "sp", "tp"),
        P(),
        P(),
        P("tp", ("sp", "fs")),
        P("tp", ("sp", "fs")),
        P(),
    )
    out_specs = P("fs", "sp", "tp")
    return jax.shard_map(body, mesh=mesh, in_specs=in_specs, out_specs=out_specs, check_vma=False)
```

```python
import functools

import jax
import jax.numpy as jnp
from jax import lax
from jax.experimental import pallas as pl
from jax.experimental.pallas import tpu as pltpu
from jax.sharding import PartitionSpec as P

D = 4096
HEAD_DIM = 64
STATE = 128
CONV = 4
BLOCK = 128
POOL_GROUPS = 4
POOL_GROUP = 256


eps = 1e-06


def passed_along(block, axis, distance):
    devices = range(lax.axis_size(axis))
    route = [(i - distance, i) for i in devices if i - distance in devices]
    return lax.ppermute(block, axis, route)


def entering_2(array, axis, join, neutral):
    place = lax.axis_index(axis)
    gathered = jax.tree.map(
        lambda a, kind: lax.all_gather(a.astype(kind), axis), array, (jnp.bfloat16, jnp.bfloat16)
    )
    state = jax.tree.map(lambda a, e: jnp.zeros_like(a) + jnp.asarray(e, a.dtype), array, neutral)

    def one(lap, state):
        return join(
            state,
            jax.tree.map(
                lambda a, own: lax.dynamic_index_in_dim(a, lap, 0, False).astype(own.dtype),
                gathered,
                array,
            ),
        )

    return lax.fori_loop(0, place, one, state)


MESH_IDS = pl.DeviceIdType.MESH
EXACT = lax.Precision.HIGHEST
CHUNKS, CHAINS = 6, 4
NAMES = ("out", "gain", "scale", "bias")
INPUTS, GATE, VECTORS = 16, 1, 12
SOURCES, OTHERS = (0, 2, 3, 10), (4, 5, 6, 7, 8, 9, 11, 12, 13, 14, 15)


class Links:
    def __init__(self, sp_size, fs_size):
        self.n = sp_size
        self.z = lax.axis_index("sp")
        self.fs = lax.axis_index("fs")
        self.core = lax.axis_index("tp")
        self.x = lax.rem(self.fs, 2)
        self.y = self.fs // 2
        self.beside = {"fs": self.fs + 1 - 2 * self.x}
        self.across = {"fs": self.fs + 2 - 4 * self.y}
        self.sibling = {"tp": 1 - self.core}

    def barrier(self):
        barrier = pltpu.get_barrier_semaphore()
        near = [{"sp": lax.rem(self.z + far, self.n)} for far in (1, self.n - 1)]
        for other in (*near, self.beside, self.across, self.sibling):
            pl.semaphore_signal(barrier, inc=1, device_id=other, device_id_type=MESH_IDS)
        pl.semaphore_wait(barrier, len(near) + 3)

    def within(self, place):
        return jnp.logical_and(place >= 0, place < self.n)

    def nearest(self, turn):
        if turn == 0:
            return self.z
        low, high = self.z, self.n - 1 - self.z
        small = jnp.minimum(low, high)
        both = turn <= 2 * small
        far = jnp.where(both, (turn + 1) // 2, turn - small)
        sign = jnp.where(both, 1 - 2 * (turn % 2), jnp.where(high > low, 1, -1))
        return self.z + sign * far


def remote(src, dst, sends, arrivals, spot, device):
    return pltpu.make_async_remote_copy(
        src_ref=src,
        dst_ref=dst,
        send_sem=sends.at[spot],
        recv_sem=arrivals.at[spot],
        device_id=device,
        device_id_type=MESH_IDS,
    )


class Weights:
    def __init__(self, links, whole, width, z_sems, y_sems):
        self.links, self.whole, self.width = links, whole, width
        self.z_sems, self.y_sems = z_sems, y_sems
        self.rows = whole.shape[0] // CHUNKS
        self.direct = range(CHUNKS - 1)
        self.turned = (CHUNKS - 1,)
        self.sent = {}

    def region(self, chunk, z, y):
        at = pl.multiple_of((z * 2 + y) * self.width, self.width)
        return self.whole.at[pl.ds(chunk * self.rows, self.rows), pl.ds(at, self.width)]

    def along(self, chunk, step, way, side, arriving):
        links = self.links
        origin = links.z - way * (step if arriving else step - 1)
        y = links.y if side == 0 else 1 - links.y
        spot = ((chunk * (links.n - 1) + step - 1) * 2 + (way < 0)) * 2 + side
        place = self.region(chunk, jnp.clip(origin, 0, links.n - 1), y)
        copy = remote(place, place, *self.z_sems, spot, {"sp": links.z + way})
        far = links.z if arriving else links.z + way
        return copy, jnp.logical_and(links.within(origin), links.within(far))

    def over(self, chunk, offset, arriving):
        links = self.links
        y = 1 - links.y if arriving else links.y
        origin = links.z + offset
        place = self.region(chunk, jnp.clip(origin, 0, links.n - 1), y)
        spot = chunk * (2 * links.n - 1) + offset + links.n - 1
        copy = remote(place, place, *self.y_sems, spot, links.across)
        return copy, links.within(origin)

    def go(self, kind, *key):
        copy, here = kind(*key, False)
        self.sent[kind.__name__, key] = kind
        pl.when(here)(copy.start)

    def take(self, kind, *key):
        copy, here = kind(*key, True)
        pl.when(here)(copy.wait_recv)

    def pass_on(self, chunk, step, way, side):
        if step < self.links.n and not self.single(step, way, side):
            self.go(self.along, chunk, step, way, side)

    def single(self, step, way, side):
        return step >= self.links.n - 2 and way == 1 and side == 1

    def begin(self):
        for chunk in (*self.turned, *self.direct):
            self.go(self.over, chunk, 0)

    def own(self, chunks, sides=(0,), ways=(1, -1)):
        for chunk in chunks:
            for side in sides:
                for way in ways:
                    self.pass_on(chunk, 1, way, side)

    def turn(self):
        for chunk in self.turned:
            self.take(self.over, chunk, 0)

    def hop(self, step, chunks, sides=(0,), ways=(1, -1)):
        for chunk in chunks:
            for way in ways:
                for side in sides:
                    if not self.single(step, way, side):
                        self.take(self.along, chunk, step, way, side)
                        self.pass_on(chunk, step + 1, way, side)
                if chunk in self.direct or (0 in sides and self.single(step, way, 1)):
                    self.go(self.over, chunk, -way * step)

    def settle(self, step):
        for chunk in self.direct:
            for offset in (0,) if step == 0 else (step, -step):
                self.take(self.over, chunk, offset)
        if self.single(step, 1, 1):
            for chunk in self.turned:
                self.take(self.over, chunk, -step)

    def finish(self):
        for (_, key), kind in self.sent.items():
            copy, here = kind(*key, False)
            pl.when(here)(copy.wait_send)


def silu(rows):
    return rows / (1.0 + jnp.exp(-rows))


def softplus(rows):
    return jnp.maximum(rows, 0.0) + jnp.log(1.0 + jnp.exp(-jnp.abs(rows)))


def piece(vector, offset, size):
    at = pl.multiple_of(offset, 128)
    return vector[pl.ds(at, size)].astype(jnp.float32)[None]


def chosen(core, options):
    best = options[0]
    for at in range(1, len(options)):
        best = jnp.where(core == at, options[at], best)
    return best


def mixers(links, tail, cores, vectors, fetches, refs, sems):
    (x_in, gate, b_in, c_in, dt, added, rates, x_taps, b_taps, c_taps, pool_in,
     pool_weight, prior_x, prior_b, prior_c, prior_pool, x_pad, bc_pad, pool_pad,
     pool_two, pool_four, x_split, bc_conv, b_turned, flat, upright, within, grown, local_in,
     state, before, carry_in, carry_out, channels, far_channels) = refs
    sends, arrivals = sems
    rows, inner = x_in.shape[1:]
    heads = dt.shape[1]
    wide = b_in.shape[2]
    pool = pool_in.shape[2]
    groups = wide // STATE
    span = inner // groups
    blocks = rows // BLOCK
    z, core = links.z, links.core
    lead = 8
    parts = CHAINS
    length = inner // parts
    sources = ((x_in, prior_x), (b_in, prior_b), (c_in, prior_c), (pool_in, prior_pool))

    def tails(at):
        source, target = sources[at]
        return remote(
            source.at[0, pl.ds(rows - tail, tail)], target, sends, arrivals, at, {"sp": z + 1}
        )

    def chain(group):
        return remote(
            carry_out.at[group], carry_in.at[group], sends, arrivals, 4 + group, {"sp": z + 1}
        )

    def pool_letter():
        cols = pl.ds(inner, pool)
        return remote(
            channels.at[:, cols], far_channels.at[:, cols], sends, arrivals, 4 + parts, links.beside
        )

    def block_letter(at):
        place = (pl.ds(at * BLOCK, BLOCK), pl.ds(0, inner))
        return remote(
            channels.at[place], far_channels.at[place], sends, arrivals, 5 + parts + at, links.beside
        )

    follows = z + 1 < links.n
    yield "loaded"
    for at in SOURCES:
        fetches[at].wait()

    @pl.when(follows)
    def _():
        for at in range(4):
            tails(at).start()

    yield "start"
    for at in OTHERS:
        fetches[at].wait()
    x_pad[tail:] = x_in[0].astype(jnp.float32)
    bc_pad[tail:, 0:wide] = b_in[0].astype(jnp.float32)
    bc_pad[tail:, wide:] = c_in[0].astype(jnp.float32)
    pool_pad[0:lead] = jnp.zeros((lead, pool), jnp.float32)
    pool_pad[lead + tail :] = pool_in[0].astype(jnp.float32)
    steps_flat = softplus(dt[0].astype(jnp.float32))
    table = (heads, rates.shape[1])
    picked = lax.broadcasted_iota(jnp.int32, table, 1) == (
        core * heads + lax.broadcasted_iota(jnp.int32, table, 0)
    )
    own_rates = jnp.sum(
        jnp.where(picked, jnp.broadcast_to(rates[...], table), 0.0), axis=1, keepdims=True
    )
    logs_flat = -steps_flat * jnp.exp(own_rates) + added[0]
    flat[...] = jnp.zeros_like(flat)
    down = lax.broadcasted_iota(jnp.int32, (BLOCK, BLOCK), 0)
    over = lax.broadcasted_iota(jnp.int32, (BLOCK, BLOCK), 1)
    causal = down >= over
    upper = (down <= over).astype(jnp.float32)
    first_half = lax.broadcasted_iota(jnp.int32, (BLOCK, 2 * HEAD_DIM), 1) < HEAD_DIM

    def mine(ref, size):
        at = pl.multiple_of(core * size, size)
        return ref[:, pl.ds(at, size)].astype(jnp.float32)

    taps_x = mine(x_taps, inner)
    taps_bc = jnp.concatenate([mine(b_taps, wide), mine(c_taps, wide)], axis=1)
    bias_b = piece(vectors["bias"], core * wide, wide)
    bias_bc = jnp.concatenate([bias_b, jnp.zeros_like(bias_b)], axis=1)

    @pl.when(z == 0)
    def _():
        x_pad[0:tail] = jnp.zeros((tail, inner), jnp.float32)
        bc_pad[0:tail] = jnp.zeros((tail, 2 * wide), jnp.float32)
        pool_pad[lead : lead + tail] = jnp.zeros((tail, pool), jnp.float32)

    @pl.when(z > 0)
    def _():
        for at in range(4):
            tails(at).wait_recv()
        x_pad[0:tail] = prior_x[...].astype(jnp.float32)
        bc_pad[0:tail, 0:wide] = prior_b[...].astype(jnp.float32)
        bc_pad[0:tail, wide:] = prior_c[...].astype(jnp.float32)
        pool_pad[lead : lead + tail] = prior_pool[...].astype(jnp.float32)

    def taps(pad, weights, at, cols):
        total = None
        for tap in range(CONV):
            begin = at * BLOCK + tail - CONV + 1 + tap
            term = pad[begin : begin + BLOCK, cols] * weights[tap : tap + 1, cols]
            total = term if total is None else total + term
        return total

    def spread(narrow, head):
        shape = (BLOCK, 2 * HEAD_DIM)
        return jnp.where(
            first_half,
            jnp.broadcast_to(narrow[:, head : head + 1], shape),
            jnp.broadcast_to(narrow[:, head + 1 : head + 2], shape),
        )

    pairs = span // (2 * HEAD_DIM)
    ends = []
    state[...] = jnp.zeros_like(state)
    for at in range(blocks):
        now = slice(at * BLOCK, (at + 1) * BLOCK)
        bc_conv[now] = silu(taps(bc_pad, taps_bc, at, slice(0, 2 * wide)) + bias_bc).astype(
            jnp.bfloat16
        )
        flat[at, 0:heads] = jnp.dot(
            logs_flat[:, now], upper, precision=EXACT, preferred_element_type=jnp.float32
        )
        flat[at, heads : 2 * heads] = steps_flat[:, now]
        upright[at] = jnp.transpose(flat[at])
        cum = upright[at, :, 0:heads]
        decayed = jnp.exp(cum)
        closing = jnp.exp(cum[BLOCK - 1 : BLOCK] - cum) * upright[at, :, heads : 2 * heads]
        ended = []
        for group in range(groups):
            cols = slice(group * span, (group + 1) * span)
            x_now = silu(taps(x_pad, taps_x, at, cols))
            b_now = bc_conv[now, group * STATE : (group + 1) * STATE]
            b_flat = jnp.transpose(b_now.astype(jnp.float32)).astype(jnp.bfloat16)
            b_turned[at * groups + group] = b_flat
            scaled = []
            for pair in range(pairs):
                head = group * (span // HEAD_DIM) + 2 * pair
                lanes = slice(pair * 2 * HEAD_DIM, (pair + 1) * 2 * HEAD_DIM)
                here = slice(head * HEAD_DIM, (head + 2) * HEAD_DIM)
                x_pair = x_now[:, lanes]
                x_split[at, 0:BLOCK, here] = jnp.where(first_half, x_pair, 0.0).astype(jnp.bfloat16)
                x_split[at, BLOCK : 2 * BLOCK, here] = jnp.where(first_half, 0.0, x_pair).astype(
                    jnp.bfloat16
                )
                x_half = x_pair.astype(jnp.bfloat16).astype(jnp.float32)
                scaled.append((x_half * spread(closing, head)).astype(jnp.bfloat16))
                grown[now, here] = spread(decayed, head)
            end = grown[(at + 1) * BLOCK - 1 : (at + 1) * BLOCK, cols]
            ended.append(end)
            local_in[at, :, cols] = state[:, cols]
            state[:, cols] = state[:, cols] * end + jnp.dot(
                b_flat, jnp.concatenate(scaled, axis=1), preferred_element_type=jnp.float32
            )
        yield at
        ends.append(ended)

    def hand_on():
        @pl.when(z == 0)
        def _():
            before[...] = jnp.zeros_like(before)

        for link in range(parts):
            cols = slice(link * length, (link + 1) * length)
            group, at_end = link * length // span, slice(link * length % span, link * length % span + length)

            @pl.when(z > 0)
            def _(link=link, cols=cols):
                chain(link).wait_recv()
                before[:, cols] = carry_in[link].astype(jnp.float32)

            @pl.when(follows)
            def _(link=link, cols=cols, group=group, at_end=at_end):
                falling = ends[0][group][:, at_end]
                for at in range(1, blocks):
                    falling = falling * ends[at][group][:, at_end]
                carry_out[link] = (before[:, cols] * falling + state[:, cols]).astype(jnp.bfloat16)
                chain(link).start()

    def chain_point(place, last=False):
        pl.when(z >= place if last else z == place)(hand_on)

    chain_point(0)
    yield "states"
    place = z * rows
    position = (place + lax.broadcasted_iota(jnp.int32, (rows, 1), 0)).astype(jnp.float32) + 1.0
    pool_groups = pool // POOL_GROUP
    for group in range(pool_groups):
        cols = slice(group * POOL_GROUP, (group + 1) * POOL_GROUP)
        size = rows + tail
        two = pool_pad[lead:, cols] + pool_pad[lead - 1 : lead - 1 + size, cols]
        pool_two[0:lead] = jnp.zeros((lead, POOL_GROUP), jnp.float32)
        pool_two[lead:] = two
        four = two + pool_two[lead - 2 : lead - 2 + size]
        pool_four[0:lead] = jnp.zeros((lead, POOL_GROUP), jnp.float32)
        pool_four[lead:] = four
        eight = four + pool_four[lead - 4 : lead - 4 + size]
        sixteen = eight[tail:] + eight[tail - 8 : size - 8]
        sums = [two[tail:], four[tail:], eight[tail:], sixteen]
        picks = [c * pool_groups + group for c in range(cores)]
        running = chosen(core, [sums[pick] for pick in picks])
        reach = chosen(core, [jnp.float32(2 ** (pick + 1)) for pick in picks])
        pooled = running / jnp.minimum(position, reach) - pool_in[0, :, cols].astype(jnp.float32)
        mixed = jnp.dot(
            pooled.astype(jnp.bfloat16),
            pool_weight[core * pool_groups + group],
            preferred_element_type=jnp.float32,
        )
        scale = piece(vectors["scale"], core * pool + group * POOL_GROUP, POOL_GROUP)
        out = inner + group * POOL_GROUP
        channels[:, out : out + POOL_GROUP] = (mixed * scale).astype(jnp.bfloat16)
    pool_letter().start()
    for at in range(blocks):
        now = slice(at * BLOCK, (at + 1) * BLOCK)
        cum = upright[at, :, 0:heads]
        cum_flat = flat[at, 0:heads]
        step_flat = flat[at, heads : 2 * heads]
        for group in range(groups):
            c_now = bc_conv[now, wide + group * STATE : wide + (group + 1) * STATE]
            scores = jnp.dot(
                c_now, b_turned[at * groups + group], preferred_element_type=jnp.float32
            )
            for pair in range(pairs):
                first = group * (span // HEAD_DIM) + 2 * pair
                both = []
                for head in (first, first + 1):
                    gap = cum[:, head : head + 1] - cum_flat[head : head + 1]
                    decay = jnp.exp(jnp.where(causal, gap, -1e30))
                    both.append((scores * decay * step_flat[head : head + 1]).astype(jnp.bfloat16))
                here = slice(first * HEAD_DIM, (first + 2) * HEAD_DIM)
                within[now, here] = jnp.dot(
                    jnp.concatenate(both, axis=1),
                    x_split[at, :, here],
                    preferred_element_type=jnp.float32,
                )
    chain_point(1)
    yield "second"
    chain_point(2)
    yield "third"
    chain_point(3, True)
    falling = [None] * groups
    fetches[GATE].wait()
    for at in range(blocks):
        now = slice(at * BLOCK, (at + 1) * BLOCK)
        for group in range(groups):
            cols = slice(group * span, (group + 1) * span)
            earlier = before[:, cols]
            if at:
                earlier = earlier * falling[group]
            entering = local_in[at, :, cols] + earlier
            c_now = bc_conv[now, wide + group * STATE : wide + (group + 1) * STATE]
            carried = jnp.dot(
                c_now, entering.astype(jnp.bfloat16), preferred_element_type=jnp.float32
            )
            mixed = (within[now, cols] + carried * grown[now, cols]) * silu(
                gate[0, now, cols].astype(jnp.float32)
            )
            root = lax.rsqrt(jnp.mean(mixed * mixed, axis=1, keepdims=True) + eps)
            gain = piece(vectors["gain"], core * inner + group * span, span)
            channels[now, cols] = (mixed * root * gain).astype(jnp.bfloat16)
            end = ends[at][group]
            falling[group] = end if at == 0 else falling[group] * end
        block_letter(at).start()
    letters = [pool_letter(), *(block_letter(at) for at in range(blocks))]

    def received():
        for letter in letters:
            letter.wait_recv()

    def finish():
        for letter in letters:
            letter.wait_send()

        @pl.when(follows)
        def _():
            for at in range(4):
                tails(at).wait_send()
            for link in range(parts):
                chain(link).wait_send()

    return received, finish


def whole_kernel(sp_size, fs_size, cores, tail, *refs):
    inputs, ssd_weight, pool_rows, out = refs[:INPUTS], *refs[INPUTS : INPUTS + 3]
    (z_sends, z_arrivals, y_sends, y_arrivals, m_sends, m_arrivals, p_sends, p_arrivals, o_sends,
     o_arrivals, local_sems, whole, parts, part_in, returned, return_in, squares, squares_in,
     *rest) = refs[INPUTS + 3 :]
    held, rest = rest[:INPUTS], rest[INPUTS:]
    vectors = dict(zip(NAMES, held[VECTORS:]))
    held = held[:VECTORS]
    channels, far_channels = rest[-2:]
    links = Links(sp_size, fs_size)
    width = ssd_weight.shape[1]
    inner = ssd_weight.shape[0]
    rows = channels.shape[0]
    half = sp_size // cores
    core = links.core
    own_at = pl.multiple_of((links.z * 2 + links.y) * width, width)
    loads = [
        pltpu.make_async_copy(
            source, whole.at[pl.ds(begin, source.shape[0]), pl.ds(own_at, width)], local_sems.at[at]
        )
        for at, (source, begin) in enumerate(((ssd_weight, 0), (pool_rows, inner)))
    ]
    fetches = [
        pltpu.make_async_copy(source, place, local_sems.at[2 + at])
        for at, (source, place) in enumerate(zip(inputs, (*held, *vectors.values())))
    ]
    for load in loads:
        load.start()
    for at in (*SOURCES, *OTHERS, GATE):
        fetches[at].start()
    links.barrier()
    weights = Weights(links, whole, width, (z_sends, z_arrivals), (y_sends, y_arrivals))
    work = mixers(links, tail, cores, vectors, fetches, (*held, *rest), (m_sends, m_arrivals))

    direct, turned = weights.direct, weights.turned
    both = (0, 1)
    last = sp_size - 1
    mixed = None
    while mixed is None:
        try:
            mark = next(work)
        except StopIteration as ended:
            mixed = ended.value
            break
        if mark == "loaded":
            for load in loads:
                load.wait()
            weights.begin()
            weights.own(direct[:3], ways=(-1,))
        elif mark == "start":
            weights.own(direct[:3], ways=(1,))
        elif mark == 1:
            weights.own(direct[3:4])
        elif mark == "states":
            weights.own(direct[4:])
            weights.turn()
            weights.own(turned, both, (-1,))
            pl.when(links.z == last)(lambda: weights.own(turned, both, (1,)))
            weights.hop(1, direct[:1], ways=(-1,))
        elif mark == "second":
            weights.hop(1, direct[1:3], ways=(-1,))
            pl.when(links.z == 1)(lambda: weights.own(turned, both, (1,)))
            pl.when(links.z == 1)(lambda: weights.hop(1, direct[:4], ways=(1,)))
            pl.when(links.z == last)(lambda: weights.hop(1, direct, ways=(1,)))
            inner_late = jnp.logical_and(links.z >= 2, links.z < last)
            pl.when(inner_late)(lambda: weights.hop(1, direct[:3], ways=(1,)))
        elif mark == "third":
            pl.when(inner_late)(lambda: weights.own(turned, both, (1,)))
            pl.when(inner_late)(lambda: weights.hop(1, direct[3:], ways=(1,)))
            pl.when(links.z == last)(lambda: weights.hop(2, direct[:3], ways=(1,)))
            pl.when(links.z >= 2)(lambda: weights.hop(1, direct[3:], ways=(-1,)))
    received, finish_mixers = mixed
    pl.when(links.z == 0)(lambda: weights.own(turned, both, (1,)))
    pl.when(links.z == 1)(lambda: weights.hop(1, direct[4:], ways=(1,)))
    pl.when(links.z <= 1)(lambda: weights.hop(1, direct[3:], ways=(-1,)))

    def multiply(turn, far, sides=both):
        z = links.nearest(turn)
        source = far_channels if far else channels

        @pl.loop(0, len(sides))
        def _(at):
            y = lax.rem(links.y + sides[0] + at, 2)
            slab = z * 2 + y
            lanes = pl.ds(pl.multiple_of(slab * width, width), width)
            parts[far, slab] = jnp.dot(
                source[...], whole[:, lanes], preferred_element_type=jnp.float32
            ).astype(jnp.bfloat16)

            @pl.when(z // half != core)
            def _():
                part_letter(z, y, far).start()

    def part_letter(z, y, far):
        slab = z * 2 + y
        return remote(
            parts.at[far, slab],
            part_in.at[far, lax.rem(z, half) * 2 + y],
            p_sends,
            p_arrivals,
            far * 2 * sp_size + slab,
            links.sibling,
        )

    def return_letter(slot):
        return remote(
            returned.at[slot], return_in.at[slot], o_sends, o_arrivals, slot, links.beside
        )

    def give_back(turn, sides=both):
        z = links.nearest(turn)

        @pl.when(z // half == core)
        def _():
            @pl.loop(0, len(sides))
            def _(at):
                y = lax.rem(links.y + sides[0] + at, 2)
                part_letter(z, y, 1).wait_recv()
                slot = lax.rem(z, half) * 2 + y
                returned[slot] = (
                    parts[1, z * 2 + y].astype(jnp.float32) + part_in[1, slot].astype(jnp.float32)
                ).astype(jnp.bfloat16)
                return_letter(slot).start()

    edge = jnp.logical_or(links.z == 0, links.z == last)
    weights.settle(0)
    multiply(0, 0)
    for step in range(1, last):
        weights.hop(step, turned, both)
        if step + 1 < last:
            if step == 1:
                pl.when(links.z == last)(lambda: weights.hop(2, direct[3:]))
                pl.when(links.z != last)(lambda: weights.hop(2, direct))
            else:
                weights.hop(step + 1, direct)
            weights.settle(step)
            multiply(step, 0)
    received()
    share = -(-len(direct) // last)

    def ahead(turn):
        multiply(turn, 1)
        give_back(turn)
        multiply(turn, 0)

    for turn in range(last):
        pieces_now = direct[turn * share : (turn + 1) * share]
        if turn == last - 1:
            pl.when(jnp.logical_not(edge))(lambda: ahead(turn))
            weights.settle(turn)
            weights.hop(last, pieces_now)
            pl.when(edge)(lambda: ahead(turn))
        else:
            multiply(turn, 1)
            weights.hop(last, pieces_now)
            give_back(turn)
    weights.hop(last, turned, (0,))
    multiply(last, 1, (0,))
    multiply(last, 0, (0,))
    give_back(last, (0,))
    weights.hop(last, turned, (1,))
    weights.settle(last)
    multiply(last, 1, (1,))
    give_back(last, (1,))
    multiply(last, 0, (1,))
    own_half = core * half
    slots = 2 * half

    def lane_squares(values):
        values = values * values
        total = values[:, 0:128]
        for at in range(1, width // 128):
            total = total + values[:, at * 128 : (at + 1) * 128]
        return total

    def own_total(slot):
        return parts[0, own_half * 2 + slot].astype(jnp.float32) + part_in[0, slot].astype(
            jnp.float32
        )

    squares[...] = jnp.zeros_like(squares)

    @pl.loop(0, slots)
    def _(slot):
        part_letter(own_half + slot // 2, lax.rem(slot, 2), 0).wait_recv()
        squares[...] += lane_squares(own_total(slot))

    @pl.loop(0, slots)
    def _(slot):
        return_letter(slot).wait_recv()
        squares[...] += lane_squares(return_in[slot].astype(jnp.float32))

    exchange = remote(squares, squares_in, o_sends, o_arrivals, slots, links.sibling)
    exchange.start()
    exchange.wait_recv()
    row_squares = jnp.sum(squares[...] + squares_in[...], axis=1, keepdims=True)
    features = cores * out.shape[2]
    root = lax.rsqrt(row_squares / features + eps)

    @pl.loop(0, slots)
    def _(slot):
        first = (slot // 2) * fs_size + 2 * lax.rem(slot, 2)
        for values, x in (
            (own_total(slot), links.x),
            (return_in[slot].astype(jnp.float32), 1 - links.x),
        ):
            at = pl.multiple_of((first + x) * width, width)
            gain = piece(vectors["out"], core * out.shape[2] + at, width)
            out[0, :, pl.ds(at, width)] = (values * root * gain).astype(jnp.bfloat16)

    exchange.wait_send()
    weights.finish()
    finish_mixers()

    @pl.loop(0, 2 * half)
    def _(slot):
        return_letter(slot).wait_send()
        other = (1 - core) * half
        for far in range(2):
            part_letter(other + slot // 2, lax.rem(slot, 2), far).wait_send()


def mixed_and_projected(inputs, vectors, ssd_weight, pool_rows, tail):
    sp_size, fs_size, cores = lax.axis_size("sp"), lax.axis_size("fs"), lax.axis_size("tp")
    width = ssd_weight.shape[1]
    x_in, b_in, pool_in = inputs[0], inputs[2], inputs[10]
    features = vectors["out"].shape[0]
    inputs = (*inputs, *(vectors[name] for name in NAMES))
    tok_rows, inner = x_in.shape[1:]
    wide, pool = b_in.shape[2], pool_in.shape[2]
    groups = wide // STATE
    blocks = tok_rows // BLOCK
    half = sp_size // cores
    slots = 2 * half
    vmem = pl.BlockSpec(memory_space=pltpu.VMEM)
    hbm = pl.BlockSpec(memory_space=pltpu.HBM)
    dma = pltpu.SemaphoreType.DMA
    half_type, full_type = jnp.bfloat16, jnp.float32
    z_spots, y_spots = CHUNKS * (sp_size - 1) * 4, CHUNKS * (2 * sp_size - 1)
    letters = 5 + CHAINS + blocks
    return pl.pallas_call(
        functools.partial(whole_kernel, sp_size, fs_size, cores, tail),
        out_shape=pltpu.VMEM((1, tok_rows, features // cores), half_type),
        in_specs=[hbm] * (len(inputs) + 2),
        out_specs=vmem,
        scratch_shapes=[
            dma((z_spots,)),
            dma((z_spots,)),
            dma((y_spots,)),
            dma((y_spots,)),
            dma((letters,)),
            dma((letters,)),
            dma((4 * sp_size,)),
            dma((4 * sp_size,)),
            dma((slots + 1,)),
            dma((slots + 1,)),
            dma((2 + len(inputs),)),
            pltpu.VMEM((inner + pool, width * 2 * sp_size), half_type),
            pltpu.VMEM((2, 2 * sp_size, tok_rows, width), half_type),
            pltpu.VMEM((2, slots, tok_rows, width), half_type),
            pltpu.VMEM((slots, tok_rows, width), half_type),
            pltpu.VMEM((slots, tok_rows, width), half_type),
            pltpu.VMEM((tok_rows, 128), full_type),
            pltpu.VMEM((tok_rows, 128), full_type),
            *(pltpu.VMEM(array.shape, array.dtype) for array in inputs),
            pltpu.VMEM((tail, inner), half_type),
            pltpu.VMEM((tail, wide), half_type),
            pltpu.VMEM((tail, wide), half_type),
            pltpu.VMEM((tail, pool), half_type),
            pltpu.VMEM((tail + tok_rows, inner), full_type),
            pltpu.VMEM((tail + tok_rows, 2 * wide), full_type),
            pltpu.VMEM((8 + tail + tok_rows, pool), full_type),
            pltpu.VMEM((8 + tail + tok_rows, POOL_GROUP), full_type),
            pltpu.VMEM((8 + tail + tok_rows, POOL_GROUP), full_type),
            pltpu.VMEM((blocks, 2 * BLOCK, inner), half_type),
            pltpu.VMEM((tok_rows, 2 * wide), half_type),
            pltpu.VMEM((blocks * groups, STATE, BLOCK), half_type),
            pltpu.VMEM((blocks, 128, BLOCK), full_type),
            pltpu.VMEM((blocks, BLOCK, 128), full_type),
            pltpu.VMEM((tok_rows, inner), full_type),
            pltpu.VMEM((tok_rows, inner), full_type),
            pltpu.VMEM((blocks, STATE, inner), full_type),
            pltpu.VMEM((STATE, inner), full_type),
            pltpu.VMEM((STATE, inner), full_type),
            pltpu.VMEM((CHAINS, STATE, inner // CHAINS), half_type),
            pltpu.VMEM((CHAINS, STATE, inner // CHAINS), half_type),
            pltpu.VMEM((tok_rows, inner + pool), half_type),
            pltpu.VMEM((tok_rows, inner + pool), half_type),
        ],
        compiler_params=pltpu.CompilerParams(
            collective_id=0, has_side_effects=True, vmem_limit_bytes=48 * 2**20
        ),
        name="paired_mixers",
    )(*(pltpu.with_memory_space_constraint(array, pltpu.HBM) for array in (*inputs, ssd_weight, pool_rows)))


def causal_taps(input_rows, prior_rows, tap_weights, offset_bias):
    padded = jnp.concatenate([prior_rows, input_rows], axis=0).astype(jnp.float32)
    tok_rows = input_rows.shape[0]
    running = jnp.zeros(input_rows.shape, jnp.float32) + offset_bias
    for tap_index in range(tap_weights.shape[0]):
        running = (
            running
            + tap_weights[tap_index].astype(jnp.float32) * padded[tap_index : tap_index + tok_rows]
        )
    return jax.nn.silu(running).astype(jnp.bfloat16)


def pool_mix(input_rows, prior_rows, positions, group_ids, local_weight, local_scale):
    tail_rows = prior_rows.shape[0]
    tok_rows = input_rows.shape[0]
    padded = jnp.concatenate([prior_rows, input_rows], axis=0).astype(jnp.float32)
    window_reach = jnp.left_shift(jnp.int32(2), group_ids)
    running = jnp.zeros(input_rows.shape, jnp.float32)
    for offset_back in range(tail_rows + 1):
        start_row = tail_rows - offset_back
        running = running + padded[start_row : start_row + tok_rows] * (
            offset_back < window_reach
        ).astype(jnp.float32)
    window_count = jnp.minimum(positions[:, None] + 1.0, window_reach.astype(jnp.float32)[None, :])
    pooled = (running / window_count - input_rows.astype(jnp.float32)).astype(jnp.bfloat16)
    grouped = pooled.reshape(tok_rows, local_weight.shape[0], local_weight.shape[1])
    mixed = jnp.einsum("lgc,gcd->lgd", grouped, local_weight, preferred_element_type=jnp.float32)
    return (mixed.reshape(input_rows.shape) * local_scale.astype(jnp.float32)).astype(jnp.bfloat16)


def join_states(earlier, later_part):
    return (
        earlier[0] + later_part[0],
        earlier[1] * jnp.exp(later_part[0])[..., None, None] + later_part[1],
    )


def body(
    statespace_input,
    output_gate_input,
    state_input_projection,
    state_output_projection,
    step_size_input,
    added_log_decay,
    logarithm_rates,
    head_channel_taps,
    input_projection_taps,
    output_projection_taps,
    input_projection_bias,
    group_norm_gain,
    pooling_input,
    pooling_group_weight,
    pooling_channel_scale,
    statespace_output_weight,
    pooling_output_weight,
    output_norm_gain,
):
    core_count = lax.axis_size("tp")
    sp_size, fs_size = lax.axis_size("sp"), lax.axis_size("fs")
    pool_tail = 2**POOL_GROUPS - 1
    paired = (
        statespace_output_weight.shape[1] % 128 == 0
        and fs_size == 4
        and core_count == 2
        and sp_size in (4, 8)
    )
    if paired:
        return mixed_and_projected(
            (
                statespace_input,
                output_gate_input,
                state_input_projection,
                state_output_projection,
                jnp.swapaxes(step_size_input, 1, 2),
                jnp.swapaxes(added_log_decay, 1, 2),
                logarithm_rates[None],
                head_channel_taps,
                input_projection_taps,
                output_projection_taps,
                pooling_input,
                pooling_group_weight,
            ),
            {
                "out": output_norm_gain,
                "gain": group_norm_gain,
                "scale": pooling_channel_scale,
                "bias": input_projection_bias,
            },
            statespace_output_weight,
            pooling_output_weight,
            pool_tail + 1,
        )
    core_index = lax.axis_index("tp")
    seq_index = lax.axis_index("sp")
    head_channel_rows = statespace_input[0]
    output_gate_rows = output_gate_input[0]
    input_projection_rows = state_input_projection[0]
    output_projection_rows = state_output_projection[0]
    step_size_rows = step_size_input[0]
    decay_spikes = added_log_decay[0]
    pooling_rows = pooling_input[0]
    tok_rows = head_channel_rows.shape[0]
    inner_local = head_channel_rows.shape[1]
    heads_local = step_size_rows.shape[1]
    state_local = input_projection_rows.shape[1]
    pool_local = pooling_rows.shape[1]
    groups_local = state_local // STATE
    per_group = heads_local // groups_local
    groups_pool = pool_local // POOL_GROUP
    conv_tail = CONV - 1
    own_columns = jnp.concatenate([statespace_output_weight, pooling_output_weight], axis=0)
    tails = jnp.concatenate(
        [
            jnp.pad(rows[tok_rows - tail :], ((pool_tail - tail, 0), (0, 0)))
            for rows, tail in (
                (head_channel_rows, conv_tail),
                (input_projection_rows, conv_tail),
                (output_projection_rows, conv_tail),
                (pooling_rows, pool_tail),
            )
        ],
        axis=1,
    )
    prior = passed_along(tails, "sp", 1)
    widths = (inner_local, state_local, state_local, pool_local)
    prior_x, prior_b, prior_c, prior_pool = (
        prior[pool_tail - tail :, sum(widths[:at]) : sum(widths[: at + 1])]
        for at, tail in enumerate((conv_tail, conv_tail, conv_tail, pool_tail))
    )
    taps_x = lax.dynamic_slice_in_dim(head_channel_taps, core_index * inner_local, inner_local, 1)
    taps_b = lax.dynamic_slice_in_dim(
        input_projection_taps, core_index * state_local, state_local, 1
    )
    taps_c = lax.dynamic_slice_in_dim(
        output_projection_taps, core_index * state_local, state_local, 1
    )
    bias_b = lax.dynamic_slice_in_dim(
        input_projection_bias, core_index * state_local, state_local, 0
    )
    gain_ssd = lax.dynamic_slice_in_dim(group_norm_gain, core_index * inner_local, inner_local, 0)
    head_decay_rates = jnp.exp(
        lax.dynamic_slice_in_dim(logarithm_rates, core_index * heads_local, heads_local, 0)
    )
    gain_pool = lax.dynamic_slice_in_dim(
        pooling_channel_scale, core_index * pool_local, pool_local, 0
    )
    weight_pool = lax.dynamic_slice_in_dim(
        pooling_group_weight, core_index * groups_pool, groups_pool, 0
    )
    whole_columns = lax.all_gather(own_columns, ("sp", "fs"), axis=1, tiled=True)
    x_conv = causal_taps(head_channel_rows, prior_x, taps_x, 0.0)
    b_conv = causal_taps(input_projection_rows, prior_b, taps_b, bias_b.astype(jnp.float32))
    c_conv = causal_taps(output_projection_rows, prior_c, taps_c, 0.0)
    blocks = tok_rows // BLOCK
    discrete_step_size = jax.nn.softplus(step_size_rows.astype(jnp.float32))
    logarithm_decay = -discrete_step_size * head_decay_rates + decay_spikes
    cumulative_decay = jnp.cumsum(
        logarithm_decay.reshape(blocks, BLOCK, groups_local, per_group), axis=1
    )
    cum_t = cumulative_decay.transpose(0, 2, 3, 1)
    step_t = discrete_step_size.reshape(blocks, BLOCK, groups_local, per_group).transpose(
        0, 2, 3, 1
    )
    heads_x = x_conv.reshape(blocks, BLOCK, groups_local, per_group, HEAD_DIM)
    group_b = b_conv.reshape(blocks, BLOCK, groups_local, STATE)
    group_c = c_conv.reshape(blocks, BLOCK, groups_local, STATE)
    scores = jnp.einsum("ktgn,kugn->kgtu", group_c, group_b, preferred_element_type=jnp.float32)
    causal = jnp.arange(BLOCK)[:, None] >= jnp.arange(BLOCK)[None, :]
    decay_gap = cum_t[..., :, None] - cum_t[..., None, :]
    decay_factor = jnp.where(causal, jnp.exp(jnp.where(causal, decay_gap, 0.0)), 0.0)
    weights = (scores[:, :, None] * decay_factor * step_t[..., None, :]).astype(jnp.bfloat16)
    within = jnp.einsum("kgetu,kugep->ktgep", weights, heads_x, preferred_element_type=jnp.float32)
    block_end = cum_t[..., -1]
    end_weight = jnp.exp(block_end[..., None] - cum_t) * step_t
    scaled_x = (heads_x * end_weight.transpose(0, 3, 1, 2)[..., None]).astype(jnp.bfloat16)
    block_state = jnp.einsum(
        "kugep,kugn->kgepn", scaled_x, group_b, preferred_element_type=jnp.float32
    )

    def local_chain(state_now, current_inputs):
        piece_state, piece_fall = current_inputs
        return (state_now * jnp.exp(piece_fall)[..., None, None] + piece_state, state_now)

    final_state, local_entering = lax.scan(
        local_chain, jnp.zeros(block_state.shape[1:], jnp.float32), (block_state, block_end)
    )
    log_total = jnp.sum(block_end, axis=0)
    prefix_log = jnp.cumsum(block_end, axis=0) - block_end
    log_before, state_before = entering_2(
        (log_total, final_state),
        "sp",
        join_states,
        (jnp.zeros_like(log_total), jnp.zeros_like(final_state)),
    )
    entering = (local_entering + jnp.exp(prefix_log)[..., None, None] * state_before[None]).astype(
        jnp.bfloat16
    )
    carried_out = jnp.einsum(
        "ktgn,kgepn->ktgep", group_c, entering, preferred_element_type=jnp.float32
    )
    carried_out = carried_out * jnp.exp(cumulative_decay)[..., None]
    mixed_ssd = (within + carried_out).reshape(tok_rows, inner_local) * jax.nn.silu(
        output_gate_rows.astype(jnp.float32)
    )
    grouped = mixed_ssd.reshape(tok_rows, groups_local, inner_local // groups_local)
    normed = grouped * lax.rsqrt(jnp.mean(grouped * grouped, axis=-1, keepdims=True) + eps)
    ssd_out = (normed.reshape(tok_rows, inner_local) * gain_ssd.astype(jnp.float32)).astype(
        jnp.bfloat16
    )
    positions = (seq_index * tok_rows + jnp.arange(tok_rows, dtype=jnp.int32)).astype(jnp.float32)
    group_ids = core_index * groups_pool + jnp.arange(pool_local, dtype=jnp.int32) // POOL_GROUP
    pool_out = pool_mix(pooling_rows, prior_pool, positions, group_ids, weight_pool, gain_pool)
    channels = jnp.concatenate([ssd_out, pool_out], axis=1)
    half_width = D // core_count
    gain_out = lax.dynamic_slice_in_dim(
        output_norm_gain, core_index * half_width, half_width, 0
    ).astype(jnp.float32)
    partial = jnp.dot(channels, whole_columns, preferred_element_type=jnp.float32).astype(
        jnp.bfloat16
    )
    own_half = lax.dynamic_slice_in_dim(partial, core_index * half_width, half_width, 1).astype(
        jnp.float32
    )
    for hop in range(1, core_count):
        target = lax.rem(core_index + hop, core_count)
        leaving = lax.dynamic_slice_in_dim(partial, target * half_width, half_width, 1)
        route = [(i, (i + hop) % core_count) for i in range(core_count)]
        own_half = own_half + lax.ppermute(leaving, "tp", route).astype(jnp.float32)
    row_squares = lax.psum(jnp.sum(own_half * own_half, axis=1), "tp")
    result = own_half * lax.rsqrt(row_squares / D + eps)[:, None] * gain_out
    return result.astype(jnp.bfloat16)[None]


def solution(mesh):
    in_specs = (
        P("fs", "sp", "tp"),
        P("fs", "sp", "tp"),
        P("fs", "sp", "tp"),
        P("fs", "sp", "tp"),
        P("fs", "sp", "tp"),
        P("fs", "sp", "tp"),
        P(),
        P(),
        P(),
        P(),
        P(),
        P(),
        P("fs", "sp", "tp"),
        P(),
        P(),
        P("tp", ("sp", "fs")),
        P("tp", ("sp", "fs")),
        P(),
    )
    out_specs = P("fs", "sp", "tp")
    return jax.shard_map(body, mesh=mesh, in_specs=in_specs, out_specs=out_specs, check_vma=False)
```

```python
import functools

import jax
import jax.numpy as jnp
from jax import lax
from jax.experimental import pallas as pl
from jax.experimental.pallas import tpu as pltpu
from jax.sharding import PartitionSpec as P

D = 4096
HEAD_DIM = 64
STATE = 128
CONV = 4
BLOCK = 128
POOL_GROUPS = 4
POOL_GROUP = 256


eps = 1e-06


def passed_along(block, axis, distance):
    devices = range(lax.axis_size(axis))
    route = [(i - distance, i) for i in devices if i - distance in devices]
    return lax.ppermute(block, axis, route)


def entering_2(array, axis, join, neutral):
    place = lax.axis_index(axis)
    gathered = jax.tree.map(
        lambda a, kind: lax.all_gather(a.astype(kind), axis), array, (jnp.bfloat16, jnp.bfloat16)
    )
    state = jax.tree.map(lambda a, e: jnp.zeros_like(a) + jnp.asarray(e, a.dtype), array, neutral)

    def one(lap, state):
        return join(
            state,
            jax.tree.map(
                lambda a, own: lax.dynamic_index_in_dim(a, lap, 0, False).astype(own.dtype),
                gathered,
                array,
            ),
        )

    return lax.fori_loop(0, place, one, state)


MESH_IDS = pl.DeviceIdType.MESH
EXACT = lax.Precision.HIGHEST
CHUNKS, CHAINS = 6, 4
NAMES = ("out", "gain", "scale", "bias")
INPUTS, GATE, VECTORS = 16, 1, 12
SOURCES, OTHERS = (0, 2, 3, 10), (4, 5, 6, 7, 8, 9, 11, 12, 13, 14, 15)


class Links:
    def __init__(self, sp_size, fs_size):
        self.n = sp_size
        self.z = lax.axis_index("sp")
        self.fs = lax.axis_index("fs")
        self.core = lax.axis_index("tp")
        self.x = lax.rem(self.fs, 2)
        self.y = self.fs // 2
        self.beside = {"fs": self.fs + 1 - 2 * self.x}
        self.across = {"fs": self.fs + 2 - 4 * self.y}
        self.sibling = {"tp": 1 - self.core}

    def barrier(self):
        barrier = pltpu.get_barrier_semaphore()
        near = [{"sp": lax.rem(self.z + far, self.n)} for far in (1, self.n - 1)]
        for other in (*near, self.beside, self.across, self.sibling):
            pl.semaphore_signal(barrier, inc=1, device_id=other, device_id_type=MESH_IDS)
        pl.semaphore_wait(barrier, len(near) + 3)

    def within(self, place):
        return jnp.logical_and(place >= 0, place < self.n)

    def nearest(self, turn):
        if turn == 0:
            return self.z
        low, high = self.z, self.n - 1 - self.z
        small = jnp.minimum(low, high)
        both = turn <= 2 * small
        far = jnp.where(both, (turn + 1) // 2, turn - small)
        sign = jnp.where(both, 1 - 2 * (turn % 2), jnp.where(high > low, 1, -1))
        return self.z + sign * far


def remote(src, dst, sends, arrivals, spot, device):
    return pltpu.make_async_remote_copy(
        src_ref=src,
        dst_ref=dst,
        send_sem=sends.at[spot],
        recv_sem=arrivals.at[spot],
        device_id=device,
        device_id_type=MESH_IDS,
    )


class Weights:
    def __init__(self, links, whole, width, z_sems, y_sems):
        self.links, self.whole, self.width = links, whole, width
        self.z_sems, self.y_sems = z_sems, y_sems
        self.rows = whole.shape[0] // CHUNKS
        self.direct = range(CHUNKS - 1)
        self.turned = (CHUNKS - 1,)
        self.sent = {}

    def region(self, chunk, z, y):
        at = pl.multiple_of((z * 2 + y) * self.width, self.width)
        return self.whole.at[pl.ds(chunk * self.rows, self.rows), pl.ds(at, self.width)]

    def along(self, chunk, step, way, side, arriving):
        links = self.links
        origin = links.z - way * (step if arriving else step - 1)
        y = links.y if side == 0 else 1 - links.y
        spot = ((chunk * (links.n - 1) + step - 1) * 2 + (way < 0)) * 2 + side
        place = self.region(chunk, jnp.clip(origin, 0, links.n - 1), y)
        copy = remote(place, place, *self.z_sems, spot, {"sp": links.z + way})
        far = links.z if arriving else links.z + way
        return copy, jnp.logical_and(links.within(origin), links.within(far))

    def over(self, chunk, offset, arriving):
        links = self.links
        y = 1 - links.y if arriving else links.y
        origin = links.z + offset
        place = self.region(chunk, jnp.clip(origin, 0, links.n - 1), y)
        spot = chunk * (2 * links.n - 1) + offset + links.n - 1
        copy = remote(place, place, *self.y_sems, spot, links.across)
        return copy, links.within(origin)

    def go(self, kind, *key):
        copy, here = kind(*key, False)
        self.sent[kind.__name__, key] = kind
        pl.when(here)(copy.start)

    def take(self, kind, *key):
        copy, here = kind(*key, True)
        pl.when(here)(copy.wait_recv)

    def pass_on(self, chunk, step, way, side):
        if step < self.links.n and not self.single(step, way, side):
            self.go(self.along, chunk, step, way, side)

    def single(self, step, way, side):
        return step >= self.links.n - 2 and way == 1 and side == 1

    def begin(self):
        for chunk in (*self.turned, *self.direct):
            self.go(self.over, chunk, 0)

    def own(self, chunks, sides=(0,), ways=(1, -1)):
        for chunk in chunks:
            for side in sides:
                for way in ways:
                    self.pass_on(chunk, 1, way, side)

    def turn(self):
        for chunk in self.turned:
            self.take(self.over, chunk, 0)

    def hop(self, step, chunks, sides=(0,), ways=(1, -1)):
        for chunk in chunks:
            for way in ways:
                for side in sides:
                    if not self.single(step, way, side):
                        self.take(self.along, chunk, step, way, side)
                        self.pass_on(chunk, step + 1, way, side)
                if chunk in self.direct or (0 in sides and self.single(step, way, 1)):
                    self.go(self.over, chunk, -way * step)

    def settle(self, step):
        for chunk in self.direct:
            for offset in (0,) if step == 0 else (step, -step):
                self.take(self.over, chunk, offset)
        if self.single(step, 1, 1):
            for chunk in self.turned:
                self.take(self.over, chunk, -step)

    def finish(self):
        for (_, key), kind in self.sent.items():
            copy, here = kind(*key, False)
            pl.when(here)(copy.wait_send)


def silu(rows):
    return rows / (1.0 + jnp.exp(-rows))


def softplus(rows):
    return jnp.maximum(rows, 0.0) + jnp.log(1.0 + jnp.exp(-jnp.abs(rows)))


def piece(vector, offset, size):
    at = pl.multiple_of(offset, 128)
    return vector[pl.ds(at, size)].astype(jnp.float32)[None]


def chosen(core, options):
    best = options[0]
    for at in range(1, len(options)):
        best = jnp.where(core == at, options[at], best)
    return best


def mixers(links, tail, cores, vectors, fetches, refs, sems):
    (x_in, gate, b_in, c_in, dt, added, rates, x_taps, b_taps, c_taps, pool_in,
     pool_weight, prior_x, prior_b, prior_c, prior_pool, x_pad, bc_pad, pool_pad,
     pool_two, pool_four, x_split, bc_conv, b_turned, flat, upright, within, grown, local_in,
     state, before, carry_in, carry_out, channels, far_channels) = refs
    sends, arrivals = sems
    rows, inner = x_in.shape[1:]
    heads = dt.shape[1]
    wide = b_in.shape[2]
    pool = pool_in.shape[2]
    groups = wide // STATE
    span = inner // groups
    blocks = rows // BLOCK
    z, core = links.z, links.core
    lead = 8
    parts = CHAINS
    length = inner // parts
    sources = ((x_in, prior_x), (b_in, prior_b), (c_in, prior_c), (pool_in, prior_pool))

    def tails(at):
        source, target = sources[at]
        return remote(
            source.at[0, pl.ds(rows - tail, tail)], target, sends, arrivals, at, {"sp": z + 1}
        )

    def chain(group):
        return remote(
            carry_out.at[group], carry_in.at[group], sends, arrivals, 4 + group, {"sp": z + 1}
        )

    def pool_letter():
        cols = pl.ds(inner, pool)
        return remote(
            channels.at[:, cols], far_channels.at[:, cols], sends, arrivals, 4 + parts, links.beside
        )

    def block_letter(at):
        place = (pl.ds(at * BLOCK, BLOCK), pl.ds(0, inner))
        return remote(
            channels.at[place], far_channels.at[place], sends, arrivals, 5 + parts + at, links.beside
        )

    follows = z + 1 < links.n
    yield "loaded"
    for at in SOURCES:
        fetches[at].wait()

    @pl.when(follows)
    def _():
        for at in range(4):
            tails(at).start()

    yield "start"
    for at in OTHERS:
        fetches[at].wait()
    x_pad[tail:] = x_in[0].astype(jnp.float32)
    bc_pad[tail:, 0:wide] = b_in[0].astype(jnp.float32)
    bc_pad[tail:, wide:] = c_in[0].astype(jnp.float32)
    pool_pad[0:lead] = jnp.zeros((lead, pool), jnp.float32)
    pool_pad[lead + tail :] = pool_in[0].astype(jnp.float32)
    steps_flat = softplus(dt[0].astype(jnp.float32))
    table = (heads, rates.shape[1])
    picked = lax.broadcasted_iota(jnp.int32, table, 1) == (
        core * heads + lax.broadcasted_iota(jnp.int32, table, 0)
    )
    own_rates = jnp.sum(
        jnp.where(picked, jnp.broadcast_to(rates[...], table), 0.0), axis=1, keepdims=True
    )
    logs_flat = -steps_flat * jnp.exp(own_rates) + added[0]
    flat[...] = jnp.zeros_like(flat)
    down = lax.broadcasted_iota(jnp.int32, (BLOCK, BLOCK), 0)
    over = lax.broadcasted_iota(jnp.int32, (BLOCK, BLOCK), 1)
    causal = down >= over
    upper = (down <= over).astype(jnp.float32)
    first_half = lax.broadcasted_iota(jnp.int32, (BLOCK, 2 * HEAD_DIM), 1) < HEAD_DIM

    def mine(ref, size):
        at = pl.multiple_of(core * size, size)
        return ref[:, pl.ds(at, size)].astype(jnp.float32)

    taps_x = mine(x_taps, inner)
    taps_bc = jnp.concatenate([mine(b_taps, wide), mine(c_taps, wide)], axis=1)
    bias_b = piece(vectors["bias"], core * wide, wide)
    bias_bc = jnp.concatenate([bias_b, jnp.zeros_like(bias_b)], axis=1)

    @pl.when(z == 0)
    def _():
        x_pad[0:tail] = jnp.zeros((tail, inner), jnp.float32)
        bc_pad[0:tail] = jnp.zeros((tail, 2 * wide), jnp.float32)
        pool_pad[lead : lead + tail] = jnp.zeros((tail, pool), jnp.float32)

    @pl.when(z > 0)
    def _():
        for at in range(4):
            tails(at).wait_recv()
        x_pad[0:tail] = prior_x[...].astype(jnp.float32)
        bc_pad[0:tail, 0:wide] = prior_b[...].astype(jnp.float32)
        bc_pad[0:tail, wide:] = prior_c[...].astype(jnp.float32)
        pool_pad[lead : lead + tail] = prior_pool[...].astype(jnp.float32)

    def taps(pad, weights, at, cols):
        total = None
        for tap in range(CONV):
            begin = at * BLOCK + tail - CONV + 1 + tap
            term = pad[begin : begin + BLOCK, cols] * weights[tap : tap + 1, cols]
            total = term if total is None else total + term
        return total

    def spread(narrow, head):
        shape = (BLOCK, 2 * HEAD_DIM)
        return jnp.where(
            first_half,
            jnp.broadcast_to(narrow[:, head : head + 1], shape),
            jnp.broadcast_to(narrow[:, head + 1 : head + 2], shape),
        )

    pairs = span // (2 * HEAD_DIM)
    ends = []
    state[...] = jnp.zeros_like(state)
    for at in range(blocks):
        now = slice(at * BLOCK, (at + 1) * BLOCK)
        bc_conv[now] = silu(taps(bc_pad, taps_bc, at, slice(0, 2 * wide)) + bias_bc).astype(
            jnp.bfloat16
        )
        flat[at, 0:heads] = jnp.dot(
            logs_flat[:, now], upper, precision=EXACT, preferred_element_type=jnp.float32
        )
        flat[at, heads : 2 * heads] = steps_flat[:, now]
        upright[at] = jnp.transpose(flat[at])
        cum = upright[at, :, 0:heads]
        decayed = jnp.exp(cum)
        closing = jnp.exp(cum[BLOCK - 1 : BLOCK] - cum) * upright[at, :, heads : 2 * heads]
        ended = []
        for group in range(groups):
            cols = slice(group * span, (group + 1) * span)
            x_now = silu(taps(x_pad, taps_x, at, cols))
            b_now = bc_conv[now, group * STATE : (group + 1) * STATE]
            b_flat = jnp.transpose(b_now.astype(jnp.float32)).astype(jnp.bfloat16)
            b_turned[at * groups + group] = b_flat
            scaled = []
            for pair in range(pairs):
                head = group * (span // HEAD_DIM) + 2 * pair
                lanes = slice(pair * 2 * HEAD_DIM, (pair + 1) * 2 * HEAD_DIM)
                here = slice(head * HEAD_DIM, (head + 2) * HEAD_DIM)
                x_pair = x_now[:, lanes]
                x_split[at, 0:BLOCK, here] = jnp.where(first_half, x_pair, 0.0).astype(jnp.bfloat16)
                x_split[at, BLOCK : 2 * BLOCK, here] = jnp.where(first_half, 0.0, x_pair).astype(
                    jnp.bfloat16
                )
                x_half = x_pair.astype(jnp.bfloat16).astype(jnp.float32)
                scaled.append((x_half * spread(closing, head)).astype(jnp.bfloat16))
                grown[now, here] = spread(decayed, head)
            end = grown[(at + 1) * BLOCK - 1 : (at + 1) * BLOCK, cols]
            ended.append(end)
            local_in[at, :, cols] = state[:, cols]
            state[:, cols] = state[:, cols] * end + jnp.dot(
                b_flat, jnp.concatenate(scaled, axis=1), preferred_element_type=jnp.float32
            )
        yield at
        ends.append(ended)

    def hand_on():
        @pl.when(z == 0)
        def _():
            before[...] = jnp.zeros_like(before)

        for link in range(parts):
            cols = slice(link * length, (link + 1) * length)
            group, at_end = link * length // span, slice(link * length % span, link * length % span + length)

            @pl.when(z > 0)
            def _(link=link, cols=cols):
                chain(link).wait_recv()
                before[:, cols] = carry_in[link].astype(jnp.float32)

            @pl.when(follows)
            def _(link=link, cols=cols, group=group, at_end=at_end):
                falling = ends[0][group][:, at_end]
                for at in range(1, blocks):
                    falling = falling * ends[at][group][:, at_end]
                carry_out[link] = (before[:, cols] * falling + state[:, cols]).astype(jnp.bfloat16)
                chain(link).start()

    def chain_point(place, last=False):
        pl.when(z >= place if last else z == place)(hand_on)

    chain_point(0)
    yield "states"
    place = z * rows
    position = (place + lax.broadcasted_iota(jnp.int32, (rows, 1), 0)).astype(jnp.float32) + 1.0
    pool_groups = pool // POOL_GROUP
    for group in range(pool_groups):
        cols = slice(group * POOL_GROUP, (group + 1) * POOL_GROUP)
        size = rows + tail
        two = pool_pad[lead:, cols] + pool_pad[lead - 1 : lead - 1 + size, cols]
        pool_two[0:lead] = jnp.zeros((lead, POOL_GROUP), jnp.float32)
        pool_two[lead:] = two
        four = two + pool_two[lead - 2 : lead - 2 + size]
        pool_four[0:lead] = jnp.zeros((lead, POOL_GROUP), jnp.float32)
        pool_four[lead:] = four
        eight = four + pool_four[lead - 4 : lead - 4 + size]
        sixteen = eight[tail:] + eight[tail - 8 : size - 8]
        sums = [two[tail:], four[tail:], eight[tail:], sixteen]
        picks = [c * pool_groups + group for c in range(cores)]
        running = chosen(core, [sums[pick] for pick in picks])
        reach = chosen(core, [jnp.float32(2 ** (pick + 1)) for pick in picks])
        pooled = running / jnp.minimum(position, reach) - pool_in[0, :, cols].astype(jnp.float32)
        mixed = jnp.dot(
            pooled.astype(jnp.bfloat16),
            pool_weight[core * pool_groups + group],
            preferred_element_type=jnp.float32,
        )
        scale = piece(vectors["scale"], core * pool + group * POOL_GROUP, POOL_GROUP)
        out = inner + group * POOL_GROUP
        channels[:, out : out + POOL_GROUP] = (mixed * scale).astype(jnp.bfloat16)
    pool_letter().start()
    for at in range(blocks):
        now = slice(at * BLOCK, (at + 1) * BLOCK)
        cum = upright[at, :, 0:heads]
        cum_flat = flat[at, 0:heads]
        step_flat = flat[at, heads : 2 * heads]
        for group in range(groups):
            c_now = bc_conv[now, wide + group * STATE : wide + (group + 1) * STATE]
            scores = jnp.dot(
                c_now, b_turned[at * groups + group], preferred_element_type=jnp.float32
            )
            for pair in range(pairs):
                first = group * (span // HEAD_DIM) + 2 * pair
                both = []
                for head in (first, first + 1):
                    gap = cum[:, head : head + 1] - cum_flat[head : head + 1]
                    decay = jnp.exp(jnp.where(causal, gap, -1e30))
                    both.append((scores * decay * step_flat[head : head + 1]).astype(jnp.bfloat16))
                here = slice(first * HEAD_DIM, (first + 2) * HEAD_DIM)
                within[now, here] = jnp.dot(
                    jnp.concatenate(both, axis=1),
                    x_split[at, :, here],
                    preferred_element_type=jnp.float32,
                )
    chain_point(1)
    yield "second"
    chain_point(2)
    yield "third"
    chain_point(3, True)
    falling = [None] * groups
    fetches[GATE].wait()
    for at in range(blocks):
        now = slice(at * BLOCK, (at + 1) * BLOCK)
        for group in range(groups):
            cols = slice(group * span, (group + 1) * span)
            earlier = before[:, cols]
            if at:
                earlier = earlier * falling[group]
            entering = local_in[at, :, cols] + earlier
            c_now = bc_conv[now, wide + group * STATE : wide + (group + 1) * STATE]
            carried = jnp.dot(
                c_now, entering.astype(jnp.bfloat16), preferred_element_type=jnp.float32
            )
            mixed = (within[now, cols] + carried * grown[now, cols]) * silu(
                gate[0, now, cols].astype(jnp.float32)
            )
            root = lax.rsqrt(jnp.mean(mixed * mixed, axis=1, keepdims=True) + eps)
            gain = piece(vectors["gain"], core * inner + group * span, span)
            channels[now, cols] = (mixed * root * gain).astype(jnp.bfloat16)
            end = ends[at][group]
            falling[group] = end if at == 0 else falling[group] * end
        block_letter(at).start()
    letters = [pool_letter(), *(block_letter(at) for at in range(blocks))]

    def received():
        for letter in letters:
            letter.wait_recv()

    def finish():
        for letter in letters:
            letter.wait_send()

        @pl.when(follows)
        def _():
            for at in range(4):
                tails(at).wait_send()
            for link in range(parts):
                chain(link).wait_send()

    return received, finish


def whole_kernel(sp_size, fs_size, cores, tail, *refs):
    inputs, ssd_weight, pool_rows, out = refs[:INPUTS], *refs[INPUTS : INPUTS + 3]
    (z_sends, z_arrivals, y_sends, y_arrivals, m_sends, m_arrivals, p_sends, p_arrivals, o_sends,
     o_arrivals, local_sems, whole, parts, part_in, returned, return_in, squares, squares_in,
     *rest) = refs[INPUTS + 3 :]
    held, rest = rest[:INPUTS], rest[INPUTS:]
    vectors = dict(zip(NAMES, held[VECTORS:]))
    held = held[:VECTORS]
    channels, far_channels = rest[-2:]
    links = Links(sp_size, fs_size)
    width = ssd_weight.shape[1]
    inner = ssd_weight.shape[0]
    rows = channels.shape[0]
    half = sp_size // cores
    core = links.core
    own_at = pl.multiple_of((links.z * 2 + links.y) * width, width)
    loads = [
        pltpu.make_async_copy(
            source, whole.at[pl.ds(begin, source.shape[0]), pl.ds(own_at, width)], local_sems.at[at]
        )
        for at, (source, begin) in enumerate(((ssd_weight, 0), (pool_rows, inner)))
    ]
    fetches = [
        pltpu.make_async_copy(source, place, local_sems.at[2 + at])
        for at, (source, place) in enumerate(zip(inputs, (*held, *vectors.values())))
    ]
    for load in loads:
        load.start()
    for at in (*SOURCES, *OTHERS, GATE):
        fetches[at].start()
    links.barrier()
    weights = Weights(links, whole, width, (z_sends, z_arrivals), (y_sends, y_arrivals))
    work = mixers(links, tail, cores, vectors, fetches, (*held, *rest), (m_sends, m_arrivals))

    direct, turned = weights.direct, weights.turned
    both = (0, 1)
    last = sp_size - 1
    mixed = None
    while mixed is None:
        try:
            mark = next(work)
        except StopIteration as ended:
            mixed = ended.value
            break
        if mark == "loaded":
            for load in loads:
                load.wait()
            weights.begin()
            weights.own(direct[:3], ways=(-1,))
        elif mark == "start":
            weights.own(direct[:3], ways=(1,))
        elif mark == 1:
            weights.own(direct[3:4])
        elif mark == "states":
            weights.own(direct[4:])
            weights.turn()
            weights.own(turned, both, (-1,))
            pl.when(links.z == last)(lambda: weights.own(turned, both, (1,)))
            weights.hop(1, direct[:1], ways=(-1,))
        elif mark == "second":
            weights.hop(1, direct[1:3], ways=(-1,))
            pl.when(links.z == 1)(lambda: weights.own(turned, both, (1,)))
            pl.when(links.z == 1)(lambda: weights.hop(1, direct[:4], ways=(1,)))
            pl.when(links.z == last)(lambda: weights.hop(1, direct, ways=(1,)))
            inner_late = jnp.logical_and(links.z >= 2, links.z < last)
            pl.when(inner_late)(lambda: weights.hop(1, direct[:3], ways=(1,)))
        elif mark == "third":
            pl.when(inner_late)(lambda: weights.own(turned, both, (1,)))
            pl.when(inner_late)(lambda: weights.hop(1, direct[3:], ways=(1,)))
            pl.when(links.z == last)(lambda: weights.hop(2, direct[:3], ways=(1,)))
            pl.when(links.z >= 2)(lambda: weights.hop(1, direct[3:], ways=(-1,)))
    received, finish_mixers = mixed
    pl.when(links.z == 0)(lambda: weights.own(turned, both, (1,)))
    pl.when(links.z == 1)(lambda: weights.hop(1, direct[4:], ways=(1,)))
    pl.when(links.z <= 1)(lambda: weights.hop(1, direct[3:], ways=(-1,)))

    def multiply(turn, far, sides=both):
        z = links.nearest(turn)
        source = far_channels if far else channels

        @pl.loop(0, len(sides))
        def _(at):
            y = lax.rem(links.y + sides[0] + at, 2)
            slab = z * 2 + y
            lanes = pl.ds(pl.multiple_of(slab * width, width), width)
            parts[far, slab] = jnp.dot(
                source[...], whole[:, lanes], preferred_element_type=jnp.float32
            ).astype(jnp.bfloat16)

            @pl.when(z // half != core)
            def _():
                part_letter(z, y, far).start()

    def part_letter(z, y, far):
        slab = z * 2 + y
        return remote(
            parts.at[far, slab],
            part_in.at[far, lax.rem(z, half) * 2 + y],
            p_sends,
            p_arrivals,
            far * 2 * sp_size + slab,
            links.sibling,
        )

    def return_letter(slot):
        return remote(
            returned.at[slot], return_in.at[slot], o_sends, o_arrivals, slot, links.beside
        )

    def give_back(turn, sides=both):
        z = links.nearest(turn)

        @pl.when(z // half == core)
        def _():
            @pl.loop(0, len(sides))
            def _(at):
                y = lax.rem(links.y + sides[0] + at, 2)
                part_letter(z, y, 1).wait_recv()
                slot = lax.rem(z, half) * 2 + y
                returned[slot] = (
                    parts[1, z * 2 + y].astype(jnp.float32) + part_in[1, slot].astype(jnp.float32)
                ).astype(jnp.bfloat16)
                return_letter(slot).start()

    edge = jnp.logical_or(links.z == 0, links.z == last)
    weights.settle(0)
    multiply(0, 0)
    for step in range(1, last):
        weights.hop(step, turned, both)
        if step + 1 < last:
            if step == 1:
                pl.when(links.z == last)(lambda: weights.hop(2, direct[3:]))
                pl.when(links.z != last)(lambda: weights.hop(2, direct))
            else:
                weights.hop(step + 1, direct)
            weights.settle(step)
            multiply(step, 0)
    received()
    share = -(-len(direct) // last)

    def ahead(turn):
        multiply(turn, 1)
        give_back(turn)
        multiply(turn, 0)

    for turn in range(last):
        pieces_now = direct[turn * share : (turn + 1) * share]
        if turn == last - 1:
            pl.when(jnp.logical_not(edge))(lambda: ahead(turn))
            weights.settle(turn)
            weights.hop(last, pieces_now)
            pl.when(edge)(lambda: ahead(turn))
        else:
            multiply(turn, 1)
            weights.hop(last, pieces_now)
            give_back(turn)
    weights.hop(last, turned, (0,))
    multiply(last, 1, (0,))
    multiply(last, 0, (0,))
    give_back(last, (0,))
    weights.hop(last, turned, (1,))
    weights.settle(last)
    multiply(last, 1, (1,))
    give_back(last, (1,))
    multiply(last, 0, (1,))
    own_half = core * half
    slots = 2 * half

    def lane_squares(values):
        values = values * values
        total = values[:, 0:128]
        for at in range(1, width // 128):
            total = total + values[:, at * 128 : (at + 1) * 128]
        return total

    def own_total(slot):
        return parts[0, own_half * 2 + slot].astype(jnp.float32) + part_in[0, slot].astype(
            jnp.float32
        )

    squares[...] = jnp.zeros_like(squares)

    @pl.loop(0, slots)
    def _(slot):
        part_letter(own_half + slot // 2, lax.rem(slot, 2), 0).wait_recv()
        squares[...] += lane_squares(own_total(slot))

    @pl.loop(0, slots)
    def _(slot):
        return_letter(slot).wait_recv()
        squares[...] += lane_squares(return_in[slot].astype(jnp.float32))

    exchange = remote(squares, squares_in, o_sends, o_arrivals, slots, links.sibling)
    exchange.start()
    exchange.wait_recv()
    row_squares = jnp.sum(squares[...] + squares_in[...], axis=1, keepdims=True)
    features = cores * out.shape[2]
    root = lax.rsqrt(row_squares / features + eps)

    @pl.loop(0, slots, unroll=True)
    def _(slot):
        first = (slot // 2) * fs_size + 2 * lax.rem(slot, 2)
        for values, x in (
            (own_total(slot), links.x),
            (return_in[slot].astype(jnp.float32), 1 - links.x),
        ):
            at = pl.multiple_of((first + x) * width, width)
            gain = piece(vectors["out"], core * out.shape[2] + at, width)
            out[0, :, pl.ds(at, width)] = (values * root * gain).astype(jnp.bfloat16)

    exchange.wait_send()
    weights.finish()
    finish_mixers()

    @pl.loop(0, 2 * half)
    def _(slot):
        return_letter(slot).wait_send()
        other = (1 - core) * half
        for far in range(2):
            part_letter(other + slot // 2, lax.rem(slot, 2), far).wait_send()


def mixed_and_projected(inputs, vectors, ssd_weight, pool_rows, tail):
    sp_size, fs_size, cores = lax.axis_size("sp"), lax.axis_size("fs"), lax.axis_size("tp")
    width = ssd_weight.shape[1]
    x_in, b_in, pool_in = inputs[0], inputs[2], inputs[10]
    features = vectors["out"].shape[0]
    inputs = (*inputs, *(vectors[name] for name in NAMES))
    tok_rows, inner = x_in.shape[1:]
    wide, pool = b_in.shape[2], pool_in.shape[2]
    groups = wide // STATE
    blocks = tok_rows // BLOCK
    half = sp_size // cores
    slots = 2 * half
    vmem = pl.BlockSpec(memory_space=pltpu.VMEM)
    hbm = pl.BlockSpec(memory_space=pltpu.HBM)
    dma = pltpu.SemaphoreType.DMA
    half_type, full_type = jnp.bfloat16, jnp.float32
    z_spots, y_spots = CHUNKS * (sp_size - 1) * 4, CHUNKS * (2 * sp_size - 1)
    letters = 5 + CHAINS + blocks
    return pl.pallas_call(
        functools.partial(whole_kernel, sp_size, fs_size, cores, tail),
        out_shape=pltpu.VMEM((1, tok_rows, features // cores), half_type),
        in_specs=[hbm] * (len(inputs) + 2),
        out_specs=vmem,
        scratch_shapes=[
            dma((z_spots,)),
            dma((z_spots,)),
            dma((y_spots,)),
            dma((y_spots,)),
            dma((letters,)),
            dma((letters,)),
            dma((4 * sp_size,)),
            dma((4 * sp_size,)),
            dma((slots + 1,)),
            dma((slots + 1,)),
            dma((2 + len(inputs),)),
            pltpu.VMEM((inner + pool, width * 2 * sp_size), half_type),
            pltpu.VMEM((2, 2 * sp_size, tok_rows, width), half_type),
            pltpu.VMEM((2, slots, tok_rows, width), half_type),
            pltpu.VMEM((slots, tok_rows, width), half_type),
            pltpu.VMEM((slots, tok_rows, width), half_type),
            pltpu.VMEM((tok_rows, 128), full_type),
            pltpu.VMEM((tok_rows, 128), full_type),
            *(pltpu.VMEM(array.shape, array.dtype) for array in inputs),
            pltpu.VMEM((tail, inner), half_type),
            pltpu.VMEM((tail, wide), half_type),
            pltpu.VMEM((tail, wide), half_type),
            pltpu.VMEM((tail, pool), half_type),
            pltpu.VMEM((tail + tok_rows, inner), full_type),
            pltpu.VMEM((tail + tok_rows, 2 * wide), full_type),
            pltpu.VMEM((8 + tail + tok_rows, pool), full_type),
            pltpu.VMEM((8 + tail + tok_rows, POOL_GROUP), full_type),
            pltpu.VMEM((8 + tail + tok_rows, POOL_GROUP), full_type),
            pltpu.VMEM((blocks, 2 * BLOCK, inner), half_type),
            pltpu.VMEM((tok_rows, 2 * wide), half_type),
            pltpu.VMEM((blocks * groups, STATE, BLOCK), half_type),
            pltpu.VMEM((blocks, 128, BLOCK), full_type),
            pltpu.VMEM((blocks, BLOCK, 128), full_type),
            pltpu.VMEM((tok_rows, inner), full_type),
            pltpu.VMEM((tok_rows, inner), full_type),
            pltpu.VMEM((blocks, STATE, inner), full_type),
            pltpu.VMEM((STATE, inner), full_type),
            pltpu.VMEM((STATE, inner), full_type),
            pltpu.VMEM((CHAINS, STATE, inner // CHAINS), half_type),
            pltpu.VMEM((CHAINS, STATE, inner // CHAINS), half_type),
            pltpu.VMEM((tok_rows, inner + pool), half_type),
            pltpu.VMEM((tok_rows, inner + pool), half_type),
        ],
        compiler_params=pltpu.CompilerParams(
            collective_id=0, has_side_effects=True, vmem_limit_bytes=48 * 2**20
        ),
        name="paired_mixers",
    )(*(pltpu.with_memory_space_constraint(array, pltpu.HBM) for array in (*inputs, ssd_weight, pool_rows)))


def causal_taps(input_rows, prior_rows, tap_weights, offset_bias):
    padded = jnp.concatenate([prior_rows, input_rows], axis=0).astype(jnp.float32)
    tok_rows = input_rows.shape[0]
    running = jnp.zeros(input_rows.shape, jnp.float32) + offset_bias
    for tap_index in range(tap_weights.shape[0]):
        running = (
            running
            + tap_weights[tap_index].astype(jnp.float32) * padded[tap_index : tap_index + tok_rows]
        )
    return jax.nn.silu(running).astype(jnp.bfloat16)


def pool_mix(input_rows, prior_rows, positions, group_ids, local_weight, local_scale):
    tail_rows = prior_rows.shape[0]
    tok_rows = input_rows.shape[0]
    padded = jnp.concatenate([prior_rows, input_rows], axis=0).astype(jnp.float32)
    window_reach = jnp.left_shift(jnp.int32(2), group_ids)
    running = jnp.zeros(input_rows.shape, jnp.float32)
    for offset_back in range(tail_rows + 1):
        start_row = tail_rows - offset_back
        running = running + padded[start_row : start_row + tok_rows] * (
            offset_back < window_reach
        ).astype(jnp.float32)
    window_count = jnp.minimum(positions[:, None] + 1.0, window_reach.astype(jnp.float32)[None, :])
    pooled = (running / window_count - input_rows.astype(jnp.float32)).astype(jnp.bfloat16)
    grouped = pooled.reshape(tok_rows, local_weight.shape[0], local_weight.shape[1])
    mixed = jnp.einsum("lgc,gcd->lgd", grouped, local_weight, preferred_element_type=jnp.float32)
    return (mixed.reshape(input_rows.shape) * local_scale.astype(jnp.float32)).astype(jnp.bfloat16)


def join_states(earlier, later_part):
    return (
        earlier[0] + later_part[0],
        earlier[1] * jnp.exp(later_part[0])[..., None, None] + later_part[1],
    )


def body(
    statespace_input,
    output_gate_input,
    state_input_projection,
    state_output_projection,
    step_size_input,
    added_log_decay,
    logarithm_rates,
    head_channel_taps,
    input_projection_taps,
    output_projection_taps,
    input_projection_bias,
    group_norm_gain,
    pooling_input,
    pooling_group_weight,
    pooling_channel_scale,
    statespace_output_weight,
    pooling_output_weight,
    output_norm_gain,
):
    core_count = lax.axis_size("tp")
    sp_size, fs_size = lax.axis_size("sp"), lax.axis_size("fs")
    pool_tail = 2**POOL_GROUPS - 1
    paired = (
        statespace_output_weight.shape[1] % 128 == 0
        and fs_size == 4
        and core_count == 2
        and sp_size in (4, 8)
    )
    if paired:
        return mixed_and_projected(
            (
                statespace_input,
                output_gate_input,
                state_input_projection,
                state_output_projection,
                jnp.swapaxes(step_size_input, 1, 2),
                jnp.swapaxes(added_log_decay, 1, 2),
                logarithm_rates[None],
                head_channel_taps,
                input_projection_taps,
                output_projection_taps,
                pooling_input,
                pooling_group_weight,
            ),
            {
                "out": output_norm_gain,
                "gain": group_norm_gain,
                "scale": pooling_channel_scale,
                "bias": input_projection_bias,
            },
            statespace_output_weight,
            pooling_output_weight,
            pool_tail + 1,
        )
    core_index = lax.axis_index("tp")
    seq_index = lax.axis_index("sp")
    head_channel_rows = statespace_input[0]
    output_gate_rows = output_gate_input[0]
    input_projection_rows = state_input_projection[0]
    output_projection_rows = state_output_projection[0]
    step_size_rows = step_size_input[0]
    decay_spikes = added_log_decay[0]
    pooling_rows = pooling_input[0]
    tok_rows = head_channel_rows.shape[0]
    inner_local = head_channel_rows.shape[1]
    heads_local = step_size_rows.shape[1]
    state_local = input_projection_rows.shape[1]
    pool_local = pooling_rows.shape[1]
    groups_local = state_local // STATE
    per_group = heads_local // groups_local
    groups_pool = pool_local // POOL_GROUP
    conv_tail = CONV - 1
    own_columns = jnp.concatenate([statespace_output_weight, pooling_output_weight], axis=0)
    tails = jnp.concatenate(
        [
            jnp.pad(rows[tok_rows - tail :], ((pool_tail - tail, 0), (0, 0)))
            for rows, tail in (
                (head_channel_rows, conv_tail),
                (input_projection_rows, conv_tail),
                (output_projection_rows, conv_tail),
                (pooling_rows, pool_tail),
            )
        ],
        axis=1,
    )
    prior = passed_along(tails, "sp", 1)
    widths = (inner_local, state_local, state_local, pool_local)
    prior_x, prior_b, prior_c, prior_pool = (
        prior[pool_tail - tail :, sum(widths[:at]) : sum(widths[: at + 1])]
        for at, tail in enumerate((conv_tail, conv_tail, conv_tail, pool_tail))
    )
    taps_x = lax.dynamic_slice_in_dim(head_channel_taps, core_index * inner_local, inner_local, 1)
    taps_b = lax.dynamic_slice_in_dim(
        input_projection_taps, core_index * state_local, state_local, 1
    )
    taps_c = lax.dynamic_slice_in_dim(
        output_projection_taps, core_index * state_local, state_local, 1
    )
    bias_b = lax.dynamic_slice_in_dim(
        input_projection_bias, core_index * state_local, state_local, 0
    )
    gain_ssd = lax.dynamic_slice_in_dim(group_norm_gain, core_index * inner_local, inner_local, 0)
    head_decay_rates = jnp.exp(
        lax.dynamic_slice_in_dim(logarithm_rates, core_index * heads_local, heads_local, 0)
    )
    gain_pool = lax.dynamic_slice_in_dim(
        pooling_channel_scale, core_index * pool_local, pool_local, 0
    )
    weight_pool = lax.dynamic_slice_in_dim(
        pooling_group_weight, core_index * groups_pool, groups_pool, 0
    )
    whole_columns = lax.all_gather(own_columns, ("sp", "fs"), axis=1, tiled=True)
    x_conv = causal_taps(head_channel_rows, prior_x, taps_x, 0.0)
    b_conv = causal_taps(input_projection_rows, prior_b, taps_b, bias_b.astype(jnp.float32))
    c_conv = causal_taps(output_projection_rows, prior_c, taps_c, 0.0)
    blocks = tok_rows // BLOCK
    discrete_step_size = jax.nn.softplus(step_size_rows.astype(jnp.float32))
    logarithm_decay = -discrete_step_size * head_decay_rates + decay_spikes
    cumulative_decay = jnp.cumsum(
        logarithm_decay.reshape(blocks, BLOCK, groups_local, per_group), axis=1
    )
    cum_t = cumulative_decay.transpose(0, 2, 3, 1)
    step_t = discrete_step_size.reshape(blocks, BLOCK, groups_local, per_group).transpose(
        0, 2, 3, 1
    )
    heads_x = x_conv.reshape(blocks, BLOCK, groups_local, per_group, HEAD_DIM)
    group_b = b_conv.reshape(blocks, BLOCK, groups_local, STATE)
    group_c = c_conv.reshape(blocks, BLOCK, groups_local, STATE)
    scores = jnp.einsum("ktgn,kugn->kgtu", group_c, group_b, preferred_element_type=jnp.float32)
    causal = jnp.arange(BLOCK)[:, None] >= jnp.arange(BLOCK)[None, :]
    decay_gap = cum_t[..., :, None] - cum_t[..., None, :]
    decay_factor = jnp.where(causal, jnp.exp(jnp.where(causal, decay_gap, 0.0)), 0.0)
    weights = (scores[:, :, None] * decay_factor * step_t[..., None, :]).astype(jnp.bfloat16)
    within = jnp.einsum("kgetu,kugep->ktgep", weights, heads_x, preferred_element_type=jnp.float32)
    block_end = cum_t[..., -1]
    end_weight = jnp.exp(block_end[..., None] - cum_t) * step_t
    scaled_x = (heads_x * end_weight.transpose(0, 3, 1, 2)[..., None]).astype(jnp.bfloat16)
    block_state = jnp.einsum(
        "kugep,kugn->kgepn", scaled_x, group_b, preferred_element_type=jnp.float32
    )

    def local_chain(state_now, current_inputs):
        piece_state, piece_fall = current_inputs
        return (state_now * jnp.exp(piece_fall)[..., None, None] + piece_state, state_now)

    final_state, local_entering = lax.scan(
        local_chain, jnp.zeros(block_state.shape[1:], jnp.float32), (block_state, block_end)
    )
    log_total = jnp.sum(block_end, axis=0)
    prefix_log = jnp.cumsum(block_end, axis=0) - block_end
    log_before, state_before = entering_2(
        (log_total, final_state),
        "sp",
        join_states,
        (jnp.zeros_like(log_total), jnp.zeros_like(final_state)),
    )
    entering = (local_entering + jnp.exp(prefix_log)[..., None, None] * state_before[None]).astype(
        jnp.bfloat16
    )
    carried_out = jnp.einsum(
        "ktgn,kgepn->ktgep", group_c, entering, preferred_element_type=jnp.float32
    )
    carried_out = carried_out * jnp.exp(cumulative_decay)[..., None]
    mixed_ssd = (within + carried_out).reshape(tok_rows, inner_local) * jax.nn.silu(
        output_gate_rows.astype(jnp.float32)
    )
    grouped = mixed_ssd.reshape(tok_rows, groups_local, inner_local // groups_local)
    normed = grouped * lax.rsqrt(jnp.mean(grouped * grouped, axis=-1, keepdims=True) + eps)
    ssd_out = (normed.reshape(tok_rows, inner_local) * gain_ssd.astype(jnp.float32)).astype(
        jnp.bfloat16
    )
    positions = (seq_index * tok_rows + jnp.arange(tok_rows, dtype=jnp.int32)).astype(jnp.float32)
    group_ids = core_index * groups_pool + jnp.arange(pool_local, dtype=jnp.int32) // POOL_GROUP
    pool_out = pool_mix(pooling_rows, prior_pool, positions, group_ids, weight_pool, gain_pool)
    channels = jnp.concatenate([ssd_out, pool_out], axis=1)
    half_width = D // core_count
    gain_out = lax.dynamic_slice_in_dim(
        output_norm_gain, core_index * half_width, half_width, 0
    ).astype(jnp.float32)
    partial = jnp.dot(channels, whole_columns, preferred_element_type=jnp.float32).astype(
        jnp.bfloat16
    )
    own_half = lax.dynamic_slice_in_dim(partial, core_index * half_width, half_width, 1).astype(
        jnp.float32
    )
    for hop in range(1, core_count):
        target = lax.rem(core_index + hop, core_count)
        leaving = lax.dynamic_slice_in_dim(partial, target * half_width, half_width, 1)
        route = [(i, (i + hop) % core_count) for i in range(core_count)]
        own_half = own_half + lax.ppermute(leaving, "tp", route).astype(jnp.float32)
    row_squares = lax.psum(jnp.sum(own_half * own_half, axis=1), "tp")
    result = own_half * lax.rsqrt(row_squares / D + eps)[:, None] * gain_out
    return result.astype(jnp.bfloat16)[None]


def solution(mesh):
    in_specs = (
        P("fs", "sp", "tp"),
        P("fs", "sp", "tp"),
        P("fs", "sp", "tp"),
        P("fs", "sp", "tp"),
        P("fs", "sp", "tp"),
        P("fs", "sp", "tp"),
        P(),
        P(),
        P(),
        P(),
        P(),
        P(),
        P("fs", "sp", "tp"),
        P(),
        P(),
        P("tp", ("sp", "fs")),
        P("tp", ("sp", "fs")),
        P(),
    )
    out_specs = P("fs", "sp", "tp")
    return jax.shard_map(body, mesh=mesh, in_specs=in_specs, out_specs=out_specs, check_vma=False)
```
